32 devices in a mesh: sp: 4 (over y, x), tp: 8 (over z, core).
Axes of the slice: x: 2, y: 2, z: 4, core: 2. Of those that a mesh axis runs over, the one named last changes fastest.
Arguments:
- resid: bfloat16 [2048, 2048], P(('sp', 'tp')), may hold values from -6 to 6
- query_a: bfloat16 [2048, 16, 128], P('sp', 'tp'), may hold values from -16 to 16
- key_a: bfloat16 [2048, 16, 128], P('sp', 'tp'), may hold values from -16 to 16
- value_a: bfloat16 [2048, 16, 128], P('sp', 'tp'), may hold values from -6 to 6
- query_b: bfloat16 [2048, 16, 64], P('sp', 'tp'), may hold values from -16 to 16
- key_b: bfloat16 [2048, 16, 64], P('sp', 'tp'), may hold values from -16 to 16
- value_b: bfloat16 [2048, 16, 64], P('sp', 'tp'), may hold values from -6 to 6
- mix_a: float32 [16], P('tp'), may hold values from 0.3 to 0.8
- mix_b: float32 [16], P('tp'), may hold values from 0.3 to 0.8
- head_gain_a: float32 [128], replicated, may hold values from 0.1 to 1.9
- head_gain_b: float32 [64], replicated, may hold values from 0.1 to 1.9
- proj_a: bfloat16 [2048, 2048], P('tp'), may hold values from -0.109375 to 0.109375
- proj_b: bfloat16 [1024, 2048], P('tp'), may hold values from -0.109375 to 0.109375
- norm_gain: float32 [2048], replicated, may hold values from 0.1 to 1.9
- route_ids: int32 [2048, 2], P(('sp', 'tp')), may hold values from 0 to 3, all different within a row; in each aligned block of 64 rows (0 to 63, 64 to 127, ...) at most 48 rows name the same one
- route_weights: float32 [2048, 2], P(('sp', 'tp')), may hold values from 0.2 to 1
- expert_gate: bfloat16 [4, 2048, 6144], P('sp', None, 'tp'), may hold values from -0.125 to 0.125
- expert_up: bfloat16 [4, 2048, 6144], P('sp', None, 'tp'), may hold values from -0.125 to 0.125
- expert_down: bfloat16 [4, 6144, 2048], P('sp', 'tp'), may hold values from -0.078125 to 0.078125
Outputs:
- out: bfloat16 [2048, 2048], P(('sp', 'tp'))
The draws below stay inside these ranges and needn't reach their ends.
Inputs may be any that keep to these rules, and one draw needn't show every extreme that they name: `route_ids`: each row names 2 different experts. Within the rows of one device (aligned blocks of 64 rows) no expert is named by more than 48 rows, and in every draw some device's block names some expert exactly 48 times.
All inputs are finite; a program needn't handle non-finite values.
Results may differ from the reference program's by a relative error of at most 0.02.
Values may be sent and summed in bfloat16 or wider, within the bound.
No kernel may reach another device: no remote copies, remote signals or barrier semaphores. Data moves between devices by JAX's collectives and lax.ppermute only.
A program may use at most 128 MiB of HBM per device.

```python
import math
import jax
import jax.numpy as jnp
import numpy as np
from jax import lax

D = 2048
HEADS_A = 16
QK_A = 64
V_A = 128
HEADS_B = 16
QK_B = 32
V_B = 64
FF = 6144
TOP = 2
SEQ_DEV = 512
EXPERTS = 4
TOK_DEV = 64
CAP = 48
TOKENS = 2048
N_TP = 8


def drawn_pair(key, heads, width):
    shape = (TOKENS, heads, 2 * width)
    query = jnp.clip(jax.random.normal(jax.random.fold_in(key, 21), shape, jnp.float32) * 1.3, -8.0, 8.0)
    keys = jnp.clip(jax.random.normal(jax.random.fold_in(key, 22), shape, jnp.float32) * 1.3, -8.0, 8.0)
    return (query, keys)


def draw_query_a(key, part):
    return drawn_pair(jax.random.fold_in(key, 1), HEADS_A, QK_A)[0].astype(jnp.bfloat16)


def draw_key_a(key, part):
    return drawn_pair(jax.random.fold_in(key, 1), HEADS_A, QK_A)[1].astype(jnp.bfloat16)


def draw_query_b(key, part):
    return drawn_pair(jax.random.fold_in(key, 2), HEADS_B, QK_B)[0].astype(jnp.bfloat16)


def draw_key_b(key, part):
    return drawn_pair(jax.random.fold_in(key, 2), HEADS_B, QK_B)[1].astype(jnp.bfloat16)


def level_of(stream_key, shape, split, smallest, largest):
    def one(axis_at, parts):
        steps = jax.random.uniform(jax.random.fold_in(jax.random.fold_in(stream_key, 6), axis_at), (parts,), jnp.float32, smallest / len(split), largest / len(split))
        return jnp.repeat(jnp.exp(steps), shape[axis_at] // parts).reshape((-1,) + (1,) * (len(shape) - axis_at - 1))

    loudness = one(*split[0])
    for cut in split[1:]:
        loudness = loudness * one(*cut)
    return loudness


def routed_block(key, own, number, rows, number_of, top, most, skew):
    order = jax.random.permutation(key, number_of)
    packed, common = shares(number_of, rows * top, most, skew, True), shares(number_of, rows * top, most, skew, False)
    places = jnp.arange(number_of)

    def named(tallies, turn):
        used = int((tallies > 0).sum())
        fixed = max(1, used // 4)
        moved = fixed + (places - fixed + turn * (used - fixed)) % max(1, number_of - fixed)
        return jnp.zeros((number_of,), jnp.int32).at[order[jnp.where(places < fixed, places, moved)]].set(jnp.asarray(tallies, jnp.int32))

    tallies = jnp.where(number % 4 == 0, named(packed, number // 4), named(common, number - number // 4 - 1))
    mixed = jax.random.permutation(jax.random.fold_in(own, 3), number_of)
    source_of, sink = mixed[0:number_of // 2 * 2:2], mixed[1:number_of // 2 * 2:2]
    margin = jnp.minimum(tallies[source_of] - 1, most - tallies[sink]) // 2
    margin = jnp.where((source_of == order[0]) | (sink == order[0]) | (tallies[sink] == 0), 0, jnp.maximum(margin, 0))
    moved = jax.random.randint(jax.random.fold_in(own, 4), (number_of // 2,), 0, 1 << 20) % (margin + 1)
    tallies = tallies.at[source_of].add(-moved).at[sink].add(moved)
    items = jnp.searchsorted(jnp.cumsum(tallies), jnp.arange(rows * top), side="right").astype(jnp.int32)
    table = items.reshape(top, rows).T
    table = table[jax.random.permutation(jax.random.fold_in(own, 1), rows)]
    turn = jax.random.randint(jax.random.fold_in(own, 2), (rows, 1), 0, top)
    return jnp.take_along_axis(table, (jnp.arange(top)[None, :] + turn) % top, axis=1)


def shares(number_of, total, reach, skew, full):
    loads = [(1 << 20) // math.isqrt(grade ** skew) + 1 for grade in range(1, number_of + 1)]
    largest = reach if full else min(reach, max(-(-total // number_of), total * loads[0] // sum(loads)))
    least = 1 if total - largest >= number_of - 1 else 0
    given, spare = [largest] + [least] * (number_of - 1), total - largest - least * (number_of - 1)
    while spare > 0:
        movable = [i for i in range(1, number_of) if given[i] < largest] or [i for i in range(1, number_of) if given[i] < reach]
        mass, remaining = sum([loads[i] for i in movable]), spare
        for i in movable:
            more = min(reach - given[i], max(1, remaining * loads[i] // mass), spare)
            given[i] = given[i] + more
            spare = spare - more
    return np.array(given)


def gaussian(stream_key, dims, scale, most, shards=(), held_as=jnp.bfloat16):
    drawn = jax.random.normal(stream_key, dims, jnp.float32) * scale
    if len(shards) > 0:
        drawn = level_of(stream_key, dims, shards, -0.22, 0.18) * drawn
    return jnp.clip(drawn, min=-most, max=most).astype(held_as)


def setup_inputs(seed: int = 0) -> dict:
    streams_of = jax.random.split(jax.random.key(seed), 20)
    resid = gaussian(streams_of[0], (TOKENS, D), 1.0, 6.0, ((0, 32),))
    query_a = draw_query_a(jax.random.fold_in(streams_of[19], 71), 0)
    key_a = draw_key_a(jax.random.fold_in(streams_of[19], 71), 0)
    value_a = gaussian(streams_of[3], (TOKENS, HEADS_A, V_A), 1.0, 6.0, ((0, 4), (1, 8)))
    query_b = draw_query_b(jax.random.fold_in(streams_of[19], 71), 0)
    key_b = draw_key_b(jax.random.fold_in(streams_of[19], 71), 0)
    value_b = gaussian(streams_of[6], (TOKENS, HEADS_B, V_B), 1.0, 6.0, ((0, 4), (1, 8)))
    mix_a = jnp.clip(0.3 + 0.5 * jax.random.uniform(streams_of[7], (HEADS_A,), jnp.float32) ** level_of(streams_of[7], (HEADS_A,), ((0, 8),), -0.2, 0.2), 0.3, 0.8)
    mix_b = jnp.clip(0.3 + 0.5 * jax.random.uniform(streams_of[8], (HEADS_B,), jnp.float32) ** level_of(streams_of[8], (HEADS_B,), ((0, 8),), -0.2, 0.2), 0.3, 0.8)
    head_gain_a = jnp.clip(1.0 + 0.18 * jax.random.normal(streams_of[9], (V_A,), jnp.float32), 0.1, 1.9)
    head_gain_b = jnp.clip(1.0 + 0.18 * jax.random.normal(streams_of[10], (V_B,), jnp.float32), 0.1, 1.9)
    proj_a = gaussian(streams_of[11], (HEADS_A * V_A, D), (HEADS_A * V_A + HEADS_B * V_B) ** -0.5, 0.109375, ((0, 8),))
    proj_b = gaussian(streams_of[12], (HEADS_B * V_B, D), (HEADS_A * V_A + HEADS_B * V_B) ** -0.5, 0.109375, ((0, 8),))
    norm_gain = jnp.clip(1.0 + 0.18 * jax.random.normal(streams_of[13], (D,), jnp.float32), 0.1, 1.9)
    route_ids_keys = jax.random.split(jax.random.fold_in(streams_of[14], 1), TOKENS // TOK_DEV)
    route_ids_turns = jax.random.permutation(jax.random.fold_in(streams_of[14], 3), TOKENS // TOK_DEV)
    route_ids = jax.vmap(lambda own, number: routed_block(jax.random.fold_in(streams_of[14], 2), own, number, TOK_DEV, EXPERTS, TOP, CAP, 1))(route_ids_keys, route_ids_turns).reshape((TOKENS, TOP))
    route_weights = jnp.clip(0.2 + 0.8 * jax.random.uniform(streams_of[15], (TOKENS, TOP), jnp.float32) ** level_of(streams_of[15], (TOKENS, TOP), ((0, 32),), -0.2, 0.2), 0.2, 1.0)
    expert_gate = gaussian(streams_of[16], (EXPERTS, D, FF), D ** -0.5, 0.125, ((0, 4), (2, 8)))
    expert_up = gaussian(streams_of[17], (EXPERTS, D, FF), D ** -0.5, 0.125, ((0, 4), (2, 8)))
    expert_down = gaussian(streams_of[18], (EXPERTS, FF, D), FF ** -0.5, 0.078125, ((0, 4), (1, 8)))
    return {"resid": resid, "query_a": query_a, "key_a": key_a, "value_a": value_a, "query_b": query_b, "key_b": key_b, "value_b": value_b, "mix_a": mix_a, "mix_b": mix_b, "head_gain_a": head_gain_a, "head_gain_b": head_gain_b, "proj_a": proj_a, "proj_b": proj_b, "norm_gain": norm_gain, "route_ids": route_ids, "route_weights": route_weights, "expert_gate": expert_gate, "expert_up": expert_up, "expert_down": expert_down}


EPS = 1e-06
HEAD_SCALE = 1.0 - (0.8 - 0.6 * math.exp(-0.3))

def attend(query, key, value, mix, gain):
    length, heads, double = query.shape
    width = double // 2
    scale = 1.0 / math.sqrt(width)
    block_rows = SEQ_DEV // 2
    keys_float = key.astype(jnp.float32)
    values_float = value.astype(jnp.float32)
    key_pos = jnp.arange(length, dtype=jnp.int32)

    def one_block(index):
        first = index * block_rows
        block = lax.dynamic_slice_in_dim(query, first, block_rows, 0).astype(jnp.float32)
        query_pos = first + jnp.arange(block_rows, dtype=jnp.int32)
        allowed = key_pos[None, :] <= query_pos[:, None]
        results = []
        for which in range(2):
            scores = jnp.einsum('qhd,khd->hqk', block[:, :, which * width:(which + 1) * width], keys_float[:, :, which * width:(which + 1) * width]) * scale
            scores = jnp.where(allowed[None], scores, -jnp.inf)
            shifted = jnp.exp(scores - lax.optimization_barrier(jnp.max(scores, axis=2, keepdims=True)))
            sums = lax.optimization_barrier(jnp.sum(shifted, axis=2))
            rounded = lax.optimization_barrier(shifted.astype(jnp.bfloat16)).astype(jnp.float32)
            weighted = jnp.einsum('hqk,khv->qhv', rounded, values_float)
            results.append(weighted / jnp.transpose(sums)[:, :, None])
        return results[0] - mix[None, :, None] * results[1]
    mixed = lax.map(one_block, jnp.arange(length // block_rows, dtype=jnp.int32))
    mixed = mixed.reshape(length, heads, -1)
    normed = mixed * lax.rsqrt(lax.optimization_barrier(jnp.mean(mixed * mixed, axis=2, keepdims=True)) + EPS) * gain * HEAD_SCALE
    return normed.astype(jnp.bfloat16).reshape(length, -1)

def slot_numbers(route_rows, experts, capacity):
    count, top_count = route_rows.shape
    flat = route_rows.reshape(count * top_count)
    onehot = (flat[:, None] == jnp.arange(experts, dtype=jnp.int32)[None, :]).astype(jnp.int32)
    ranks = lax.optimization_barrier(jnp.sum((jnp.cumsum(onehot, axis=0) - onehot) * onehot, axis=1))
    return (flat * capacity + ranks).reshape(count, top_count)

def reference(resid, query_a, key_a, value_a, query_b, key_b, value_b, mix_a, mix_b, head_gain_a, head_gain_b, proj_a, proj_b, norm_gain, route_ids, route_weights, expert_gate, expert_up, expert_down):
    heads_a = attend(query_a, key_a, value_a, mix_a, head_gain_a)
    heads_b = attend(query_b, key_b, value_b, mix_b, head_gain_b)
    cols_a = heads_a.shape[1] // N_TP
    cols_b = heads_b.shape[1] // N_TP
    mixed = resid.astype(jnp.float32)
    for shard in range(N_TP):
        partial_sum = jnp.dot(heads_a[:, shard * cols_a:(shard + 1) * cols_a], proj_a[shard * cols_a:(shard + 1) * cols_a], preferred_element_type=jnp.float32)
        partial_sum = partial_sum + jnp.dot(heads_b[:, shard * cols_b:(shard + 1) * cols_b], proj_b[shard * cols_b:(shard + 1) * cols_b], preferred_element_type=jnp.float32)
        mixed = mixed + lax.optimization_barrier(partial_sum.astype(jnp.bfloat16)).astype(jnp.float32)
    normed = (mixed * lax.rsqrt(lax.optimization_barrier(jnp.mean(mixed * mixed, axis=1, keepdims=True)) + EPS) * norm_gain).astype(jnp.bfloat16)
    blocks = TOKENS // TOK_DEV
    local = jax.vmap(lambda rows_in: slot_numbers(rows_in, EXPERTS, CAP))(route_ids.reshape(blocks, TOK_DEV, TOP))
    row_index = (jnp.arange(blocks, dtype=jnp.int32)[:, None, None] * CAP + local % CAP).reshape(-1)
    expert_index = route_ids.reshape(-1)
    buffer = jnp.zeros((EXPERTS, blocks * CAP, D), jnp.bfloat16)
    buffer = buffer.at[expert_index, row_index].set(jnp.repeat(normed, TOP, axis=0))
    block_width = FF // N_TP

    def run_expert(operands):
        rows_in, gate_w, up_w, down_w = operands
        gate = jnp.dot(rows_in, gate_w, preferred_element_type=jnp.float32)
        upward = jnp.dot(rows_in, up_w, preferred_element_type=jnp.float32)
        hidden = (jax.nn.silu(gate) * upward).astype(jnp.bfloat16)
        summed = jnp.zeros((rows_in.shape[0], D), jnp.float32)
        for shard in range(N_TP):
            part = jnp.dot(hidden[:, shard * block_width:(shard + 1) * block_width], down_w[shard * block_width:(shard + 1) * block_width], preferred_element_type=jnp.float32)
            summed = summed + lax.optimization_barrier(part.astype(jnp.bfloat16)).astype(jnp.float32)
        return summed.astype(jnp.bfloat16)
    outputs = lax.map(run_expert, (buffer, expert_gate, expert_up, expert_down))
    picked = outputs[expert_index, row_index].reshape(TOKENS, TOP, D).astype(jnp.float32)
    result = mixed + lax.optimization_barrier(jnp.sum(route_weights[:, :, None] * picked, axis=1))
    return result.astype(jnp.bfloat16)
```

```python
import math

import jax
import jax.numpy as jnp
from jax import lax
from jax.experimental import pallas as pl
from jax.experimental.pallas import tpu as pltpu
from jax.sharding import PartitionSpec as P

EPS = 1e-06
NEG = -1e30
HEAD_SCALE = 1.0 - (0.8 - 0.6 * math.exp(-0.3))
KEY_STEP = 512


def partner(value, axis, apart):
    return lax.ppermute(value, axis, [(i, i ^ 1 << apart) for i in range(lax.axis_size(axis))])


def rms_scaled(values, gain):
    return values * lax.rsqrt(jnp.mean(values * values, axis=-1, keepdims=True) + EPS) * gain


def slot_numbers(route_rows, experts, capacity):
    count, top_count = route_rows.shape
    flat = route_rows.reshape(count * top_count)
    onehot = (flat[:, None] == jnp.arange(experts, dtype=jnp.int32)[None, :]).astype(jnp.int32)
    ranks = jnp.sum((jnp.cumsum(onehot, axis=0) - onehot) * onehot, axis=1)
    return (flat * capacity + ranks).reshape(count, top_count)


def empty_map(count, heads, width):
    return (
        jnp.zeros((count, heads, width), jnp.float32),
        jnp.full((heads, count), NEG, jnp.float32),
        jnp.zeros((heads, count), jnp.float32),
    )


def empty_group(query, value):
    return (
        empty_map(query.shape[0], query.shape[1], value.shape[2]),
        empty_map(query.shape[0], query.shape[1], value.shape[2]),
    )


def map_update(state, query, keys, values, allowed, scale):
    weighted, maximum, sums = state
    scores = jnp.einsum("qhd,khd->hqk", query, keys, preferred_element_type=jnp.float32) * scale
    scores = jnp.where(allowed[None], scores, NEG)
    fresh = jnp.maximum(maximum, jnp.max(scores, axis=2))
    weights = jnp.where(allowed[None], jnp.exp(scores - fresh[:, :, None]), 0.0)
    factor = jnp.exp(maximum - fresh)
    sums = sums * factor + jnp.sum(weights, axis=2)
    added = jnp.einsum(
        "hqk,khv->qhv", weights.astype(jnp.bfloat16), values, preferred_element_type=jnp.float32
    )
    weighted = weighted * jnp.transpose(factor)[:, :, None] + added
    return (weighted, fresh, sums)


def group_update(states, query, keys, values, allowed):
    width = query.shape[2] // 2
    scale = 1.0 / math.sqrt(width)
    return tuple(
        (
            map_update(
                states[which],
                query[:, :, which * width : (which + 1) * width],
                keys[:, :, which * width : (which + 1) * width],
                values,
                allowed,
                scale,
            )
            for which in range(2)
        )
    )


def set_update(carry, queries, pieces):
    rows_a, rows_b, query_pos = queries
    piece_key_a, piece_value_a, piece_key_b, piece_value_b = pieces
    length = piece_key_a.shape[0]
    step = math.gcd(length, KEY_STEP)
    latest = query_pos[-1]

    def inner(index, states):
        first = index * step

        def compute(current):
            keys_a = lax.dynamic_slice_in_dim(piece_key_a, first, step, 0)
            values_a = lax.dynamic_slice_in_dim(piece_value_a, first, step, 0)
            keys_b = lax.dynamic_slice_in_dim(piece_key_b, first, step, 0)
            values_b = lax.dynamic_slice_in_dim(piece_value_b, first, step, 0)
            key_pos = first + jnp.arange(step, dtype=jnp.int32)
            allowed = key_pos[None, :] <= query_pos[:, None]
            return (
                group_update(current[0], rows_a, keys_a, values_a, allowed),
                group_update(current[1], rows_b, keys_b, values_b, allowed),
            )

        return lax.cond(first <= latest, compute, lambda current: current, states)

    return lax.fori_loop(0, length // step, inner, carry)


def finish_group(states, mix, gain):
    outputs = [state[0] / jnp.transpose(state[2])[:, :, None] for state in states]
    mixed = outputs[0] - mix[None, :, None] * outputs[1]
    normed = rms_scaled(mixed, gain) * HEAD_SCALE
    return normed.astype(jnp.bfloat16).reshape(mixed.shape[0], -1)


def attend_kernel(scalars, packed, rows, out, scores, *, step, width):
    place = pl.program_id(0)
    coef = scalars[0]
    query = packed[pl.ds(place * step, step), 0:width]
    queries = [query * rows[which : which + 1, :].astype(jnp.bfloat16) for which in range(2)]
    outputs = []

    def fold(values, combine):
        parts = [values[:, at * width : (at + 1) * width] for at in range(step // width)]
        while len(parts) > 1:
            parts = [combine(*parts[at : at + 2]) for at in range(0, len(parts), 2)]
        return parts[0]

    def raw(which, index):
        keys = packed[pl.ds(index * step, step), width : 2 * width]
        return lax.dot_general(
            queries[which], keys, (((1,), (1,)), ((), ())), preferred_element_type=jnp.float32
        )

    row = lax.broadcasted_iota(jnp.int32, (step, step), 0)
    column = lax.broadcasted_iota(jnp.int32, (step, step), 1)
    allowed = column <= row
    highest = []
    for which in range(2):
        own = jnp.where(allowed, raw(which, place), NEG)
        scores[which, place] = own
        highest.append(fold(own, jnp.maximum))

    def first_pass(index, carry):
        found = []
        for which in range(2):
            block = raw(which, index)
            scores[which, index] = block
            found.append(jnp.maximum(carry[which], fold(block, jnp.maximum)))
        return tuple(found)

    highest = lax.fori_loop(0, place, first_pass, tuple(highest))
    tops = [jnp.max(found, axis=1, keepdims=True) * coef for found in highest]

    def second_pass(index, carry):
        values = packed[pl.ds(index * step, step), 2 * width : 3 * width]
        found = []
        for which in range(2):
            total, mixed = carry[which]
            weights = jnp.exp2(scores[which, index] * coef - tops[which])
            total = total + fold(weights, jnp.add)
            mixed = mixed + jnp.dot(
                weights.astype(jnp.bfloat16), values, preferred_element_type=jnp.float32
            )
            found.append((total, mixed))
        return tuple(found)

    empty = jnp.zeros((step, width), jnp.float32)
    found = lax.fori_loop(0, place + 1, second_pass, ((empty, empty), (empty, empty)))
    outputs = [mixed / jnp.sum(total, axis=1, keepdims=True) for total, mixed in found]
    mixed = outputs[0] - scalars[1] * outputs[1]
    square = jnp.sum(mixed * mixed, axis=1, keepdims=True) * scalars[2]
    out[0] = (mixed * lax.rsqrt(square + EPS) * rows[2:3, :]).astype(jnp.bfloat16)


def widen(values, width):
    missing = width - values.shape[-1]
    return jnp.pad(values, [(0, 0)] * (values.ndim - 1) + [(0, missing)]) if missing else values


def exchanged_attention(query_a, key_a, value_a, query_b, key_b, value_b, mix_a, mix_b, head_gain_a, head_gain_b):
    seq_rows, heads_a, _ = query_a.shape
    ways = lax.axis_size("sp")
    place = lax.axis_index("sp")
    groups = ((query_a, key_a, value_a), (query_b, key_b, value_b))
    widest = max(array.shape[2] for group in groups for array in group)
    width = -(-widest // 128) * 128
    outgoing = jnp.concatenate(
        [
            jnp.concatenate([jnp.transpose(widen(array, width), (1, 0, 2)) for array in group], axis=2)
            for group in groups
        ],
        axis=0,
    )
    arrived = lax.all_to_all(outgoing, "sp", split_axis=0, concat_axis=0, tiled=True)
    packed = arrived.reshape(ways * seq_rows, 3 * width)
    first = place < heads_a
    maps = jnp.where(first, query_a.shape[2] // 2, query_b.shape[2] // 2)
    lanes = jnp.arange(width, dtype=jnp.int32)
    gain = jnp.where(first, widen(head_gain_a, width), widen(head_gain_b, width)) * HEAD_SCALE
    rows = jnp.stack(
        [(lanes < maps).astype(jnp.float32), ((lanes >= maps) & (lanes < 2 * maps)).astype(jnp.float32), gain]
    )
    coef_a, coef_b = [math.log2(math.e) / math.sqrt(group[0].shape[2] // 2) for group in groups]
    scalars = jnp.stack(
        [
            jnp.where(first, coef_a, coef_b).astype(jnp.float32),
            lax.dynamic_index_in_dim(jnp.concatenate([mix_a, mix_b]), place, 0, False),
            jnp.where(first, 1.0 / value_a.shape[2], 1.0 / value_b.shape[2]).astype(jnp.float32),
        ]
    )
    mixed = pl.pallas_call(
        lambda *refs: attend_kernel(*refs, step=seq_rows, width=width),
        grid=(ways,),
        in_specs=[
            pl.BlockSpec(memory_space=pltpu.SMEM),
            pl.BlockSpec(packed.shape, lambda index: (0, 0)),
            pl.BlockSpec(rows.shape, lambda index: (0, 0)),
        ],
        out_specs=pl.BlockSpec((1, seq_rows, width), lambda index: (index, 0, 0)),
        out_shape=jax.ShapeDtypeStruct((ways, seq_rows, width), jnp.bfloat16),
        scratch_shapes=[pltpu.VMEM((2, ways, seq_rows, seq_rows), jnp.float32)],
        compiler_params=pltpu.CompilerParams(dimension_semantics=("arbitrary",)),
        name="attend",
    )(scalars, packed, rows)
    return lax.all_to_all(mixed, "sp", split_axis=0, concat_axis=0, tiled=True)


def widened_rows(proj, heads, width):
    per_head = proj.reshape(heads, -1, proj.shape[1])
    return jnp.pad(per_head, ((0, 0), (0, width - per_head.shape[1]), (0, 0)))


def gathered_attention(query_a, key_a, value_a, query_b, key_b, value_b, mix_a, mix_b, head_gain_a, head_gain_b):
    seq_rows = query_a.shape[0]
    sp_ways = lax.axis_size("sp")
    place = lax.axis_index("sp")
    positions = place * seq_rows + jnp.arange(seq_rows, dtype=jnp.int32)
    levels = sp_ways.bit_length() - 1
    half = seq_rows // 2
    moved = jnp.concatenate(
        [query_a[half:].reshape(half, -1), query_b[half:].reshape(half, -1)], axis=1
    )
    for bit in range(levels):
        moved = partner(moved, "sp", bit)
    split_at = query_a.shape[1] * query_a.shape[2]
    far_a = moved[:, :split_at].reshape(half, query_a.shape[1], query_a.shape[2])
    far_b = moved[:, split_at:].reshape(half, query_b.shape[1], query_b.shape[2])
    far_pos = (sp_ways - 1 - place) * seq_rows + half + jnp.arange(half, dtype=jnp.int32)
    query_sets = ((query_a[:half], query_b[:half], positions[:half]), (far_a, far_b, far_pos))

    def fold_keys(carry, pieces):
        return tuple(
            (set_update(states, queries, pieces) for states, queries in zip(carry, query_sets))
        )

    initial = tuple(
        (
            (empty_group(queries[0], value_a), empty_group(queries[1], value_b))
            for queries in query_sets
        )
    )
    results = fold_keys(
        initial,
        (
            lax.all_gather(key_a, "sp", axis=0, tiled=True),
            lax.all_gather(value_a, "sp", axis=0, tiled=True),
            lax.all_gather(key_b, "sp", axis=0, tiled=True),
            lax.all_gather(value_b, "sp", axis=0, tiled=True),
        ),
    )
    finished = [
        (finish_group(states[0], mix_a, head_gain_a), finish_group(states[1], mix_b, head_gain_b))
        for states in results
    ]
    returned = jnp.concatenate([finished[1][0], finished[1][1]], axis=1)
    for bit in range(levels):
        returned = partner(returned, "sp", bit)
    width_a = finished[0][0].shape[1]
    heads_out_a = jnp.concatenate([finished[0][0], returned[:, :width_a]], axis=0)
    heads_out_b = jnp.concatenate([finished[0][1], returned[:, width_a:]], axis=0)
    return heads_out_a, heads_out_b


def per_device(
    resid,
    query_a,
    key_a,
    value_a,
    query_b,
    key_b,
    value_b,
    mix_a,
    mix_b,
    head_gain_a,
    head_gain_b,
    proj_a,
    proj_b,
    norm_gain,
    route_ids,
    route_weights,
    expert_gate,
    expert_up,
    expert_down,
):
    sp_ways = lax.axis_size("sp")
    attended = (query_a, key_a, value_a, query_b, key_b, value_b, mix_a, mix_b, head_gain_a, head_gain_b)
    if query_a.shape[1] + query_b.shape[1] == sp_ways:
        heads_out = exchanged_attention(*attended)
        head_width = heads_out.shape[2]
        left = jnp.transpose(heads_out, (1, 0, 2)).reshape(heads_out.shape[1], -1)
        right = jnp.concatenate(
            [
                widened_rows(proj_a, query_a.shape[1], head_width),
                widened_rows(proj_b, query_b.shape[1], head_width),
            ]
        ).reshape(left.shape[1], -1)
        term = jnp.dot(left, right, preferred_element_type=jnp.float32)
    else:
        heads_out_a, heads_out_b = gathered_attention(*attended)
        term = jnp.dot(heads_out_a, proj_a, preferred_element_type=jnp.float32)
        term = term + jnp.dot(heads_out_b, proj_b, preferred_element_type=jnp.float32)
    width = resid.shape[1]
    tok_rows = resid.shape[0]
    top_count = route_ids.shape[1]
    capacity = 3 * top_count * tok_rows // (2 * sp_ways)
    own_slots = slot_numbers(route_ids, sp_ways, capacity)
    mixed = resid.astype(jnp.float32) + lax.psum_scatter(
        lax.optimization_barrier(term.astype(jnp.bfloat16))
        .astype(jnp.float32)
        .astype(jnp.bfloat16),
        "tp",
        scatter_dimension=0,
        tiled=True,
    ).astype(jnp.float32)
    normed = rms_scaled(mixed, norm_gain).astype(jnp.bfloat16)
    lookup = jnp.arange(sp_ways * capacity, dtype=jnp.int32)[:, None]
    spread = jnp.zeros((sp_ways * capacity, tok_rows), jnp.float32)
    for which in range(top_count):
        spread = spread + (own_slots[:, which][None, :] == lookup).astype(jnp.float32)
    outgoing = jnp.dot(
        spread.astype(jnp.bfloat16), normed, preferred_element_type=jnp.float32
    ).astype(jnp.bfloat16)
    arrived = lax.all_to_all(
        outgoing.reshape(sp_ways, capacity, width), "sp", split_axis=0, concat_axis=0, tiled=True
    )
    piece = lax.all_gather(arrived.reshape(sp_ways * capacity, width), "tp", axis=0, tiled=True)
    gate = jnp.dot(piece, expert_gate[0], preferred_element_type=jnp.float32)
    upward = jnp.dot(piece, expert_up[0], preferred_element_type=jnp.float32)
    hidden = (jax.nn.silu(gate) * upward).astype(jnp.bfloat16)
    term = jnp.dot(hidden, expert_down[0], preferred_element_type=jnp.float32)
    summed = lax.psum_scatter(
        lax.optimization_barrier(term.astype(jnp.bfloat16))
        .astype(jnp.float32)
        .astype(jnp.bfloat16),
        "tp",
        scatter_dimension=0,
        tiled=True,
    )
    finished_rows = summed.reshape(sp_ways, capacity, width)
    back = lax.all_to_all(finished_rows, "sp", split_axis=0, concat_axis=0, tiled=True)
    picked = jnp.take(back.reshape(sp_ways * capacity, width), own_slots.reshape(-1), axis=0)
    picked = picked.reshape(tok_rows, top_count, width)
    output = mixed + jnp.sum(route_weights[:, :, None] * picked.astype(jnp.float32), axis=1)
    return output.astype(jnp.bfloat16)


def solution(mesh):
    placed = (
        P(("sp", "tp"), None),
        P("sp", "tp", None),
        P("sp", "tp", None),
        P("sp", "tp", None),
        P("sp", "tp", None),
        P("sp", "tp", None),
        P("sp", "tp", None),
        P("tp"),
        P("tp"),
        P(),
        P(),
        P("tp", None),
        P("tp", None),
        P(),
        P(("sp", "tp"), None),
        P(("sp", "tp"), None),
        P("sp", None, "tp"),
        P("sp", None, "tp"),
        P("sp", "tp", None),
    )
    return jax.shard_map(
        per_device, mesh=mesh, in_specs=placed, out_specs=P(("sp", "tp"), None), check_vma=False
    )
```

```python
import math

import jax
import jax.numpy as jnp
from jax import lax
from jax.experimental import pallas as pl
from jax.experimental.pallas import tpu as pltpu
from jax.sharding import Mesh, PartitionSpec as P

EPS = 1e-06
NEG = -1e30
HEAD_SCALE = 1.0 - (0.8 - 0.6 * math.exp(-0.3))
KEY_STEP = 512


def partner(value, axis, apart):
    return lax.ppermute(value, axis, [(i, i ^ 1 << apart) for i in range(lax.axis_size(axis))])


def rms_scaled(values, gain):
    return values * lax.rsqrt(jnp.mean(values * values, axis=-1, keepdims=True) + EPS) * gain


def slot_numbers(route_rows, experts, capacity):
    count, top_count = route_rows.shape
    flat = route_rows.reshape(count * top_count)
    onehot = (flat[:, None] == jnp.arange(experts, dtype=jnp.int32)[None, :]).astype(jnp.int32)
    ranks = jnp.sum((jnp.cumsum(onehot, axis=0) - onehot) * onehot, axis=1)
    return (flat * capacity + ranks).reshape(count, top_count)


def empty_map(count, heads, width):
    return (
        jnp.zeros((count, heads, width), jnp.float32),
        jnp.full((heads, count), NEG, jnp.float32),
        jnp.zeros((heads, count), jnp.float32),
    )


def empty_group(query, value):
    return (
        empty_map(query.shape[0], query.shape[1], value.shape[2]),
        empty_map(query.shape[0], query.shape[1], value.shape[2]),
    )


def map_update(state, query, keys, values, allowed, scale):
    weighted, maximum, sums = state
    scores = jnp.einsum("qhd,khd->hqk", query, keys, preferred_element_type=jnp.float32) * scale
    scores = jnp.where(allowed[None], scores, NEG)
    fresh = jnp.maximum(maximum, jnp.max(scores, axis=2))
    weights = jnp.where(allowed[None], jnp.exp(scores - fresh[:, :, None]), 0.0)
    factor = jnp.exp(maximum - fresh)
    sums = sums * factor + jnp.sum(weights, axis=2)
    added = jnp.einsum(
        "hqk,khv->qhv", weights.astype(jnp.bfloat16), values, preferred_element_type=jnp.float32
    )
    weighted = weighted * jnp.transpose(factor)[:, :, None] + added
    return (weighted, fresh, sums)


def group_update(states, query, keys, values, allowed):
    width = query.shape[2] // 2
    scale = 1.0 / math.sqrt(width)
    return tuple(
        (
            map_update(
                states[which],
                query[:, :, which * width : (which + 1) * width],
                keys[:, :, which * width : (which + 1) * width],
                values,
                allowed,
                scale,
            )
            for which in range(2)
        )
    )


def set_update(carry, queries, pieces):
    rows_a, rows_b, query_pos = queries
    piece_key_a, piece_value_a, piece_key_b, piece_value_b = pieces
    length = piece_key_a.shape[0]
    step = math.gcd(length, KEY_STEP)
    latest = query_pos[-1]

    def inner(index, states):
        first = index * step

        def compute(current):
            keys_a = lax.dynamic_slice_in_dim(piece_key_a, first, step, 0)
            values_a = lax.dynamic_slice_in_dim(piece_value_a, first, step, 0)
            keys_b = lax.dynamic_slice_in_dim(piece_key_b, first, step, 0)
            values_b = lax.dynamic_slice_in_dim(piece_value_b, first, step, 0)
            key_pos = first + jnp.arange(step, dtype=jnp.int32)
            allowed = key_pos[None, :] <= query_pos[:, None]
            return (
                group_update(current[0], rows_a, keys_a, values_a, allowed),
                group_update(current[1], rows_b, keys_b, values_b, allowed),
            )

        return lax.cond(first <= latest, compute, lambda current: current, states)

    return lax.fori_loop(0, length // step, inner, carry)


def finish_group(states, mix, gain):
    outputs = [state[0] / jnp.transpose(state[2])[:, :, None] for state in states]
    mixed = outputs[0] - mix[None, :, None] * outputs[1]
    normed = rms_scaled(mixed, gain) * HEAD_SCALE
    return normed.astype(jnp.bfloat16).reshape(mixed.shape[0], -1)


def gathered_device(
    resid,
    query_a,
    key_a,
    value_a,
    query_b,
    key_b,
    value_b,
    mix_a,
    mix_b,
    head_gain_a,
    head_gain_b,
    proj_a,
    proj_b,
    norm_gain,
    route_ids,
    route_weights,
    expert_gate,
    expert_up,
    expert_down,
):
    seq_rows = query_a.shape[0]
    sp_ways = lax.axis_size("sp")
    place = lax.axis_index("sp")
    positions = place * seq_rows + jnp.arange(seq_rows, dtype=jnp.int32)
    levels = sp_ways.bit_length() - 1
    half = seq_rows // 2
    moved = jnp.concatenate(
        [query_a[half:].reshape(half, -1), query_b[half:].reshape(half, -1)], axis=1
    )
    for bit in range(levels):
        moved = partner(moved, "sp", bit)
    split_at = query_a.shape[1] * query_a.shape[2]
    far_a = moved[:, :split_at].reshape(half, query_a.shape[1], query_a.shape[2])
    far_b = moved[:, split_at:].reshape(half, query_b.shape[1], query_b.shape[2])
    far_pos = (sp_ways - 1 - place) * seq_rows + half + jnp.arange(half, dtype=jnp.int32)
    query_sets = ((query_a[:half], query_b[:half], positions[:half]), (far_a, far_b, far_pos))

    def fold_keys(carry, pieces):
        return tuple(
            (set_update(states, queries, pieces) for states, queries in zip(carry, query_sets))
        )

    initial = tuple(
        (
            (empty_group(queries[0], value_a), empty_group(queries[1], value_b))
            for queries in query_sets
        )
    )
    results = fold_keys(
        initial,
        (
            lax.all_gather(key_a, "sp", axis=0, tiled=True),
            lax.all_gather(value_a, "sp", axis=0, tiled=True),
            lax.all_gather(key_b, "sp", axis=0, tiled=True),
            lax.all_gather(value_b, "sp", axis=0, tiled=True),
        ),
    )
    finished = [
        (finish_group(states[0], mix_a, head_gain_a), finish_group(states[1], mix_b, head_gain_b))
        for states in results
    ]
    returned = jnp.concatenate([finished[1][0], finished[1][1]], axis=1)
    for bit in range(levels):
        returned = partner(returned, "sp", bit)
    width_a = finished[0][0].shape[1]
    heads_out_a = jnp.concatenate([finished[0][0], returned[:, :width_a]], axis=0)
    heads_out_b = jnp.concatenate([finished[0][1], returned[:, width_a:]], axis=0)
    width = resid.shape[1]
    tok_rows = resid.shape[0]
    top_count = route_ids.shape[1]
    capacity = 3 * top_count * tok_rows // (2 * sp_ways)
    own_slots = slot_numbers(route_ids, sp_ways, capacity)
    term = jnp.dot(heads_out_a, proj_a, preferred_element_type=jnp.float32)
    term = term + jnp.dot(heads_out_b, proj_b, preferred_element_type=jnp.float32)
    mixed = resid.astype(jnp.float32) + lax.psum_scatter(
        lax.optimization_barrier(term.astype(jnp.bfloat16))
        .astype(jnp.float32)
        .astype(jnp.bfloat16),
        "tp",
        scatter_dimension=0,
        tiled=True,
    ).astype(jnp.float32)
    normed = rms_scaled(mixed, norm_gain).astype(jnp.bfloat16)
    lookup = jnp.arange(sp_ways * capacity, dtype=jnp.int32)[:, None]
    spread = jnp.zeros((sp_ways * capacity, tok_rows), jnp.float32)
    for which in range(top_count):
        spread = spread + (own_slots[:, which][None, :] == lookup).astype(jnp.float32)
    outgoing = jnp.dot(
        spread.astype(jnp.bfloat16), normed, preferred_element_type=jnp.float32
    ).astype(jnp.bfloat16)
    arrived = lax.all_to_all(
        outgoing.reshape(sp_ways, capacity, width), "sp", split_axis=0, concat_axis=0, tiled=True
    )
    piece = lax.all_gather(arrived.reshape(sp_ways * capacity, width), "tp", axis=0, tiled=True)
    gate = jnp.dot(piece, expert_gate[0], preferred_element_type=jnp.float32)
    upward = jnp.dot(piece, expert_up[0], preferred_element_type=jnp.float32)
    hidden = (jax.nn.silu(gate) * upward).astype(jnp.bfloat16)
    term = jnp.dot(hidden, expert_down[0], preferred_element_type=jnp.float32)
    summed = lax.psum_scatter(
        lax.optimization_barrier(term.astype(jnp.bfloat16))
        .astype(jnp.float32)
        .astype(jnp.bfloat16),
        "tp",
        scatter_dimension=0,
        tiled=True,
    )
    finished_rows = summed.reshape(sp_ways, capacity, width)
    back = lax.all_to_all(finished_rows, "sp", split_axis=0, concat_axis=0, tiled=True)
    picked = jnp.take(back.reshape(sp_ways * capacity, width), own_slots.reshape(-1), axis=0)
    picked = picked.reshape(tok_rows, top_count, width)
    output = mixed + jnp.sum(route_weights[:, :, None] * picked.astype(jnp.float32), axis=1)
    return output.astype(jnp.bfloat16)


def attend_kernel(scalars, packed, rows, out, scores, *, step, width, block):
    place = pl.program_id(0)
    coef = scalars[0]
    query = packed[pl.ds(place * step, step), 0:width]
    queries = [query * rows[which : which + 1, :].astype(jnp.bfloat16) for which in range(2)]
    outputs = []

    def fold(values, combine):
        parts = [values[:, at * width : (at + 1) * width] for at in range(step // width)]
        while len(parts) > 1:
            parts = [combine(*parts[at : at + 2]) for at in range(0, len(parts), 2)]
        return parts[0]

    def raw(which, index):
        keys = packed[pl.ds(index * step, step), width : 2 * width]
        return lax.dot_general(
            queries[which], keys, (((1,), (1,)), ((), ())), preferred_element_type=jnp.float32
        )

    row = lax.broadcasted_iota(jnp.int32, (step, step), 0)
    column = lax.broadcasted_iota(jnp.int32, (step, step), 1)
    allowed = column <= row
    highest = []
    for which in range(2):
        own = jnp.where(allowed, raw(which, place), NEG)
        scores[which, place] = own
        highest.append(fold(own, jnp.maximum))

    def first_pass(index, carry):
        found = []
        for which in range(2):
            block = raw(which, index)
            scores[which, index] = block
            found.append(jnp.maximum(carry[which], fold(block, jnp.maximum)))
        return tuple(found)

    highest = lax.fori_loop(0, place, first_pass, tuple(highest))
    tops = [jnp.max(found, axis=1, keepdims=True) * coef for found in highest]

    def second_pass(index, carry):
        values = packed[pl.ds(index * step, step), 2 * width : 3 * width]
        found = []
        for which in range(2):
            total, mixed = carry[which]
            weights = jnp.exp2(scores[which, index] * coef - tops[which])
            total = total + fold(weights, jnp.add)
            mixed = mixed + jnp.dot(
                weights.astype(jnp.bfloat16), values, preferred_element_type=jnp.float32
            )
            found.append((total, mixed))
        return tuple(found)

    empty = jnp.zeros((step, width), jnp.float32)
    found = lax.fori_loop(0, place + 1, second_pass, ((empty, empty), (empty, empty)))
    outputs = [mixed / jnp.sum(total, axis=1, keepdims=True) for total, mixed in found]
    mixed = outputs[0] - scalars[1] * outputs[1]
    square = jnp.sum(mixed * mixed, axis=1, keepdims=True) * scalars[2]
    normed = (mixed * lax.rsqrt(square + EPS) * rows[2:3, :]).astype(jnp.bfloat16)
    cores = out.shape[1]
    for at in range(step // block):
        first = at // cores * block
        out[0, at % cores, first : first + block] = normed[at * block : (at + 1) * block]


def widen(values, width):
    missing = width - values.shape[-1]
    return jnp.pad(values, [(0, 0)] * (values.ndim - 1) + [(0, missing)]) if missing else values


def mirrored(value, axis, apart):
    return lax.ppermute(value, axis, [(i, i ^ apart) for i in range(lax.axis_size(axis))])


def whole_call(body, outs, name, *operands, scalars=0):
    vmem = pl.BlockSpec(memory_space=pltpu.VMEM)
    smem = pl.BlockSpec(memory_space=pltpu.SMEM)
    return pl.pallas_call(
        body,
        in_specs=[smem] * scalars + [vmem] * (len(operands) - scalars),
        out_specs=[vmem] * len(outs),
        out_shape=[jax.ShapeDtypeStruct(shape, dtype) for shape, dtype in outs],
        name=name,
    )(*operands)


def exchanged_heads(query_a, key_a, value_a, query_b, key_b, value_b, mix_a, mix_b, head_gain_a, head_gain_b, block):
    seq_rows, heads_a, _ = query_a.shape
    ways = lax.axis_size("sp")
    cores = lax.axis_size("c")
    place = lax.axis_index("sp")
    groups = ((query_a, key_a, value_a), (query_b, key_b, value_b))
    widest = max(array.shape[2] for group in groups for array in group)
    width = -(-widest // 128) * 128
    outgoing = jnp.concatenate(
        [
            jnp.concatenate([jnp.transpose(widen(array, width), (1, 0, 2)) for array in group], axis=2)
            for group in groups
        ],
        axis=0,
    )
    arrived = lax.all_to_all(outgoing, "sp", split_axis=0, concat_axis=0, tiled=True)
    packed = arrived.reshape(ways * seq_rows, 3 * width)
    first = place < heads_a
    maps = jnp.where(first, query_a.shape[2] // 2, query_b.shape[2] // 2)
    lanes = jnp.arange(width, dtype=jnp.int32)
    gain = jnp.where(first, widen(head_gain_a, width), widen(head_gain_b, width)) * HEAD_SCALE
    rows = jnp.stack(
        [(lanes < maps).astype(jnp.float32), ((lanes >= maps) & (lanes < 2 * maps)).astype(jnp.float32), gain]
    )
    coef_a, coef_b = [math.log2(math.e) / math.sqrt(group[0].shape[2] // 2) for group in groups]
    scalars = jnp.stack(
        [
            jnp.where(first, coef_a, coef_b).astype(jnp.float32),
            lax.dynamic_index_in_dim(jnp.concatenate([mix_a, mix_b]), place, 0, False),
            jnp.where(first, 1.0 / value_a.shape[2], 1.0 / value_b.shape[2]).astype(jnp.float32),
        ]
    )
    shape = (ways, cores, seq_rows // cores, width)
    mixed = pl.pallas_call(
        lambda *refs: attend_kernel(*refs, step=seq_rows, width=width, block=block),
        grid=(ways,),
        in_specs=[
            pl.BlockSpec(memory_space=pltpu.SMEM),
            pl.BlockSpec(packed.shape, lambda index: (0, 0)),
            pl.BlockSpec(rows.shape, lambda index: (0, 0)),
        ],
        out_specs=pl.BlockSpec((1,) + shape[1:], lambda index: (index, 0, 0, 0)),
        out_shape=jax.ShapeDtypeStruct(shape, jnp.bfloat16),
        scratch_shapes=[pltpu.VMEM((2, ways, seq_rows, seq_rows), jnp.float32)],
        compiler_params=pltpu.CompilerParams(dimension_semantics=("arbitrary",)),
        name="attend",
    )(scalars, packed, rows)
    flat = mixed.reshape((ways * cores,) + shape[2:])
    return lax.all_to_all(flat, ("sp", "c"), split_axis=0, concat_axis=0, tiled=True).reshape(shape)


def project(heads, proj_a, proj_b, lines, block, heads_a):
    ways, cores, rows, width = heads.shape
    model = proj_a.shape[1]
    weights = []
    for apart in range(cores):
        weights += [proj_a, proj_b] if apart == 0 else [mirrored(proj_a, "c", apart), mirrored(proj_b, "c", apart)]
    where = jnp.stack([lax.axis_index("c"), lax.axis_index("z")]).astype(jnp.int32)
    step = model // 4
    narrow = proj_b.shape[0] // (ways - heads_a)
    wide = proj_a.shape[0] // heads_a

    def body(at, heads_ref, *refs):
        sets, outs = refs[: 2 * cores], refs[2 * cores :]
        total = None
        for apart in range(cores):
            core = at[0] ^ apart

            def taken(head, used):
                found = [heads_ref[head, core, pl.ds((at[1] ^ far) * block, block), :] for far in range(lines)]
                return jnp.concatenate(found, axis=0)[:, :used]

            left_a = jnp.concatenate([taken(head, wide) for head in range(heads_a)], axis=1)
            left_b = jnp.concatenate([taken(head, narrow) for head in range(heads_a, ways)], axis=1)
            for left, right in ((left_a, sets[2 * apart]), (left_b, sets[2 * apart + 1])):
                piece = jnp.dot(left, right[...], preferred_element_type=jnp.float32)
                total = piece if total is None else total + piece
        for far in range(lines):
            outs[far][...] = total[far * block : (far + 1) * block].astype(jnp.bfloat16)

    return pl.pallas_call(
        body,
        grid=(model // step,),
        in_specs=[pl.BlockSpec(memory_space=pltpu.SMEM), pl.BlockSpec(heads.shape, lambda index: (0, 0, 0, 0))]
        + [pl.BlockSpec((array.shape[0], step), lambda index: (0, index)) for array in weights],
        out_specs=[pl.BlockSpec((block, step), lambda index: (0, index))] * lines,
        out_shape=[jax.ShapeDtypeStruct((block, model), jnp.bfloat16)] * lines,
        name="project",
    )(where, heads, *weights)


def run_experts(rows, gate_w, up_w, down_w):
    count, model = rows.shape
    hidden = gate_w.shape[1]
    tile = math.gcd(hidden, 256)
    out_tile = math.gcd(model, 512)
    tiles = hidden // tile

    def body(rows_ref, gate_ref, up_ref, down_ref, out_ref, held):
        index = pl.program_id(0)

        @pl.when(index < tiles)
        def _():
            gate = jnp.dot(rows_ref[...], gate_ref[...], preferred_element_type=jnp.float32)
            upward = jnp.dot(rows_ref[...], up_ref[...], preferred_element_type=jnp.float32)
            held[index] = (jax.nn.silu(gate) * upward).astype(jnp.bfloat16)

        @pl.when(index >= tiles)
        def _():
            total = jnp.dot(held[0], down_ref[0:tile, :], preferred_element_type=jnp.float32)
            for at in range(1, tiles):
                total = total + jnp.dot(
                    held[at], down_ref[at * tile : (at + 1) * tile, :], preferred_element_type=jnp.float32
                )
            out_ref[...] = total.astype(jnp.bfloat16)

    early = lambda index: (0, jnp.minimum(index, tiles - 1))
    late = lambda index: (0, jnp.maximum(index - tiles, 0))
    return pl.pallas_call(
        body,
        grid=(tiles + model // out_tile,),
        in_specs=[
            pl.BlockSpec((count, model), lambda index: (0, 0)),
            pl.BlockSpec((model, tile), early),
            pl.BlockSpec((model, tile), early),
            pl.BlockSpec((hidden, out_tile), late),
        ],
        out_specs=pl.BlockSpec((count, out_tile), late),
        out_shape=jax.ShapeDtypeStruct((count, model), jnp.bfloat16),
        scratch_shapes=[pltpu.VMEM((tiles, count, tile), jnp.bfloat16)],
        compiler_params=pltpu.CompilerParams(dimension_semantics=("arbitrary",)),
        name="experts",
    )(rows, gate_w, up_w, down_w)


def exchanged_device(
    resid,
    query_a,
    key_a,
    value_a,
    query_b,
    key_b,
    value_b,
    mix_a,
    mix_b,
    head_gain_a,
    head_gain_b,
    proj_a,
    proj_b,
    norm_gain,
    route_ids,
    route_weights,
    expert_gate,
    expert_up,
    expert_down,
):
    ways, lines, cores = (lax.axis_size(axis) for axis in ("sp", "z", "c"))
    place = lax.axis_index("sp")
    tok_rows, width = resid.shape
    top_count = route_ids.shape[1]
    capacity = 3 * top_count * tok_rows // (2 * ways)
    slots_all = ways * capacity
    low = jnp.bfloat16
    head_cols = width * 5 // 16 // 128 * 128
    tail_cols = width - head_cols

    heads = exchanged_heads(
        query_a, key_a, value_a, query_b, key_b, value_b, mix_a, mix_b, head_gain_a, head_gain_b, tok_rows
    )

    slots = slot_numbers(route_ids ^ place, ways, capacity)
    routes = jnp.concatenate([slots.astype(jnp.float32), route_weights], axis=1)
    line_routes = [routes] + [mirrored(routes, "z", far) for far in range(1, lines)]
    lookup = jnp.arange(slots_all, dtype=jnp.int32)
    spreads, blends = [], []
    for found in line_routes:
        hits = [found[:, which].astype(jnp.int32)[:, None] == lookup[None, :] for which in range(top_count)]
        spread = sum(hit.astype(jnp.float32) for hit in hits)
        blend = sum(
            jnp.where(hits[which], found[:, top_count + which][:, None], 0.0) for which in range(top_count)
        )
        upper = blend.astype(low)
        spreads.append(jnp.transpose(spread).astype(low))
        blends += [upper, (blend - upper.astype(jnp.float32)).astype(low)]
    spreads = jnp.stack(spreads)
    blends = jnp.stack(blends).reshape(lines, 2, tok_rows, slots_all)

    parts = project(heads, proj_a, proj_b, lines, tok_rows, query_a.shape[1])
    parts = [parts[0]] + [mirrored(parts[far], "z", far) for far in range(1, lines)]

    def norm_body(*refs):
        part_refs, (resid_ref, gain_ref, spread_ref), outs = refs[:lines], refs[lines : lines + 3], refs[lines + 3 :]
        mixed = resid_ref[...].astype(jnp.float32)
        for part in part_refs:
            mixed = mixed + part[...].astype(jnp.float32)
        outs[0][...] = mixed
        normed = rms_scaled(mixed, gain_ref[...]).astype(low)
        outs[1][...] = normed[:, head_cols:]
        picked = jnp.dot(spread_ref[0], normed[:, :head_cols], preferred_element_type=jnp.float32).astype(low)
        for far in range(ways):
            outs[2 + far][...] = picked[far * capacity : (far + 1) * capacity]

    mixed, tail, *heads_out = whole_call(
        norm_body,
        [((tok_rows, width), jnp.float32), ((tok_rows, tail_cols), low)] + [((capacity, head_cols), low)] * ways,
        "norm",
        *parts,
        resid,
        norm_gain[None, :],
        spreads,
    )
    tails = [tail] + [mirrored(tail, "z", far) for far in range(1, lines)]
    head_own = jnp.concatenate(
        [heads_out[0]] + [mirrored(heads_out[far], "sp", far) for far in range(1, ways)], axis=0
    )
    head_blocks = [head_own] + [mirrored(head_own, "z", far) for far in range(1, lines)]

    def spread_body(*refs):
        tail_refs, spread_ref, outs = refs[:lines], refs[lines], refs[lines + 1 :]
        for line in range(lines):
            picked = jnp.dot(spread_ref[line], tail_refs[line][...], preferred_element_type=jnp.float32).astype(low)
            for far in range(ways):
                outs[far][line * capacity : (line + 1) * capacity] = picked[far * capacity : (far + 1) * capacity]

    tails_out = whole_call(
        spread_body, [((lines * capacity, tail_cols), low)] * ways, "spread", *tails, spreads
    )
    tail_blocks = [tails_out[0]] + [mirrored(tails_out[far], "sp", far) for far in range(1, ways)]

    def join_body(*refs):
        head_refs, tail_refs, (out,) = refs[:lines], refs[lines : lines + ways], refs[lines + ways :]
        for line in range(lines):
            for far in range(ways):
                first = line * slots_all + far * capacity
                out[first : first + capacity, :head_cols] = head_refs[line][far * capacity : (far + 1) * capacity]
                out[first : first + capacity, head_cols:] = tail_refs[far][line * capacity : (line + 1) * capacity]

    (rows,) = whole_call(join_body, [((lines * slots_all, width), low)], "join", *head_blocks, *tail_blocks)
    weights = (expert_gate[0], expert_up[0], expert_down[0])
    own_part = run_experts(rows, *weights)
    core_parts = [mirrored(run_experts(mirrored(rows, "c", apart), *weights), "c", apart) for apart in range(1, cores)]

    def pair_body(*refs):
        part_refs, outs = refs[:cores], refs[cores:]
        for line in range(lines):
            for far in range(ways):
                first = line * slots_all + far * capacity
                total = part_refs[0][first : first + capacity].astype(jnp.float32)
                for part in part_refs[1:]:
                    total = total + part[first : first + capacity].astype(jnp.float32)
                total = total.astype(low)
                outs[line][far * capacity : (far + 1) * capacity] = total[:, :head_cols]
                outs[lines + far][line * capacity : (line + 1) * capacity] = total[:, head_cols:]

    back = whole_call(
        pair_body,
        [((slots_all, head_cols), low)] * lines + [((lines * capacity, tail_cols), low)] * ways,
        "pair",
        own_part,
        *core_parts,
    )
    tail_back = [back[lines]] + [mirrored(back[lines + far], "sp", far) for far in range(1, ways)]
    head_back = [back[0]] + [mirrored(back[far], "z", far) for far in range(1, lines)]

    def blend_body(*refs):
        tail_refs, blend_ref, outs = refs[:ways], refs[ways], refs[ways + 1 :]
        for line in range(lines):
            block = jnp.concatenate([ref[line * capacity : (line + 1) * capacity] for ref in tail_refs], axis=0)
            total = jnp.dot(blend_ref[line, 0], block, preferred_element_type=jnp.float32)
            total = total + jnp.dot(blend_ref[line, 1], block, preferred_element_type=jnp.float32)
            outs[line][...] = total.astype(low)

    tail_sums = whole_call(blend_body, [((tok_rows, tail_cols), low)] * lines, "blend", *tail_back, blends)
    tail_sums = [tail_sums[0]] + [mirrored(tail_sums[far], "z", far) for far in range(1, lines)]

    def total_body(*refs):
        part_refs, outs = refs[:lines], refs[lines:]
        total = sum(part[...].astype(jnp.float32) for part in part_refs).astype(low)
        for far in range(ways):
            outs[far][...] = total[far * capacity : (far + 1) * capacity]

    head_sums = whole_call(total_body, [((capacity, head_cols), low)] * ways, "total", *head_back)
    head_sums = [head_sums[0]] + [mirrored(head_sums[far], "sp", far) for far in range(1, ways)]

    def final_body(mixed_ref, blend_ref, *refs):
        head_refs, tail_refs, (out,) = refs[:ways], refs[ways : ways + lines], refs[ways + lines :]
        block = jnp.concatenate([ref[...] for ref in head_refs], axis=0)
        total = mixed_ref[:, :head_cols] + jnp.dot(blend_ref[0, 0], block, preferred_element_type=jnp.float32)
        total = total + jnp.dot(blend_ref[0, 1], block, preferred_element_type=jnp.float32)
        out[:, :head_cols] = total.astype(low)
        total = mixed_ref[:, head_cols:]
        for ref in tail_refs:
            total = total + ref[...].astype(jnp.float32)
        out[:, head_cols:] = total.astype(low)

    (output,) = whole_call(
        final_body, [((tok_rows, width), low)], "final", mixed, blends, *head_sums, *tail_sums
    )
    return output


def placements(tp):
    both = ("sp",) + tp
    return (
        (
            P(both, None),
            P("sp", tp, None),
            P("sp", tp, None),
            P("sp", tp, None),
            P("sp", tp, None),
            P("sp", tp, None),
            P("sp", tp, None),
            P(tp),
            P(tp),
            P(),
            P(),
            P(tp, None),
            P(tp, None),
            P(),
            P(both, None),
            P(both, None),
            P("sp", None, tp),
            P("sp", None, tp),
            P("sp", tp, None),
        ),
        P(both, None),
    )


def solution(mesh):
    sp_ways, tp_ways = (mesh.shape[axis] for axis in ("sp", "tp"))
    cores = 2

    def program(*arrays):
        resid, query_a, query_b, route_ids = arrays[0], arrays[1], arrays[4], arrays[14]
        block = resid.shape[0] // (sp_ways * tp_ways)
        heads = (query_a.shape[1] + query_b.shape[1]) // tp_ways
        capacity = 3 * route_ids.shape[1] * block // (2 * sp_ways)
        fits = heads == sp_ways and capacity % 16 == 0 and block % 16 == 0 and resid.shape[1] % 2048 == 0
        if fits:
            devices = mesh.devices.reshape(sp_ways, tp_ways // cores, cores)
            inner, axes, body = Mesh(devices, ("sp", "z", "c")), ("z", "c"), exchanged_device
        else:
            inner, axes, body = mesh, ("tp",), gathered_device
        given, returned = placements(axes)
        return jax.shard_map(body, mesh=inner, in_specs=given, out_specs=returned, check_vma=False)(*arrays)

    return program
```

```python
import math

import jax
import jax.numpy as jnp
from jax import lax
from jax.experimental import pallas as pl
from jax.experimental.pallas import tpu as pltpu
from jax.sharding import Mesh, PartitionSpec as P

EPS = 1e-06
NEG = -1e30
HEAD_SCALE = 1.0 - (0.8 - 0.6 * math.exp(-0.3))
KEY_STEP = 512


def partner(value, axis, apart):
    return lax.ppermute(value, axis, [(i, i ^ 1 << apart) for i in range(lax.axis_size(axis))])


def rms_scaled(values, gain):
    return values * lax.rsqrt(jnp.mean(values * values, axis=-1, keepdims=True) + EPS) * gain


def slot_numbers(route_rows, experts, capacity):
    count, top_count = route_rows.shape
    flat = route_rows.reshape(count * top_count)
    onehot = (flat[:, None] == jnp.arange(experts, dtype=jnp.int32)[None, :]).astype(jnp.int32)
    ranks = jnp.sum((jnp.cumsum(onehot, axis=0) - onehot) * onehot, axis=1)
    return (flat * capacity + ranks).reshape(count, top_count)


def empty_map(count, heads, width):
    return (
        jnp.zeros((count, heads, width), jnp.float32),
        jnp.full((heads, count), NEG, jnp.float32),
        jnp.zeros((heads, count), jnp.float32),
    )


def empty_group(query, value):
    return (
        empty_map(query.shape[0], query.shape[1], value.shape[2]),
        empty_map(query.shape[0], query.shape[1], value.shape[2]),
    )


def map_update(state, query, keys, values, allowed, scale):
    weighted, maximum, sums = state
    scores = jnp.einsum("qhd,khd->hqk", query, keys, preferred_element_type=jnp.float32) * scale
    scores = jnp.where(allowed[None], scores, NEG)
    fresh = jnp.maximum(maximum, jnp.max(scores, axis=2))
    weights = jnp.where(allowed[None], jnp.exp(scores - fresh[:, :, None]), 0.0)
    factor = jnp.exp(maximum - fresh)
    sums = sums * factor + jnp.sum(weights, axis=2)
    added = jnp.einsum(
        "hqk,khv->qhv", weights.astype(jnp.bfloat16), values, preferred_element_type=jnp.float32
    )
    weighted = weighted * jnp.transpose(factor)[:, :, None] + added
    return (weighted, fresh, sums)


def group_update(states, query, keys, values, allowed):
    width = query.shape[2] // 2
    scale = 1.0 / math.sqrt(width)
    return tuple(
        (
            map_update(
                states[which],
                query[:, :, which * width : (which + 1) * width],
                keys[:, :, which * width : (which + 1) * width],
                values,
                allowed,
                scale,
            )
            for which in range(2)
        )
    )


def set_update(carry, queries, pieces):
    rows_a, rows_b, query_pos = queries
    piece_key_a, piece_value_a, piece_key_b, piece_value_b = pieces
    length = piece_key_a.shape[0]
    step = math.gcd(length, KEY_STEP)
    latest = query_pos[-1]

    def inner(index, states):
        first = index * step

        def compute(current):
            keys_a = lax.dynamic_slice_in_dim(piece_key_a, first, step, 0)
            values_a = lax.dynamic_slice_in_dim(piece_value_a, first, step, 0)
            keys_b = lax.dynamic_slice_in_dim(piece_key_b, first, step, 0)
            values_b = lax.dynamic_slice_in_dim(piece_value_b, first, step, 0)
            key_pos = first + jnp.arange(step, dtype=jnp.int32)
            allowed = key_pos[None, :] <= query_pos[:, None]
            return (
                group_update(current[0], rows_a, keys_a, values_a, allowed),
                group_update(current[1], rows_b, keys_b, values_b, allowed),
            )

        return lax.cond(first <= latest, compute, lambda current: current, states)

    return lax.fori_loop(0, length // step, inner, carry)


def finish_group(states, mix, gain):
    outputs = [state[0] / jnp.transpose(state[2])[:, :, None] for state in states]
    mixed = outputs[0] - mix[None, :, None] * outputs[1]
    normed = rms_scaled(mixed, gain) * HEAD_SCALE
    return normed.astype(jnp.bfloat16).reshape(mixed.shape[0], -1)


def gathered_device(
    resid,
    query_a,
    key_a,
    value_a,
    query_b,
    key_b,
    value_b,
    mix_a,
    mix_b,
    head_gain_a,
    head_gain_b,
    proj_a,
    proj_b,
    norm_gain,
    route_ids,
    route_weights,
    expert_gate,
    expert_up,
    expert_down,
):
    seq_rows = query_a.shape[0]
    sp_ways = lax.axis_size("sp")
    place = lax.axis_index("sp")
    positions = place * seq_rows + jnp.arange(seq_rows, dtype=jnp.int32)
    levels = sp_ways.bit_length() - 1
    half = seq_rows // 2
    moved = jnp.concatenate(
        [query_a[half:].reshape(half, -1), query_b[half:].reshape(half, -1)], axis=1
    )
    for bit in range(levels):
        moved = partner(moved, "sp", bit)
    split_at = query_a.shape[1] * query_a.shape[2]
    far_a = moved[:, :split_at].reshape(half, query_a.shape[1], query_a.shape[2])
    far_b = moved[:, split_at:].reshape(half, query_b.shape[1], query_b.shape[2])
    far_pos = (sp_ways - 1 - place) * seq_rows + half + jnp.arange(half, dtype=jnp.int32)
    query_sets = ((query_a[:half], query_b[:half], positions[:half]), (far_a, far_b, far_pos))

    def fold_keys(carry, pieces):
        return tuple(
            (set_update(states, queries, pieces) for states, queries in zip(carry, query_sets))
        )

    initial = tuple(
        (
            (empty_group(queries[0], value_a), empty_group(queries[1], value_b))
            for queries in query_sets
        )
    )
    results = fold_keys(
        initial,
        (
            lax.all_gather(key_a, "sp", axis=0, tiled=True),
            lax.all_gather(value_a, "sp", axis=0, tiled=True),
            lax.all_gather(key_b, "sp", axis=0, tiled=True),
            lax.all_gather(value_b, "sp", axis=0, tiled=True),
        ),
    )
    finished = [
        (finish_group(states[0], mix_a, head_gain_a), finish_group(states[1], mix_b, head_gain_b))
        for states in results
    ]
    returned = jnp.concatenate([finished[1][0], finished[1][1]], axis=1)
    for bit in range(levels):
        returned = partner(returned, "sp", bit)
    width_a = finished[0][0].shape[1]
    heads_out_a = jnp.concatenate([finished[0][0], returned[:, :width_a]], axis=0)
    heads_out_b = jnp.concatenate([finished[0][1], returned[:, width_a:]], axis=0)
    width = resid.shape[1]
    tok_rows = resid.shape[0]
    top_count = route_ids.shape[1]
    capacity = 3 * top_count * tok_rows // (2 * sp_ways)
    own_slots = slot_numbers(route_ids, sp_ways, capacity)
    term = jnp.dot(heads_out_a, proj_a, preferred_element_type=jnp.float32)
    term = term + jnp.dot(heads_out_b, proj_b, preferred_element_type=jnp.float32)
    mixed = resid.astype(jnp.float32) + lax.psum_scatter(
        lax.optimization_barrier(term.astype(jnp.bfloat16))
        .astype(jnp.float32)
        .astype(jnp.bfloat16),
        "tp",
        scatter_dimension=0,
        tiled=True,
    ).astype(jnp.float32)
    normed = rms_scaled(mixed, norm_gain).astype(jnp.bfloat16)
    lookup = jnp.arange(sp_ways * capacity, dtype=jnp.int32)[:, None]
    spread = jnp.zeros((sp_ways * capacity, tok_rows), jnp.float32)
    for which in range(top_count):
        spread = spread + (own_slots[:, which][None, :] == lookup).astype(jnp.float32)
    outgoing = jnp.dot(
        spread.astype(jnp.bfloat16), normed, preferred_element_type=jnp.float32
    ).astype(jnp.bfloat16)
    arrived = lax.all_to_all(
        outgoing.reshape(sp_ways, capacity, width), "sp", split_axis=0, concat_axis=0, tiled=True
    )
    piece = lax.all_gather(arrived.reshape(sp_ways * capacity, width), "tp", axis=0, tiled=True)
    gate = jnp.dot(piece, expert_gate[0], preferred_element_type=jnp.float32)
    upward = jnp.dot(piece, expert_up[0], preferred_element_type=jnp.float32)
    hidden = (jax.nn.silu(gate) * upward).astype(jnp.bfloat16)
    term = jnp.dot(hidden, expert_down[0], preferred_element_type=jnp.float32)
    summed = lax.psum_scatter(
        lax.optimization_barrier(term.astype(jnp.bfloat16))
        .astype(jnp.float32)
        .astype(jnp.bfloat16),
        "tp",
        scatter_dimension=0,
        tiled=True,
    )
    finished_rows = summed.reshape(sp_ways, capacity, width)
    back = lax.all_to_all(finished_rows, "sp", split_axis=0, concat_axis=0, tiled=True)
    picked = jnp.take(back.reshape(sp_ways * capacity, width), own_slots.reshape(-1), axis=0)
    picked = picked.reshape(tok_rows, top_count, width)
    output = mixed + jnp.sum(route_weights[:, :, None] * picked.astype(jnp.float32), axis=1)
    return output.astype(jnp.bfloat16)


def attend_kernel(scalars, packed, rows, out, scores, *, step, width, block):
    place = pl.program_id(0)
    coef = scalars[0]
    query = jnp.transpose(packed[place, 0:width, :])
    queries = [query * rows[which : which + 1, :].astype(jnp.bfloat16) for which in range(2)]
    outputs = []

    def fold(values, combine):
        parts = [values[:, at * width : (at + 1) * width] for at in range(step // width)]
        while len(parts) > 1:
            parts = [combine(*parts[at : at + 2]) for at in range(0, len(parts), 2)]
        return parts[0]

    def raw(which, index):
        return jnp.dot(
            queries[which], packed[index, width : 2 * width, :], preferred_element_type=jnp.float32
        )

    row = lax.broadcasted_iota(jnp.int32, (step, step), 0)
    column = lax.broadcasted_iota(jnp.int32, (step, step), 1)
    allowed = column <= row
    highest = []
    for which in range(2):
        own = jnp.where(allowed, raw(which, place), NEG)
        scores[which, place] = own
        highest.append(fold(own, jnp.maximum))

    def first_pass(index, carry):
        found = []
        for which in range(2):
            block = raw(which, index)
            scores[which, index] = block
            found.append(jnp.maximum(carry[which], fold(block, jnp.maximum)))
        return tuple(found)

    highest = lax.fori_loop(0, place, first_pass, tuple(highest))
    tops = [jnp.max(found, axis=1, keepdims=True) * coef for found in highest]

    def second_pass(index, carry):
        values = packed[index, 2 * width : 3 * width, :]
        found = []
        for which in range(2):
            total, mixed = carry[which]
            weights = jnp.exp2(scores[which, index] * coef - tops[which])
            total = total + fold(weights, jnp.add)
            mixed = mixed + lax.dot_general(
                weights.astype(jnp.bfloat16),
                values,
                (((1,), (1,)), ((), ())),
                preferred_element_type=jnp.float32,
            )
            found.append((total, mixed))
        return tuple(found)

    empty = jnp.zeros((step, width), jnp.float32)
    found = lax.fori_loop(0, place + 1, second_pass, ((empty, empty), (empty, empty)))
    outputs = [mixed / jnp.sum(total, axis=1, keepdims=True) for total, mixed in found]
    mixed = outputs[0] - scalars[1] * outputs[1]
    square = jnp.sum(mixed * mixed, axis=1, keepdims=True) * scalars[2]
    normed = (mixed * lax.rsqrt(square + EPS) * rows[2:3, :]).astype(jnp.bfloat16)
    cores = out.shape[1]
    for at in range(step // block):
        first = at // cores * block
        out[0, at % cores, first : first + block] = normed[at * block : (at + 1) * block]


def widen(values, width):
    missing = width - values.shape[-1]
    return jnp.pad(values, [(0, 0)] * (values.ndim - 1) + [(0, missing)]) if missing else values


def fast_memory(limit_mib):
    return pltpu.CompilerParams(vmem_limit_bytes=limit_mib << 20)


def mirrored(value, axis, apart):
    return lax.ppermute(value, axis, [(i, i ^ apart) for i in range(lax.axis_size(axis))])


def whole_call(body, outs, name, *operands, scalars=(), flops=0, scratch=(), limit=8):
    vmem = pl.BlockSpec(memory_space=pltpu.VMEM)
    return pl.pallas_call(
        body,
        in_specs=[pl.BlockSpec(memory_space=pltpu.SMEM)] * len(scalars) + [vmem] * len(operands),
        out_specs=[vmem] * len(outs),
        out_shape=[pltpu.VMEM(shape, dtype) for shape, dtype in outs],
        scratch_shapes=scratch,
        compiler_params=fast_memory(limit),
        cost_estimate=pl.CostEstimate(flops=flops, bytes_accessed=0, transcendentals=0),
        name=name,
    )(*scalars, *[pltpu.with_memory_space_constraint(operand, pltpu.VMEM) for operand in operands])


def exchanged_heads(query_a, key_a, value_a, query_b, key_b, value_b, mix_a, mix_b, head_gain_a, head_gain_b, block):
    seq_rows, heads_a, _ = query_a.shape
    ways = lax.axis_size("sp")
    cores = lax.axis_size("c")
    place = lax.axis_index("sp")
    groups = ((query_a, key_a, value_a), (query_b, key_b, value_b))
    widest = max(array.shape[2] for group in groups for array in group)
    width = -(-widest // 128) * 128
    outgoing = jnp.concatenate(
        [
            jnp.concatenate([jnp.transpose(widen(array, width), (1, 2, 0)) for array in group], axis=1)
            for group in groups
        ],
        axis=0,
    )
    arrived = lax.all_to_all(outgoing, "sp", split_axis=0, concat_axis=0, tiled=True)
    packed = arrived
    first = place < heads_a
    maps = jnp.where(first, query_a.shape[2] // 2, query_b.shape[2] // 2)
    lanes = jnp.arange(width, dtype=jnp.int32)
    gain = jnp.where(first, widen(head_gain_a, width), widen(head_gain_b, width)) * HEAD_SCALE
    rows = jnp.stack(
        [(lanes < maps).astype(jnp.float32), ((lanes >= maps) & (lanes < 2 * maps)).astype(jnp.float32), gain]
    )
    coef_a, coef_b = [math.log2(math.e) / math.sqrt(group[0].shape[2] // 2) for group in groups]
    scalars = jnp.stack(
        [
            jnp.where(first, coef_a, coef_b).astype(jnp.float32),
            lax.dynamic_index_in_dim(jnp.concatenate([mix_a, mix_b]), place, 0, False),
            jnp.where(first, 1.0 / value_a.shape[2], 1.0 / value_b.shape[2]).astype(jnp.float32),
        ]
    )
    shape = (ways, cores, seq_rows // cores, width)
    mixed = pl.pallas_call(
        lambda *refs: attend_kernel(*refs, step=seq_rows, width=width, block=block),
        grid=(ways,),
        in_specs=[
            pl.BlockSpec(memory_space=pltpu.SMEM),
            pl.BlockSpec(packed.shape, lambda index: (0, 0, 0)),
            pl.BlockSpec(rows.shape, lambda index: (0, 0)),
        ],
        out_specs=pl.BlockSpec((1,) + shape[1:], lambda index: (index, 0, 0, 0)),
        out_shape=jax.ShapeDtypeStruct(shape, jnp.bfloat16),
        scratch_shapes=[pltpu.VMEM((2, ways, seq_rows, seq_rows), jnp.float32)],
        compiler_params=pltpu.CompilerParams(dimension_semantics=("arbitrary",), vmem_limit_bytes=32 << 20),
        name="attend",
    )(scalars, packed, rows)
    flat = mixed.reshape((ways * cores,) + shape[2:])
    return lax.all_to_all(flat, ("sp", "c"), split_axis=0, concat_axis=0, tiled=True).reshape(shape)


def project(heads, proj_a, proj_b, lines, block, heads_a):
    ways, cores, rows, width = heads.shape
    model = proj_a.shape[1]
    weights = []
    for apart in range(cores):
        weights += [proj_a, proj_b] if apart == 0 else [mirrored(proj_a, "c", apart), mirrored(proj_b, "c", apart)]
    where = jnp.stack([lax.axis_index("c"), lax.axis_index("z")]).astype(jnp.int32)
    step = math.gcd(model, 512)
    narrow = proj_b.shape[0] // (ways - heads_a)
    wide = proj_a.shape[0] // heads_a

    def body(at, heads_ref, *refs):
        sets, outs = refs[: 2 * cores], refs[2 * cores :]
        pairs = []
        for apart in range(cores):
            core = at[0] ^ apart

            def taken(head, used):
                found = [heads_ref[head, core, pl.ds((at[1] ^ far) * block, block), :] for far in range(lines)]
                return jnp.concatenate(found, axis=0)[:, :used]

            left_a = jnp.concatenate([taken(head, wide) for head in range(heads_a)], axis=1)
            left_b = jnp.concatenate([taken(head, narrow) for head in range(heads_a, ways)], axis=1)
            pairs += [(left_a, sets[2 * apart]), (left_b, sets[2 * apart + 1])]
        for first in range(0, model, step):
            span = slice(first, first + step)
            total = None
            for left, right in pairs:
                piece = jnp.dot(left, right[:, span], preferred_element_type=jnp.float32)
                total = piece if total is None else total + piece
            for far in range(lines):
                outs[far][:, span] = total[far * block : (far + 1) * block].astype(jnp.bfloat16)

    return whole_call(
        body,
        [((block, model), jnp.bfloat16)] * lines,
        "project",
        heads,
        *weights,
        scalars=(where,),
        flops=2 * rows * model * (proj_a.shape[0] + proj_b.shape[0]) * cores,
    )


def expert_hidden(rows_ref, gate_ref, up_ref, held, first, count):
    hidden = gate_ref.shape[1]
    tile = math.gcd(hidden, 256)
    for at in range(hidden // tile):
        span = slice(at * tile, (at + 1) * tile)
        gate = jnp.dot(rows_ref[pl.ds(first, count), :], gate_ref[:, span], preferred_element_type=jnp.float32)
        upward = jnp.dot(rows_ref[pl.ds(first, count), :], up_ref[:, span], preferred_element_type=jnp.float32)
        held[:, span] = (jax.nn.silu(gate) * upward).astype(jnp.bfloat16)


def expert_down(held, down_ref, out_ref, first, count):
    model = down_ref.shape[1]
    tile = math.gcd(model, 512)
    for at in range(model // tile):
        span = slice(at * tile, (at + 1) * tile)
        total = jnp.dot(held, down_ref[:, span], preferred_element_type=jnp.float32)
        out_ref[pl.ds(first, count), span] = total.astype(jnp.bfloat16)


def expert_call(name, rows, weights, out_cols, after=()):
    count = rows.shape[0]
    hidden = weights[-1].shape[0] if len(weights) != 2 else weights[0].shape[1]
    tile = math.gcd(count, 256)
    flops = 2 * count * sum(weight.size for weight in weights)

    def body(rows_ref, *refs):
        weight_refs, (out_ref, held) = refs[: len(weights)], refs[-2:]

        def step(index, carry):
            first = index * tile
            if len(weights) > 1:
                expert_hidden(rows_ref, *weight_refs[:2], held, first, tile)
            if len(weights) == 2:
                out_ref[pl.ds(first, tile), :] = held[...]
            else:
                left = held[...] if len(weights) == 3 else rows_ref[pl.ds(first, tile), :]
                expert_down(left, weight_refs[-1], out_ref, first, tile)
            return carry

        lax.fori_loop(0, count // tile, step, 0)

    (out,) = whole_call(
        body,
        [((count, out_cols), jnp.bfloat16)],
        name,
        rows,
        *weights,
        *after,
        flops=flops,
        scratch=[pltpu.VMEM((tile, hidden), jnp.bfloat16)],
    )
    return out


def exchanged_device(
    resid,
    query_a,
    key_a,
    value_a,
    query_b,
    key_b,
    value_b,
    mix_a,
    mix_b,
    head_gain_a,
    head_gain_b,
    proj_a,
    proj_b,
    norm_gain,
    route_ids,
    route_weights,
    expert_gate,
    expert_up,
    down_w,
):
    ways, lines, cores = (lax.axis_size(axis) for axis in ("sp", "z", "c"))
    place = lax.axis_index("sp")
    tok_rows, width = resid.shape
    top_count = route_ids.shape[1]
    capacity = 3 * top_count * tok_rows // (2 * ways)
    slots_all = ways * capacity
    low = jnp.bfloat16
    head_cols = width * 5 // 16 // 128 * 128
    tail_cols = width - head_cols

    heads = exchanged_heads(
        query_a, key_a, value_a, query_b, key_b, value_b, mix_a, mix_b, head_gain_a, head_gain_b, tok_rows
    )

    slots = slot_numbers(route_ids ^ place, ways, capacity)
    routes = jnp.concatenate([slots.astype(jnp.float32), route_weights], axis=1)
    line_routes = [routes] + [mirrored(routes, "z", far) for far in range(1, lines)]
    lookup = jnp.arange(slots_all, dtype=jnp.int32)
    spreads, blends = [], []
    for found in line_routes:
        hits = [found[:, which].astype(jnp.int32)[:, None] == lookup[None, :] for which in range(top_count)]
        spread = sum(hit.astype(jnp.float32) for hit in hits)
        blend = sum(
            jnp.where(hits[which], found[:, top_count + which][:, None], 0.0) for which in range(top_count)
        )
        upper = blend.astype(low)
        spreads.append(jnp.transpose(spread).astype(low))
        blends += [upper, (blend - upper.astype(jnp.float32)).astype(low)]
    spreads = jnp.stack(spreads)
    blends = jnp.stack(blends).reshape(lines, 2, tok_rows, slots_all)

    parts = project(heads, proj_a, proj_b, lines, tok_rows, query_a.shape[1])
    parts = [parts[0]] + [mirrored(parts[far], "z", far) for far in range(1, lines)]

    def norm_body(*refs):
        part_refs, (resid_ref, gain_ref, spread_ref), outs = refs[:lines], refs[lines : lines + 3], refs[lines + 3 :]
        mixed = resid_ref[...].astype(jnp.float32)
        for part in part_refs:
            mixed = mixed + part[...].astype(jnp.float32)
        outs[0][...] = mixed
        normed = rms_scaled(mixed, gain_ref[...]).astype(low)
        outs[1][...] = normed[:, head_cols:]
        picked = jnp.dot(spread_ref[0], normed[:, :head_cols], preferred_element_type=jnp.float32).astype(low)
        for far in range(ways):
            outs[2 + far][...] = picked[far * capacity : (far + 1) * capacity]

    mixed, tail, *heads_out = whole_call(
        norm_body,
        [((tok_rows, width), jnp.float32), ((tok_rows, tail_cols), low)] + [((capacity, head_cols), low)] * ways,
        "norm",
        *parts,
        resid,
        norm_gain[None, :],
        spreads,
    )
    tails = [tail] + [mirrored(tail, "z", far) for far in range(1, lines)]
    head_own = jnp.concatenate(
        [heads_out[0]] + [mirrored(heads_out[far], "sp", far) for far in range(1, ways)], axis=0
    )
    head_blocks = [head_own] + [mirrored(head_own, "z", far) for far in range(1, lines)]

    def spread_body(*refs):
        tail_refs, spread_ref, outs = refs[:lines], refs[lines], refs[lines + 1 :]
        for line in range(lines):
            picked = jnp.dot(spread_ref[line], tail_refs[line][...], preferred_element_type=jnp.float32).astype(low)
            for far in range(ways):
                outs[far][line * capacity : (line + 1) * capacity] = picked[far * capacity : (far + 1) * capacity]

    tails_out = whole_call(
        spread_body, [((lines * capacity, tail_cols), low)] * ways, "spread", *tails, spreads
    )
    tail_blocks = [tails_out[0]] + [mirrored(tails_out[far], "sp", far) for far in range(1, ways)]

    def join_body(*refs):
        head_refs, tail_refs, (out,) = refs[:lines], refs[lines : lines + ways], refs[lines + ways :]
        for line in range(lines):
            for far in range(ways):
                first = line * slots_all + far * capacity
                out[first : first + capacity, :head_cols] = head_refs[line][far * capacity : (far + 1) * capacity]
                out[first : first + capacity, head_cols:] = tail_refs[far][line * capacity : (line + 1) * capacity]

    (rows,) = whole_call(join_body, [((lines * slots_all, width), low)], "join", *head_blocks, *tail_blocks)
    weights = (expert_gate[0], expert_up[0], down_w[0])
    other_rows = [mirrored(rows, "c", apart) for apart in range(1, cores)]
    hidden = expert_call("hidden", rows, weights[:2], weights[0].shape[1])
    core_parts = [
        mirrored(expert_call("experts", other, weights, width, (hidden,)), "c", apart + 1)
        for apart, other in enumerate(other_rows)
    ]
    own_part = expert_call("down", hidden, weights[2:], width)

    def pair_body(*refs):
        part_refs, outs = refs[:cores], refs[cores:]
        for line in range(lines):
            for far in range(ways):
                first = line * slots_all + far * capacity
                total = part_refs[0][first : first + capacity].astype(jnp.float32)
                for part in part_refs[1:]:
                    total = total + part[first : first + capacity].astype(jnp.float32)
                total = total.astype(low)
                outs[line][far * capacity : (far + 1) * capacity] = total[:, :head_cols]
                outs[lines + far][line * capacity : (line + 1) * capacity] = total[:, head_cols:]

    back = whole_call(
        pair_body,
        [((slots_all, head_cols), low)] * lines + [((lines * capacity, tail_cols), low)] * ways,
        "pair",
        own_part,
        *core_parts,
    )
    tail_back = [back[lines]] + [mirrored(back[lines + far], "sp", far) for far in range(1, ways)]
    head_back = [back[0]] + [mirrored(back[far], "z", far) for far in range(1, lines)]

    def blend_body(*refs):
        tail_refs, blend_ref, outs = refs[:ways], refs[ways], refs[ways + 1 :]
        for line in range(lines):
            block = jnp.concatenate([ref[line * capacity : (line + 1) * capacity] for ref in tail_refs], axis=0)
            total = jnp.dot(blend_ref[line, 0], block, preferred_element_type=jnp.float32)
            total = total + jnp.dot(blend_ref[line, 1], block, preferred_element_type=jnp.float32)
            outs[line][...] = total.astype(low)

    tail_sums = whole_call(blend_body, [((tok_rows, tail_cols), low)] * lines, "blend", *tail_back, blends)
    tail_sums = [tail_sums[0]] + [mirrored(tail_sums[far], "z", far) for far in range(1, lines)]

    def total_body(*refs):
        part_refs, outs = refs[:lines], refs[lines:]
        total = sum(part[...].astype(jnp.float32) for part in part_refs).astype(low)
        for far in range(ways):
            outs[far][...] = total[far * capacity : (far + 1) * capacity]

    head_sums = whole_call(total_body, [((capacity, head_cols), low)] * ways, "total", *head_back)
    head_sums = [head_sums[0]] + [mirrored(head_sums[far], "sp", far) for far in range(1, ways)]

    def final_body(mixed_ref, blend_ref, *refs):
        head_refs, tail_refs, (out,) = refs[:ways], refs[ways : ways + lines], refs[ways + lines :]
        block = jnp.concatenate([ref[...] for ref in head_refs], axis=0)
        total = mixed_ref[:, :head_cols] + jnp.dot(blend_ref[0, 0], block, preferred_element_type=jnp.float32)
        total = total + jnp.dot(blend_ref[0, 1], block, preferred_element_type=jnp.float32)
        out[:, :head_cols] = total.astype(low)
        total = mixed_ref[:, head_cols:]
        for ref in tail_refs:
            total = total + ref[...].astype(jnp.float32)
        out[:, head_cols:] = total.astype(low)

    (output,) = whole_call(
        final_body, [((tok_rows, width), low)], "final", mixed, blends, *head_sums, *tail_sums
    )
    return output


def placements(tp):
    both = ("sp",) + tp
    return (
        (
            P(both, None),
            P("sp", tp, None),
            P("sp", tp, None),
            P("sp", tp, None),
            P("sp", tp, None),
            P("sp", tp, None),
            P("sp", tp, None),
            P(tp),
            P(tp),
            P(),
            P(),
            P(tp, None),
            P(tp, None),
            P(),
            P(both, None),
            P(both, None),
            P("sp", None, tp),
            P("sp", None, tp),
            P("sp", tp, None),
        ),
        P(both, None),
    )


def solution(mesh):
    sp_ways, tp_ways = (mesh.shape[axis] for axis in ("sp", "tp"))
    cores = 2

    def program(*arrays):
        resid, query_a, query_b, route_ids = arrays[0], arrays[1], arrays[4], arrays[14]
        block = resid.shape[0] // (sp_ways * tp_ways)
        heads = (query_a.shape[1] + query_b.shape[1]) // tp_ways
        capacity = 3 * route_ids.shape[1] * block // (2 * sp_ways)
        fits = heads == sp_ways and capacity % 16 == 0 and block % 16 == 0 and resid.shape[1] % 2048 == 0
        if fits:
            devices = mesh.devices.reshape(sp_ways, tp_ways // cores, cores)
            inner, axes, body = Mesh(devices, ("sp", "z", "c")), ("z", "c"), exchanged_device
        else:
            inner, axes, body = mesh, ("tp",), gathered_device
        given, returned = placements(axes)
        return jax.shard_map(body, mesh=inner, in_specs=given, out_specs=returned, check_vma=False)(*arrays)

    return program
```

```python
import math

import jax
import jax.numpy as jnp
from jax import lax
from jax.experimental import pallas as pl
from jax.experimental.pallas import tpu as pltpu
from jax.sharding import Mesh, PartitionSpec as P

EPS = 1e-06
NEG = -1e30
HEAD_SCALE = 1.0 - (0.8 - 0.6 * math.exp(-0.3))
KEY_STEP = 512


def partner(value, axis, apart):
    return lax.ppermute(value, axis, [(i, i ^ 1 << apart) for i in range(lax.axis_size(axis))])


def rms_scaled(values, gain):
    return values * lax.rsqrt(jnp.mean(values * values, axis=-1, keepdims=True) + EPS) * gain


def slot_numbers(route_rows, experts, capacity):
    count, top_count = route_rows.shape
    flat = route_rows.reshape(count * top_count)
    onehot = (flat[:, None] == jnp.arange(experts, dtype=jnp.int32)[None, :]).astype(jnp.int32)
    ranks = jnp.sum((jnp.cumsum(onehot, axis=0) - onehot) * onehot, axis=1)
    return (flat * capacity + ranks).reshape(count, top_count)


def empty_map(count, heads, width):
    return (
        jnp.zeros((count, heads, width), jnp.float32),
        jnp.full((heads, count), NEG, jnp.float32),
        jnp.zeros((heads, count), jnp.float32),
    )


def empty_group(query, value):
    return (
        empty_map(query.shape[0], query.shape[1], value.shape[2]),
        empty_map(query.shape[0], query.shape[1], value.shape[2]),
    )


def map_update(state, query, keys, values, allowed, scale):
    weighted, maximum, sums = state
    scores = jnp.einsum("qhd,khd->hqk", query, keys, preferred_element_type=jnp.float32) * scale
    scores = jnp.where(allowed[None], scores, NEG)
    fresh = jnp.maximum(maximum, jnp.max(scores, axis=2))
    weights = jnp.where(allowed[None], jnp.exp(scores - fresh[:, :, None]), 0.0)
    factor = jnp.exp(maximum - fresh)
    sums = sums * factor + jnp.sum(weights, axis=2)
    added = jnp.einsum(
        "hqk,khv->qhv", weights.astype(jnp.bfloat16), values, preferred_element_type=jnp.float32
    )
    weighted = weighted * jnp.transpose(factor)[:, :, None] + added
    return (weighted, fresh, sums)


def group_update(states, query, keys, values, allowed):
    width = query.shape[2] // 2
    scale = 1.0 / math.sqrt(width)
    return tuple(
        (
            map_update(
                states[which],
                query[:, :, which * width : (which + 1) * width],
                keys[:, :, which * width : (which + 1) * width],
                values,
                allowed,
                scale,
            )
            for which in range(2)
        )
    )


def set_update(carry, queries, pieces):
    rows_a, rows_b, query_pos = queries
    piece_key_a, piece_value_a, piece_key_b, piece_value_b = pieces
    length = piece_key_a.shape[0]
    step = math.gcd(length, KEY_STEP)
    latest = query_pos[-1]

    def inner(index, states):
        first = index * step

        def compute(current):
            keys_a = lax.dynamic_slice_in_dim(piece_key_a, first, step, 0)
            values_a = lax.dynamic_slice_in_dim(piece_value_a, first, step, 0)
            keys_b = lax.dynamic_slice_in_dim(piece_key_b, first, step, 0)
            values_b = lax.dynamic_slice_in_dim(piece_value_b, first, step, 0)
            key_pos = first + jnp.arange(step, dtype=jnp.int32)
            allowed = key_pos[None, :] <= query_pos[:, None]
            return (
                group_update(current[0], rows_a, keys_a, values_a, allowed),
                group_update(current[1], rows_b, keys_b, values_b, allowed),
            )

        return lax.cond(first <= latest, compute, lambda current: current, states)

    return lax.fori_loop(0, length // step, inner, carry)


def finish_group(states, mix, gain):
    outputs = [state[0] / jnp.transpose(state[2])[:, :, None] for state in states]
    mixed = outputs[0] - mix[None, :, None] * outputs[1]
    normed = rms_scaled(mixed, gain) * HEAD_SCALE
    return normed.astype(jnp.bfloat16).reshape(mixed.shape[0], -1)


def gathered_device(
    resid,
    query_a,
    key_a,
    value_a,
    query_b,
    key_b,
    value_b,
    mix_a,
    mix_b,
    head_gain_a,
    head_gain_b,
    proj_a,
    proj_b,
    norm_gain,
    route_ids,
    route_weights,
    expert_gate,
    expert_up,
    expert_down,
):
    seq_rows = query_a.shape[0]
    sp_ways = lax.axis_size("sp")
    place = lax.axis_index("sp")
    positions = place * seq_rows + jnp.arange(seq_rows, dtype=jnp.int32)
    levels = sp_ways.bit_length() - 1
    half = seq_rows // 2
    moved = jnp.concatenate(
        [query_a[half:].reshape(half, -1), query_b[half:].reshape(half, -1)], axis=1
    )
    for bit in range(levels):
        moved = partner(moved, "sp", bit)
    split_at = query_a.shape[1] * query_a.shape[2]
    far_a = moved[:, :split_at].reshape(half, query_a.shape[1], query_a.shape[2])
    far_b = moved[:, split_at:].reshape(half, query_b.shape[1], query_b.shape[2])
    far_pos = (sp_ways - 1 - place) * seq_rows + half + jnp.arange(half, dtype=jnp.int32)
    query_sets = ((query_a[:half], query_b[:half], positions[:half]), (far_a, far_b, far_pos))

    def fold_keys(carry, pieces):
        return tuple(
            (set_update(states, queries, pieces) for states, queries in zip(carry, query_sets))
        )

    initial = tuple(
        (
            (empty_group(queries[0], value_a), empty_group(queries[1], value_b))
            for queries in query_sets
        )
    )
    results = fold_keys(
        initial,
        (
            lax.all_gather(key_a, "sp", axis=0, tiled=True),
            lax.all_gather(value_a, "sp", axis=0, tiled=True),
            lax.all_gather(key_b, "sp", axis=0, tiled=True),
            lax.all_gather(value_b, "sp", axis=0, tiled=True),
        ),
    )
    finished = [
        (finish_group(states[0], mix_a, head_gain_a), finish_group(states[1], mix_b, head_gain_b))
        for states in results
    ]
    returned = jnp.concatenate([finished[1][0], finished[1][1]], axis=1)
    for bit in range(levels):
        returned = partner(returned, "sp", bit)
    width_a = finished[0][0].shape[1]
    heads_out_a = jnp.concatenate([finished[0][0], returned[:, :width_a]], axis=0)
    heads_out_b = jnp.concatenate([finished[0][1], returned[:, width_a:]], axis=0)
    width = resid.shape[1]
    tok_rows = resid.shape[0]
    top_count = route_ids.shape[1]
    capacity = 3 * top_count * tok_rows // (2 * sp_ways)
    own_slots = slot_numbers(route_ids, sp_ways, capacity)
    term = jnp.dot(heads_out_a, proj_a, preferred_element_type=jnp.float32)
    term = term + jnp.dot(heads_out_b, proj_b, preferred_element_type=jnp.float32)
    mixed = resid.astype(jnp.float32) + lax.psum_scatter(
        lax.optimization_barrier(term.astype(jnp.bfloat16))
        .astype(jnp.float32)
        .astype(jnp.bfloat16),
        "tp",
        scatter_dimension=0,
        tiled=True,
    ).astype(jnp.float32)
    normed = rms_scaled(mixed, norm_gain).astype(jnp.bfloat16)
    lookup = jnp.arange(sp_ways * capacity, dtype=jnp.int32)[:, None]
    spread = jnp.zeros((sp_ways * capacity, tok_rows), jnp.float32)
    for which in range(top_count):
        spread = spread + (own_slots[:, which][None, :] == lookup).astype(jnp.float32)
    outgoing = jnp.dot(
        spread.astype(jnp.bfloat16), normed, preferred_element_type=jnp.float32
    ).astype(jnp.bfloat16)
    arrived = lax.all_to_all(
        outgoing.reshape(sp_ways, capacity, width), "sp", split_axis=0, concat_axis=0, tiled=True
    )
    piece = lax.all_gather(arrived.reshape(sp_ways * capacity, width), "tp", axis=0, tiled=True)
    gate = jnp.dot(piece, expert_gate[0], preferred_element_type=jnp.float32)
    upward = jnp.dot(piece, expert_up[0], preferred_element_type=jnp.float32)
    hidden = (jax.nn.silu(gate) * upward).astype(jnp.bfloat16)
    term = jnp.dot(hidden, expert_down[0], preferred_element_type=jnp.float32)
    summed = lax.psum_scatter(
        lax.optimization_barrier(term.astype(jnp.bfloat16))
        .astype(jnp.float32)
        .astype(jnp.bfloat16),
        "tp",
        scatter_dimension=0,
        tiled=True,
    )
    finished_rows = summed.reshape(sp_ways, capacity, width)
    back = lax.all_to_all(finished_rows, "sp", split_axis=0, concat_axis=0, tiled=True)
    picked = jnp.take(back.reshape(sp_ways * capacity, width), own_slots.reshape(-1), axis=0)
    picked = picked.reshape(tok_rows, top_count, width)
    output = mixed + jnp.sum(route_weights[:, :, None] * picked.astype(jnp.float32), axis=1)
    return output.astype(jnp.bfloat16)


def attend_map(coef, queries_of, keys_of, values_of, scores, step, width):
    place = pl.program_id(0)
    query = jnp.transpose(queries_of(place))

    def fold(values, combine):
        parts = [values[:, at * width : (at + 1) * width] for at in range(step // width)]
        while len(parts) > 1:
            parts = [combine(*parts[at : at + 2]) for at in range(0, len(parts), 2)]
        return parts[0]

    def raw(index):
        return jnp.dot(query, keys_of(index), preferred_element_type=jnp.float32)

    row = lax.broadcasted_iota(jnp.int32, (step, step), 0)
    column = lax.broadcasted_iota(jnp.int32, (step, step), 1)
    own = jnp.where(column <= row, raw(place), NEG)
    scores[place] = own

    def first_pass(index, highest):
        block = raw(index)
        scores[index] = block
        return jnp.maximum(highest, fold(block, jnp.maximum))

    highest = lax.fori_loop(0, place, first_pass, fold(own, jnp.maximum))
    top = jnp.max(highest, axis=1, keepdims=True) * coef

    def second_pass(index, carry):
        total, mixed = carry
        weights = jnp.exp2(scores[index] * coef - top)
        total = total + fold(weights, jnp.add)
        mixed = mixed + lax.dot_general(
            weights.astype(jnp.bfloat16),
            values_of(index),
            (((1,), (1,)), ((), ())),
            preferred_element_type=jnp.float32,
        )
        return total, mixed

    empty = jnp.zeros((step, width), jnp.float32)
    total, mixed = lax.fori_loop(0, place + 1, second_pass, (empty, empty))
    return mixed / jnp.sum(total, axis=1, keepdims=True)


def first_map_kernel(scalars, packed, out, scores, *, step, width, maps):
    out[0] = attend_map(
        scalars[0],
        lambda at: packed[at, 0:maps, :],
        lambda at: packed[at, maps : 2 * maps, :],
        lambda at: packed[at, 2 * maps : 2 * maps + width, :],
        scores,
        step,
        width,
    )


def second_map_kernel(scalars, own, packed, gain, first, *refs, step, width, maps, block):
    pieces, (out, scores, later) = refs[:-3], refs[-3:]

    @pl.when(pl.program_id(0) == 0)
    def _():
        for far, piece in enumerate(pieces):
            later[own[0] ^ far] = piece[...]

    second = attend_map(
        scalars[0],
        lambda at: later[at, 0:maps, :],
        lambda at: later[at, maps : 2 * maps, :],
        lambda at: packed[at, 2 * maps : 2 * maps + width, :],
        scores,
        step,
        width,
    )
    mixed = first[0] - scalars[1] * second
    square = jnp.sum(mixed * mixed, axis=1, keepdims=True) * scalars[2]
    normed = (mixed * lax.rsqrt(square + EPS) * gain[...]).astype(jnp.bfloat16)
    cores = out.shape[1]
    for at in range(step // block):
        begin = at // cores * block
        out[0, at % cores, begin : begin + block] = normed[at * block : (at + 1) * block]


def widen(values, width):
    missing = width - values.shape[-1]
    return jnp.pad(values, [(0, 0)] * (values.ndim - 1) + [(0, missing)]) if missing else values


def fast_memory(limit_mib):
    return pltpu.CompilerParams(vmem_limit_bytes=limit_mib << 20)


def mirrored(value, axis, apart):
    return lax.ppermute(value, axis, [(i, i ^ apart) for i in range(lax.axis_size(axis))])


def mirrored_all(values, axis):
    found = {far: mirrored(values[far], axis, far) for far in reversed(range(1, len(values)))}
    return [values[0]] + [found[far] for far in range(1, len(values))]


def whole_call(body, outs, name, *operands, scalars=(), flops=0, scratch=(), limit=8):
    vmem = pl.BlockSpec(memory_space=pltpu.VMEM)
    return pl.pallas_call(
        body,
        in_specs=[pl.BlockSpec(memory_space=pltpu.SMEM)] * len(scalars) + [vmem] * len(operands),
        out_specs=[vmem] * len(outs),
        out_shape=[pltpu.VMEM(shape, dtype) for shape, dtype in outs],
        scratch_shapes=scratch,
        compiler_params=fast_memory(limit),
        cost_estimate=pl.CostEstimate(flops=flops, bytes_accessed=0, transcendentals=0),
        name=name,
    )(*scalars, *[pltpu.with_memory_space_constraint(operand, pltpu.VMEM) for operand in operands])


def exchanged_heads(query_a, key_a, value_a, query_b, key_b, value_b, mix_a, mix_b, head_gain_a, head_gain_b, block):
    seq_rows, heads_a, _ = query_a.shape
    ways = lax.axis_size("sp")
    cores = lax.axis_size("c")
    place = lax.axis_index("sp")
    groups = ((query_a, key_a, value_a), (query_b, key_b, value_b))
    width = -(-max(group[2].shape[2] for group in groups) // 128) * 128
    maps = -(-max(group[0].shape[2] // 2 for group in groups) // 16) * 16

    def filled(array, size):
        return jnp.pad(array, ((0, 0), (0, size - array.shape[1]), (0, 0)))

    turned = lax.optimization_barrier([[jnp.transpose(array, (1, 2, 0)) for array in group] for group in groups])
    early, later = [], []
    for query, key, value in turned:
        half = query.shape[1] // 2
        early.append(
            jnp.concatenate([filled(array[:, :half], maps) for array in (query, key)] + [filled(value, width)], axis=1)
        )
        later.append(jnp.concatenate([filled(array[:, half:], maps) for array in (query, key)], axis=1))
    packed = lax.all_to_all(jnp.concatenate(early, axis=0), "sp", split_axis=0, concat_axis=0, tiled=True)
    later = jnp.concatenate(later, axis=0)
    later = mirrored_all([lax.dynamic_index_in_dim(later, place ^ far, 0, False) for far in range(ways)], "sp")
    first = place < heads_a
    gain = jnp.where(first, widen(head_gain_a, width), widen(head_gain_b, width)) * HEAD_SCALE
    coef_a, coef_b = [math.log2(math.e) / math.sqrt(group[0].shape[2] // 2) for group in groups]
    scalars = jnp.stack(
        [
            jnp.where(first, coef_a, coef_b).astype(jnp.float32),
            lax.dynamic_index_in_dim(jnp.concatenate([mix_a, mix_b]), place, 0, False),
            jnp.where(first, 1.0 / value_a.shape[2], 1.0 / value_b.shape[2]).astype(jnp.float32),
        ]
    )
    sizes = dict(step=seq_rows, width=width, maps=maps)
    pairs = (ways * seq_rows) * (ways + 1) * seq_rows // 2
    smem = pl.BlockSpec(memory_space=pltpu.SMEM)
    whole = lambda array: pl.BlockSpec(array.shape, lambda index: (0,) * array.ndim)
    scores = pltpu.VMEM((ways, seq_rows, seq_rows), jnp.float32)
    common = dict(
        grid=(ways,),
        compiler_params=pltpu.CompilerParams(dimension_semantics=("arbitrary",), vmem_limit_bytes=16 << 20),
        cost_estimate=pl.CostEstimate(
            flops=2 * pairs * (maps + width), bytes_accessed=packed.size * 2, transcendentals=pairs
        ),
    )
    mixed_first = pl.pallas_call(
        lambda *refs: first_map_kernel(*refs, **sizes),
        in_specs=[smem, whole(packed)],
        out_specs=pl.BlockSpec((1, seq_rows, width), lambda index: (index, 0, 0)),
        out_shape=jax.ShapeDtypeStruct((ways, seq_rows, width), jnp.float32),
        scratch_shapes=[scores],
        name="first_map",
        **common,
    )(scalars, packed)
    shape = (ways, cores, seq_rows // cores, width)
    mixed = pl.pallas_call(
        lambda *refs: second_map_kernel(*refs, block=block, **sizes),
        in_specs=[
            smem,
            smem,
            whole(packed),
            pl.BlockSpec((1, width), lambda index: (0, 0)),
            pl.BlockSpec((1, seq_rows, width), lambda index: (index, 0, 0)),
            *[whole(piece) for piece in later],
        ],
        out_specs=pl.BlockSpec((1,) + shape[1:], lambda index: (index, 0, 0, 0)),
        out_shape=jax.ShapeDtypeStruct(shape, jnp.bfloat16),
        scratch_shapes=[scores, pltpu.VMEM((ways, 2 * maps, seq_rows), jnp.bfloat16)],
        name="second_map",
        **common,
    )(scalars, place[None].astype(jnp.int32), packed, gain[None, :], mixed_first, *later)
    flat = mixed.reshape((ways * cores,) + shape[2:])
    return lax.all_to_all(flat, ("sp", "c"), split_axis=0, concat_axis=0, tiled=True).reshape(shape)


def project(heads, proj_a, proj_b, lines, block, heads_a):
    ways, cores, rows, width = heads.shape
    model = proj_a.shape[1]
    weights = []
    for apart in range(cores):
        weights += [proj_a, proj_b] if apart == 0 else [mirrored(proj_a, "c", apart), mirrored(proj_b, "c", apart)]
    where = jnp.stack([lax.axis_index("c"), lax.axis_index("z")]).astype(jnp.int32)
    step = math.gcd(model, 512)
    narrow = proj_b.shape[0] // (ways - heads_a)
    wide = proj_a.shape[0] // heads_a

    def body(at, heads_ref, *refs):
        sets, outs = refs[: 2 * cores], refs[2 * cores :]
        pairs = []
        for apart in range(cores):
            core = at[0] ^ apart

            def taken(head, used):
                found = [heads_ref[head, core, pl.ds((at[1] ^ far) * block, block), :] for far in range(lines)]
                return jnp.concatenate(found, axis=0)[:, :used]

            left_a = jnp.concatenate([taken(head, wide) for head in range(heads_a)], axis=1)
            left_b = jnp.concatenate([taken(head, narrow) for head in range(heads_a, ways)], axis=1)
            pairs += [(left_a, sets[2 * apart]), (left_b, sets[2 * apart + 1])]
        for first in range(0, model, step):
            span = slice(first, first + step)
            total = None
            for left, right in pairs:
                piece = jnp.dot(left, right[:, span], preferred_element_type=jnp.float32)
                total = piece if total is None else total + piece
            for far in range(lines):
                outs[far][:, span] = total[far * block : (far + 1) * block].astype(jnp.bfloat16)

    return whole_call(
        body,
        [((block, model), jnp.bfloat16)] * lines,
        "project",
        heads,
        *weights,
        scalars=(where,),
        flops=2 * rows * model * (proj_a.shape[0] + proj_b.shape[0]) * cores,
    )


def expert_hidden(rows_ref, gate_ref, up_ref, held, first, count):
    hidden = gate_ref.shape[1]
    tile = math.gcd(hidden, 256)
    for at in range(hidden // tile):
        span = slice(at * tile, (at + 1) * tile)
        gate = jnp.dot(rows_ref[pl.ds(first, count), :], gate_ref[:, span], preferred_element_type=jnp.float32)
        upward = jnp.dot(rows_ref[pl.ds(first, count), :], up_ref[:, span], preferred_element_type=jnp.float32)
        held[:, span] = (jax.nn.silu(gate) * upward).astype(jnp.bfloat16)


def expert_down(held, down_ref, out_ref, first, count):
    model = down_ref.shape[1]
    tile = math.gcd(model, 512)
    for at in range(model // tile):
        span = slice(at * tile, (at + 1) * tile)
        total = jnp.dot(held, down_ref[:, span], preferred_element_type=jnp.float32)
        out_ref[pl.ds(first, count), span] = total.astype(jnp.bfloat16)


def expert_call(name, rows, weights, out_cols, after=()):
    count = rows.shape[0]
    hidden = weights[-1].shape[0] if len(weights) != 2 else weights[0].shape[1]
    tile = math.gcd(count, 256)
    flops = 2 * count * sum(weight.size for weight in weights)

    def body(rows_ref, *refs):
        weight_refs, (out_ref, held) = refs[: len(weights)], refs[-2:]

        def step(index, carry):
            first = index * tile
            if len(weights) > 1:
                expert_hidden(rows_ref, *weight_refs[:2], held, first, tile)
            if len(weights) == 2:
                out_ref[pl.ds(first, tile), :] = held[...]
            else:
                left = held[...] if len(weights) == 3 else rows_ref[pl.ds(first, tile), :]
                expert_down(left, weight_refs[-1], out_ref, first, tile)
            return carry

        lax.fori_loop(0, count // tile, step, 0)

    (out,) = whole_call(
        body,
        [((count, out_cols), jnp.bfloat16)],
        name,
        rows,
        *weights,
        *after,
        flops=flops,
        scratch=[pltpu.VMEM((tile, hidden), jnp.bfloat16)],
    )
    return out


def exchanged_device(
    resid,
    query_a,
    key_a,
    value_a,
    query_b,
    key_b,
    value_b,
    mix_a,
    mix_b,
    head_gain_a,
    head_gain_b,
    proj_a,
    proj_b,
    norm_gain,
    route_ids,
    route_weights,
    expert_gate,
    expert_up,
    down_w,
):
    ways, lines, cores = (lax.axis_size(axis) for axis in ("sp", "z", "c"))
    place = lax.axis_index("sp")
    tok_rows, width = resid.shape
    top_count = route_ids.shape[1]
    capacity = 3 * top_count * tok_rows // (2 * ways)
    slots_all = ways * capacity
    low = jnp.bfloat16
    head_cols, back_cols = (width * part // 16 // 128 * 128 for part in (6, 5))
    tail_cols, rest_cols = width - head_cols, width - back_cols

    heads = exchanged_heads(
        query_a, key_a, value_a, query_b, key_b, value_b, mix_a, mix_b, head_gain_a, head_gain_b, tok_rows
    )

    slots = slot_numbers(route_ids ^ place, ways, capacity)
    routes = jnp.concatenate([jnp.transpose(slots).astype(jnp.float32), jnp.transpose(route_weights)], axis=0)
    line_routes = mirrored_all([routes] * lines, "z")

    def hits(routes_ref, which):
        lookup = lax.broadcasted_iota(jnp.int32, (slots_all, tok_rows), 0)
        return routes_ref[which : which + 1, :].astype(jnp.int32) == lookup

    def spread_rows(routes_ref, tokens):
        spread = sum(hits(routes_ref, which).astype(jnp.float32) for which in range(top_count)).astype(low)
        return jnp.dot(spread, tokens, preferred_element_type=jnp.float32).astype(low)

    def blend_rows(routes_ref, block):
        weights = sum(
            jnp.where(hits(routes_ref, which), routes_ref[top_count + which : top_count + which + 1, :], 0.0)
            for which in range(top_count)
        )
        upper = weights.astype(low)
        total = None
        for part in (upper, (weights - upper.astype(jnp.float32)).astype(low)):
            piece = lax.dot_general(part, block, (((0,), (0,)), ((), ())), preferred_element_type=jnp.float32)
            total = piece if total is None else total + piece
        return total

    parts = project(heads, proj_a, proj_b, lines, tok_rows, query_a.shape[1])
    parts = mirrored_all(parts, "z")

    def norm_body(*refs):
        part_refs, (resid_ref, gain_ref, routes_ref), outs = refs[:lines], refs[lines : lines + 3], refs[lines + 3 :]
        mixed = resid_ref[...].astype(jnp.float32)
        for part in part_refs:
            mixed = mixed + part[...].astype(jnp.float32)
        outs[0][...] = mixed
        normed = rms_scaled(mixed, gain_ref[...]).astype(low)
        outs[1][...] = normed[:, head_cols:]
        picked = spread_rows(routes_ref, normed[:, :head_cols])
        for far in range(ways):
            outs[2 + far][...] = picked[far * capacity : (far + 1) * capacity]

    mixed, tail, *heads_out = whole_call(
        norm_body,
        [((tok_rows, width), jnp.float32), ((tok_rows, tail_cols), low)] + [((capacity, head_cols), low)] * ways,
        "norm",
        *parts,
        resid,
        norm_gain[None, :],
        routes,
    )
    tails = mirrored_all([tail] * lines, "z")
    head_own = jnp.concatenate(mirrored_all(heads_out, "sp"), axis=0)
    head_blocks = mirrored_all([head_own] * lines, "z")

    weights = (expert_gate[0], expert_up[0], down_w[0])

    def spread_body(*refs):
        tail_refs, routes_refs, outs = refs[:lines], refs[lines : 2 * lines], refs[-ways:]
        for line in range(lines):
            picked = spread_rows(routes_refs[line], tail_refs[line][...])
            for far in range(ways):
                outs[far][line * capacity : (line + 1) * capacity] = picked[far * capacity : (far + 1) * capacity]

    tails_out = whole_call(
        spread_body, [((lines * capacity, tail_cols), low)] * ways, "spread", *tails, *line_routes, head_own, *weights[:2]
    )
    tail_blocks = mirrored_all(tails_out, "sp")

    def join_body(*refs):
        head_refs, tail_refs, (out,) = refs[:lines], refs[lines : lines + ways], refs[lines + ways :]
        for line in range(lines):
            for far in range(ways):
                first = line * slots_all + far * capacity
                out[first : first + capacity, :head_cols] = head_refs[line][far * capacity : (far + 1) * capacity]
                out[first : first + capacity, head_cols:] = tail_refs[far][line * capacity : (line + 1) * capacity]

    (rows,) = whole_call(join_body, [((lines * slots_all, width), low)], "join", *head_blocks, *tail_blocks)
    other_rows = [mirrored(rows, "c", apart) for apart in range(1, cores)]
    hidden = expert_call("hidden", rows, weights[:2], weights[0].shape[1])
    core_parts = [
        mirrored(expert_call("experts", other, weights, width, (hidden,)), "c", apart + 1)
        for apart, other in enumerate(other_rows)
    ]
    own_part = expert_call("down", hidden, weights[2:], width)

    def pair_body(*refs):
        part_refs, outs = refs[:cores], refs[cores:]
        for line in range(lines):
            for far in range(ways):
                first = line * slots_all + far * capacity
                total = part_refs[0][first : first + capacity].astype(jnp.float32)
                for part in part_refs[1:]:
                    total = total + part[first : first + capacity].astype(jnp.float32)
                total = total.astype(low)
                outs[line][far * capacity : (far + 1) * capacity] = total[:, :back_cols]
                outs[lines + far][line * capacity : (line + 1) * capacity] = total[:, back_cols:]

    back = whole_call(
        pair_body,
        [((slots_all, back_cols), low)] * lines + [((lines * capacity, rest_cols), low)] * ways,
        "pair",
        own_part,
        *core_parts,
    )
    tail_back = mirrored_all(back[lines:], "sp")
    head_back = mirrored_all(back[:lines], "z")

    def blend_body(*refs):
        tail_refs, routes_refs, outs = refs[:ways], refs[ways : ways + lines], refs[ways + lines :]
        for line in range(lines):
            block = jnp.concatenate([ref[line * capacity : (line + 1) * capacity] for ref in tail_refs], axis=0)
            outs[line][...] = blend_rows(routes_refs[line], block).astype(low)

    tail_sums = whole_call(blend_body, [((tok_rows, rest_cols), low)] * lines, "blend", *tail_back, *line_routes)
    tail_sums = mirrored_all(tail_sums, "z")

    def total_body(*refs):
        part_refs, outs = refs[:lines], refs[lines:]
        total = sum(part[...].astype(jnp.float32) for part in part_refs).astype(low)
        for far in range(ways):
            outs[far][...] = total[far * capacity : (far + 1) * capacity]

    head_sums = whole_call(total_body, [((capacity, back_cols), low)] * ways, "total", *head_back)
    head_sums = mirrored_all(head_sums, "sp")

    def final_body(mixed_ref, routes_ref, *refs):
        head_refs, tail_refs, (out,) = refs[:ways], refs[ways : ways + lines], refs[ways + lines :]
        block = jnp.concatenate([ref[...] for ref in head_refs], axis=0)
        total = mixed_ref[:, :back_cols] + blend_rows(routes_ref, block)
        out[:, :back_cols] = total.astype(low)
        total = mixed_ref[:, back_cols:]
        for ref in tail_refs:
            total = total + ref[...].astype(jnp.float32)
        out[:, back_cols:] = total.astype(low)

    (output,) = whole_call(
        final_body, [((tok_rows, width), low)], "final", mixed, routes, *head_sums, *tail_sums
    )
    return output


def placements(tp):
    both = ("sp",) + tp
    return (
        (
            P(both, None),
            P("sp", tp, None),
            P("sp", tp, None),
            P("sp", tp, None),
            P("sp", tp, None),
            P("sp", tp, None),
            P("sp", tp, None),
            P(tp),
            P(tp),
            P(),
            P(),
            P(tp, None),
            P(tp, None),
            P(),
            P(both, None),
            P(both, None),
            P("sp", None, tp),
            P("sp", None, tp),
            P("sp", tp, None),
        ),
        P(both, None),
    )


def solution(mesh):
    sp_ways, tp_ways = (mesh.shape[axis] for axis in ("sp", "tp"))
    cores = 2

    def program(*arrays):
        resid, query_a, query_b, route_ids = arrays[0], arrays[1], arrays[4], arrays[14]
        block = resid.shape[0] // (sp_ways * tp_ways)
        heads = (query_a.shape[1] + query_b.shape[1]) // tp_ways
        capacity = 3 * route_ids.shape[1] * block // (2 * sp_ways)
        fits = heads == sp_ways and capacity % 16 == 0 and block % 16 == 0 and resid.shape[1] % 2048 == 0
        if fits:
            devices = mesh.devices.reshape(sp_ways, tp_ways // cores, cores)
            inner, axes, body = Mesh(devices, ("sp", "z", "c")), ("z", "c"), exchanged_device
        else:
            inner, axes, body = mesh, ("tp",), gathered_device
        given, returned = placements(axes)
        return jax.shard_map(body, mesh=inner, in_specs=given, out_specs=returned, check_vma=False)(*arrays)

    return program
```

```python
import math

import jax
import jax.numpy as jnp
from jax import lax
from jax.experimental import pallas as pl
from jax.experimental.pallas import tpu as pltpu
from jax.sharding import Mesh, PartitionSpec as P


EPS = 1e-06
NEG = -1e30
HEAD_SCALE = 1.0 - (0.8 - 0.6 * math.exp(-0.3))
KEY_STEP = 512


def partner(value, axis, apart):
    return lax.ppermute(value, axis, [(i, i ^ 1 << apart) for i in range(lax.axis_size(axis))])


def rms_scaled(values, gain):
    return values * lax.rsqrt(jnp.mean(values * values, axis=-1, keepdims=True) + EPS) * gain


def slot_numbers(route_rows, experts, capacity):
    count, top_count = route_rows.shape
    flat = route_rows.reshape(count * top_count)
    onehot = (flat[:, None] == jnp.arange(experts, dtype=jnp.int32)[None, :]).astype(jnp.int32)
    ranks = jnp.sum((jnp.cumsum(onehot, axis=0) - onehot) * onehot, axis=1)
    return (flat * capacity + ranks).reshape(count, top_count)


def empty_map(count, heads, width):
    return (
        jnp.zeros((count, heads, width), jnp.float32),
        jnp.full((heads, count), NEG, jnp.float32),
        jnp.zeros((heads, count), jnp.float32),
    )


def empty_group(query, value):
    return (
        empty_map(query.shape[0], query.shape[1], value.shape[2]),
        empty_map(query.shape[0], query.shape[1], value.shape[2]),
    )


def map_update(state, query, keys, values, allowed, scale):
    weighted, maximum, sums = state
    scores = jnp.einsum("qhd,khd->hqk", query, keys, preferred_element_type=jnp.float32) * scale
    scores = jnp.where(allowed[None], scores, NEG)
    fresh = jnp.maximum(maximum, jnp.max(scores, axis=2))
    weights = jnp.where(allowed[None], jnp.exp(scores - fresh[:, :, None]), 0.0)
    factor = jnp.exp(maximum - fresh)
    sums = sums * factor + jnp.sum(weights, axis=2)
    added = jnp.einsum(
        "hqk,khv->qhv", weights.astype(jnp.bfloat16), values, preferred_element_type=jnp.float32
    )
    weighted = weighted * jnp.transpose(factor)[:, :, None] + added
    return (weighted, fresh, sums)


def group_update(states, query, keys, values, allowed):
    width = query.shape[2] // 2
    scale = 1.0 / math.sqrt(width)
    return tuple(
        (
            map_update(
                states[which],
                query[:, :, which * width : (which + 1) * width],
                keys[:, :, which * width : (which + 1) * width],
                values,
                allowed,
                scale,
            )
            for which in range(2)
        )
    )


def set_update(carry, queries, pieces):
    rows_a, rows_b, query_pos = queries
    piece_key_a, piece_value_a, piece_key_b, piece_value_b = pieces
    length = piece_key_a.shape[0]
    step = math.gcd(length, KEY_STEP)
    latest = query_pos[-1]

    def inner(index, states):
        first = index * step

        def compute(current):
            keys_a = lax.dynamic_slice_in_dim(piece_key_a, first, step, 0)
            values_a = lax.dynamic_slice_in_dim(piece_value_a, first, step, 0)
            keys_b = lax.dynamic_slice_in_dim(piece_key_b, first, step, 0)
            values_b = lax.dynamic_slice_in_dim(piece_value_b, first, step, 0)
            key_pos = first + jnp.arange(step, dtype=jnp.int32)
            allowed = key_pos[None, :] <= query_pos[:, None]
            return (
                group_update(current[0], rows_a, keys_a, values_a, allowed),
                group_update(current[1], rows_b, keys_b, values_b, allowed),
            )

        return lax.cond(first <= latest, compute, lambda current: current, states)

    return lax.fori_loop(0, length // step, inner, carry)


def finish_group(states, mix, gain):
    outputs = [state[0] / jnp.transpose(state[2])[:, :, None] for state in states]
    mixed = outputs[0] - mix[None, :, None] * outputs[1]
    normed = rms_scaled(mixed, gain) * HEAD_SCALE
    return normed.astype(jnp.bfloat16).reshape(mixed.shape[0], -1)


def gathered_device(
    resid,
    query_a,
    key_a,
    value_a,
    query_b,
    key_b,
    value_b,
    mix_a,
    mix_b,
    head_gain_a,
    head_gain_b,
    proj_a,
    proj_b,
    norm_gain,
    route_ids,
    route_weights,
    expert_gate,
    expert_up,
    expert_down,
):
    seq_rows = query_a.shape[0]
    sp_ways = lax.axis_size("sp")
    place = lax.axis_index("sp")
    positions = place * seq_rows + jnp.arange(seq_rows, dtype=jnp.int32)
    levels = sp_ways.bit_length() - 1
    half = seq_rows // 2
    moved = jnp.concatenate(
        [query_a[half:].reshape(half, -1), query_b[half:].reshape(half, -1)], axis=1
    )
    for bit in range(levels):
        moved = partner(moved, "sp", bit)
    split_at = query_a.shape[1] * query_a.shape[2]
    far_a = moved[:, :split_at].reshape(half, query_a.shape[1], query_a.shape[2])
    far_b = moved[:, split_at:].reshape(half, query_b.shape[1], query_b.shape[2])
    far_pos = (sp_ways - 1 - place) * seq_rows + half + jnp.arange(half, dtype=jnp.int32)
    query_sets = ((query_a[:half], query_b[:half], positions[:half]), (far_a, far_b, far_pos))

    def fold_keys(carry, pieces):
        return tuple(
            (set_update(states, queries, pieces) for states, queries in zip(carry, query_sets))
        )

    initial = tuple(
        (
            (empty_group(queries[0], value_a), empty_group(queries[1], value_b))
            for queries in query_sets
        )
    )
    results = fold_keys(
        initial,
        (
            lax.all_gather(key_a, "sp", axis=0, tiled=True),
            lax.all_gather(value_a, "sp", axis=0, tiled=True),
            lax.all_gather(key_b, "sp", axis=0, tiled=True),
            lax.all_gather(value_b, "sp", axis=0, tiled=True),
        ),
    )
    finished = [
        (finish_group(states[0], mix_a, head_gain_a), finish_group(states[1], mix_b, head_gain_b))
        for states in results
    ]
    returned = jnp.concatenate([finished[1][0], finished[1][1]], axis=1)
    for bit in range(levels):
        returned = partner(returned, "sp", bit)
    width_a = finished[0][0].shape[1]
    heads_out_a = jnp.concatenate([finished[0][0], returned[:, :width_a]], axis=0)
    heads_out_b = jnp.concatenate([finished[0][1], returned[:, width_a:]], axis=0)
    width = resid.shape[1]
    tok_rows = resid.shape[0]
    top_count = route_ids.shape[1]
    capacity = 3 * top_count * tok_rows // (2 * sp_ways)
    own_slots = slot_numbers(route_ids, sp_ways, capacity)
    term = jnp.dot(heads_out_a, proj_a, preferred_element_type=jnp.float32)
    term = term + jnp.dot(heads_out_b, proj_b, preferred_element_type=jnp.float32)
    mixed = resid.astype(jnp.float32) + lax.psum_scatter(
        lax.optimization_barrier(term.astype(jnp.bfloat16))
        .astype(jnp.float32)
        .astype(jnp.bfloat16),
        "tp",
        scatter_dimension=0,
        tiled=True,
    ).astype(jnp.float32)
    normed = rms_scaled(mixed, norm_gain).astype(jnp.bfloat16)
    lookup = jnp.arange(sp_ways * capacity, dtype=jnp.int32)[:, None]
    spread = jnp.zeros((sp_ways * capacity, tok_rows), jnp.float32)
    for which in range(top_count):
        spread = spread + (own_slots[:, which][None, :] == lookup).astype(jnp.float32)
    outgoing = jnp.dot(
        spread.astype(jnp.bfloat16), normed, preferred_element_type=jnp.float32
    ).astype(jnp.bfloat16)
    arrived = lax.all_to_all(
        outgoing.reshape(sp_ways, capacity, width), "sp", split_axis=0, concat_axis=0, tiled=True
    )
    piece = lax.all_gather(arrived.reshape(sp_ways * capacity, width), "tp", axis=0, tiled=True)
    gate = jnp.dot(piece, expert_gate[0], preferred_element_type=jnp.float32)
    upward = jnp.dot(piece, expert_up[0], preferred_element_type=jnp.float32)
    hidden = (jax.nn.silu(gate) * upward).astype(jnp.bfloat16)
    term = jnp.dot(hidden, expert_down[0], preferred_element_type=jnp.float32)
    summed = lax.psum_scatter(
        lax.optimization_barrier(term.astype(jnp.bfloat16))
        .astype(jnp.float32)
        .astype(jnp.bfloat16),
        "tp",
        scatter_dimension=0,
        tiled=True,
    )
    finished_rows = summed.reshape(sp_ways, capacity, width)
    back = lax.all_to_all(finished_rows, "sp", split_axis=0, concat_axis=0, tiled=True)
    picked = jnp.take(back.reshape(sp_ways * capacity, width), own_slots.reshape(-1), axis=0)
    picked = picked.reshape(tok_rows, top_count, width)
    output = mixed + jnp.sum(route_weights[:, :, None] * picked.astype(jnp.float32), axis=1)
    return output.astype(jnp.bfloat16)


def attend_kernel(scalars, own, gain, *refs, step, width, maps, block):
    pieces, (out, scores, packed) = refs[:-3], refs[-3:]
    place = pl.program_id(0)
    coef = scalars[0]

    @pl.when(place == 0)
    def _():
        for far, piece in enumerate(pieces):
            packed[own[0] ^ far] = piece[...]

    queries = [jnp.transpose(packed[place, 2 * which * maps : (2 * which + 1) * maps, :]) for which in range(2)]

    def fold(values, combine):
        parts = [values[:, at * width : (at + 1) * width] for at in range(step // width)]
        while len(parts) > 1:
            parts = [combine(*parts[at : at + 2]) for at in range(0, len(parts), 2)]
        return parts[0]

    def raw(which, index):
        keys = packed[index, (2 * which + 1) * maps : (2 * which + 2) * maps, :]
        return jnp.dot(queries[which], keys, preferred_element_type=jnp.float32)

    row = lax.broadcasted_iota(jnp.int32, (step, step), 0)
    column = lax.broadcasted_iota(jnp.int32, (step, step), 1)
    highest = []
    for which in range(2):
        diagonal = jnp.where(column <= row, raw(which, place), NEG)
        scores[which, place] = diagonal
        highest.append(fold(diagonal, jnp.maximum))

    def first_pass(index, carry):
        found = []
        for which in range(2):
            values = raw(which, index)
            scores[which, index] = values
            found.append(jnp.maximum(carry[which], fold(values, jnp.maximum)))
        return tuple(found)

    highest = lax.fori_loop(0, place, first_pass, tuple(highest))
    tops = [jnp.max(found, axis=1, keepdims=True) * coef for found in highest]

    def second_pass(index, carry):
        values = packed[index, 4 * maps : 4 * maps + width, :]
        found = []
        for which in range(2):
            total, mixed = carry[which]
            weights = jnp.exp2(scores[which, index] * coef - tops[which])
            total = total + fold(weights, jnp.add)
            mixed = mixed + lax.dot_general(
                weights.astype(jnp.bfloat16),
                values,
                (((1,), (1,)), ((), ())),
                preferred_element_type=jnp.float32,
            )
            found.append((total, mixed))
        return tuple(found)

    empty = jnp.zeros((step, width), jnp.float32)
    found = lax.fori_loop(0, place + 1, second_pass, ((empty, empty), (empty, empty)))
    outputs = [mixed / jnp.sum(total, axis=1, keepdims=True) for total, mixed in found]
    mixed = outputs[0] - scalars[1] * outputs[1]
    square = jnp.sum(mixed * mixed, axis=1, keepdims=True) * scalars[2]
    normed = (mixed * lax.rsqrt(square + EPS) * gain[...]).astype(jnp.bfloat16)
    cores = out.shape[1]
    for at in range(step // block):
        begin = at // cores * block
        out[0, at % cores, begin : begin + block] = normed[at * block : (at + 1) * block]


def widen(values, width):
    missing = width - values.shape[-1]
    return jnp.pad(values, [(0, 0)] * (values.ndim - 1) + [(0, missing)]) if missing else values


def fast_memory(limit_mib):
    return pltpu.CompilerParams(vmem_limit_bytes=limit_mib << 20)


def mirrored(value, axis, apart):
    return lax.ppermute(value, axis, [(i, i ^ apart) for i in range(lax.axis_size(axis))])


def mirrored_all(values, axis):
    found = {far: mirrored(values[far], axis, far) for far in reversed(range(1, len(values)))}
    return [values[0]] + [found[far] for far in range(1, len(values))]


def whole_call(body, outs, *operands, scalars=(), flops=0, scratch=(), limit=8):
    vmem = pl.BlockSpec(memory_space=pltpu.VMEM)
    return pl.pallas_call(
        body,
        in_specs=[pl.BlockSpec(memory_space=pltpu.SMEM)] * len(scalars) + [vmem] * len(operands),
        out_specs=[vmem] * len(outs),
        out_shape=[pltpu.VMEM(shape, dtype) for shape, dtype in outs],
        scratch_shapes=scratch,
        compiler_params=fast_memory(limit),
        cost_estimate=pl.CostEstimate(flops=flops, bytes_accessed=0, transcendentals=0),
    )(*scalars, *[pltpu.with_memory_space_constraint(operand, pltpu.VMEM) for operand in operands])


def exchanged_heads(query_a, key_a, value_a, query_b, key_b, value_b, mix_a, mix_b, head_gain_a, head_gain_b, block):
    seq_rows, heads_a, _ = query_a.shape
    ways = lax.axis_size("sp")
    cores = lax.axis_size("c")
    place = lax.axis_index("sp")
    groups = ((query_a, key_a, value_a), (query_b, key_b, value_b))
    width = -(-max(group[2].shape[2] for group in groups) // 128) * 128
    maps = -(-max(group[0].shape[2] // 2 for group in groups) // 16) * 16

    def filled(array, size):
        return jnp.pad(array, ((0, 0), (0, size - array.shape[1]), (0, 0)))

    turned = lax.optimization_barrier([[jnp.transpose(array, (1, 2, 0)) for array in group] for group in groups])
    outgoing = []
    for query, key, value in turned:
        half = query.shape[1] // 2
        split = [array[:, first : first + half] for first in (0, half) for array in (query, key)]
        outgoing.append(jnp.concatenate([filled(array, maps) for array in split] + [filled(value, width)], axis=1))
    outgoing = jnp.concatenate(outgoing, axis=0)
    pieces = [lax.dynamic_index_in_dim(outgoing, place ^ far, 0, False) for far in range(ways)]
    pieces = mirrored_all(pieces, "sp")
    first = place < heads_a
    gain = jnp.where(first, widen(head_gain_a, width), widen(head_gain_b, width)) * HEAD_SCALE
    coef_a, coef_b = [math.log2(math.e) / math.sqrt(group[0].shape[2] // 2) for group in groups]
    scalars = jnp.stack(
        [
            jnp.where(first, coef_a, coef_b).astype(jnp.float32),
            lax.dynamic_index_in_dim(jnp.concatenate([mix_a, mix_b]), place, 0, False),
            jnp.where(first, 1.0 / value_a.shape[2], 1.0 / value_b.shape[2]).astype(jnp.float32),
        ]
    )
    pairs = (ways * seq_rows) * (ways + 1) * seq_rows
    shape = (ways, cores, seq_rows // cores, width)
    smem = pl.BlockSpec(memory_space=pltpu.SMEM)
    mixed = pl.pallas_call(
        lambda *refs: attend_kernel(*refs, step=seq_rows, width=width, maps=maps, block=block),
        grid=(ways,),
        in_specs=[smem, smem, pl.BlockSpec((1, width), lambda index: (0, 0))]
        + [pl.BlockSpec(piece.shape, lambda index: (0, 0)) for piece in pieces],
        out_specs=pl.BlockSpec((1,) + shape[1:], lambda index: (index, 0, 0, 0)),
        out_shape=pltpu.HBM(shape, jnp.bfloat16),
        scratch_shapes=[
            pltpu.VMEM((2, ways, seq_rows, seq_rows), jnp.float32),
            pltpu.VMEM((ways,) + pieces[0].shape, jnp.bfloat16),
        ],
        compiler_params=pltpu.CompilerParams(dimension_semantics=("arbitrary",), vmem_limit_bytes=24 << 20),
        cost_estimate=pl.CostEstimate(flops=2 * pairs * (maps + width), bytes_accessed=0, transcendentals=pairs),
        name="attend",
    )(scalars, place[None].astype(jnp.int32), gain[None, :], *pieces)
    flat = mixed.reshape((ways * cores,) + shape[2:])
    return lax.all_to_all(flat, ("sp", "c"), split_axis=0, concat_axis=0, tiled=True).reshape(shape)


def project(heads, proj_a, proj_b, lines, block, heads_a):
    ways, cores, rows, _ = heads.shape
    model = proj_a.shape[1]
    weights = []
    for apart in range(cores):
        weights += [proj_a, proj_b] if apart == 0 else [mirrored(proj_a, "c", apart), mirrored(proj_b, "c", apart)]
    where = jnp.stack([lax.axis_index("c"), lax.axis_index("z")]).astype(jnp.int32)
    step = math.gcd(model, 512)
    narrow = proj_b.shape[0] // (ways - heads_a)
    wide = proj_a.shape[0] // heads_a

    def body(at, heads_ref, *refs):
        sets, outs = refs[: 2 * cores], refs[2 * cores :]
        pairs = []
        for apart in range(cores):
            core = at[0] ^ apart

            def taken(head, used):
                found = [heads_ref[head, core, pl.ds((at[1] ^ far) * block, block), :] for far in range(lines)]
                return jnp.concatenate(found, axis=0)[:, :used]

            left_a = jnp.concatenate([taken(head, wide) for head in range(heads_a)], axis=1)
            left_b = jnp.concatenate([taken(head, narrow) for head in range(heads_a, ways)], axis=1)
            pairs += [(left_a, sets[2 * apart]), (left_b, sets[2 * apart + 1])]
        for first in range(0, model, step):
            span = slice(first, first + step)
            total = None
            for left, right in pairs:
                piece = jnp.dot(left, right[:, span], preferred_element_type=jnp.float32)
                total = piece if total is None else total + piece
            for far in range(lines):
                outs[far][:, span] = total[far * block : (far + 1) * block].astype(jnp.bfloat16)

    return whole_call(
        body,
        [((block, model), jnp.bfloat16)] * lines,
        heads,
        *weights,
        scalars=(where,),
        flops=2 * rows * model * (proj_a.shape[0] + proj_b.shape[0]) * cores,
    )


def expert_hidden(rows_ref, gate_ref, up_ref, held, first, count):
    hidden = gate_ref.shape[1]
    tile = math.gcd(hidden, 256)
    for at in range(hidden // tile):
        span = slice(at * tile, (at + 1) * tile)
        gate = jnp.dot(rows_ref[pl.ds(first, count), :], gate_ref[:, span], preferred_element_type=jnp.float32)
        upward = jnp.dot(rows_ref[pl.ds(first, count), :], up_ref[:, span], preferred_element_type=jnp.float32)
        held[:, span] = (jax.nn.silu(gate) * upward).astype(jnp.bfloat16)


def expert_down(held, down_ref, out_ref, first, count):
    model = down_ref.shape[1]
    tile = math.gcd(model, 512)
    for at in range(model // tile):
        span = slice(at * tile, (at + 1) * tile)
        total = jnp.dot(held, down_ref[:, span], preferred_element_type=jnp.float32)
        out_ref[pl.ds(first, count), span] = total.astype(jnp.bfloat16)


def expert_call(rows, weights, out_cols, after=()):
    count = rows.shape[0]
    hidden = weights[-1].shape[0] if len(weights) != 2 else weights[0].shape[1]
    tile = max(size for size in range(16, 257, 16) if count % size == 0)
    flops = 2 * count * sum(weight.size for weight in weights)

    def body(rows_ref, *refs):
        weight_refs, (out_ref, held) = refs[: len(weights)], refs[-2:]

        def step(index, carry):
            first = index * tile
            if len(weights) > 1:
                expert_hidden(rows_ref, *weight_refs[:2], held, first, tile)
            if len(weights) == 2:
                out_ref[pl.ds(first, tile), :] = held[...]
            else:
                left = held[...] if len(weights) == 3 else rows_ref[pl.ds(first, tile), :]
                expert_down(left, weight_refs[-1], out_ref, first, tile)
            return carry

        lax.fori_loop(0, count // tile, step, 0)

    (out,) = whole_call(
        body,
        [((count, out_cols), jnp.bfloat16)],
        rows,
        *weights,
        *after,
        flops=flops,
        scratch=[pltpu.VMEM((tile, hidden), jnp.bfloat16)],
    )
    return out


def exchanged_device(
    resid,
    query_a,
    key_a,
    value_a,
    query_b,
    key_b,
    value_b,
    mix_a,
    mix_b,
    head_gain_a,
    head_gain_b,
    proj_a,
    proj_b,
    norm_gain,
    route_ids,
    route_weights,
    expert_gate,
    expert_up,
    down_w,
):
    ways, lines, cores = (lax.axis_size(axis) for axis in ("sp", "z", "c"))
    place = lax.axis_index("sp")
    tok_rows, width = resid.shape
    top_count = route_ids.shape[1]
    capacity = 3 * top_count * tok_rows // (2 * ways)
    slots_all = ways * capacity
    low = jnp.bfloat16
    head_cols, back_cols = (width * part // 16 // 128 * 128 for part in (6, 5))
    tail_cols, rest_cols = width - head_cols, width - back_cols

    heads = exchanged_heads(
        query_a, key_a, value_a, query_b, key_b, value_b, mix_a, mix_b, head_gain_a, head_gain_b, tok_rows
    )

    slots = slot_numbers(route_ids ^ place, ways, capacity)
    routes = jnp.concatenate([jnp.transpose(slots).astype(jnp.float32), jnp.transpose(route_weights)], axis=0)
    line_routes = mirrored_all([routes] * lines, "z")

    def hits(routes_ref, which):
        lookup = lax.broadcasted_iota(jnp.int32, (slots_all, tok_rows), 0)
        return routes_ref[which : which + 1, :].astype(jnp.int32) == lookup

    def spread_rows(routes_ref, tokens):
        spread = sum(hits(routes_ref, which).astype(jnp.float32) for which in range(top_count)).astype(low)
        return jnp.dot(spread, tokens, preferred_element_type=jnp.float32).astype(low)

    def blend_rows(routes_ref, block):
        weights = sum(
            jnp.where(hits(routes_ref, which), routes_ref[top_count + which : top_count + which + 1, :], 0.0)
            for which in range(top_count)
        )
        upper = weights.astype(low)
        total = None
        for part in (upper, (weights - upper.astype(jnp.float32)).astype(low)):
            piece = lax.dot_general(part, block, (((0,), (0,)), ((), ())), preferred_element_type=jnp.float32)
            total = piece if total is None else total + piece
        return total

    parts = project(heads, proj_a, proj_b, lines, tok_rows, query_a.shape[1])
    parts = mirrored_all(parts, "z")

    def norm_body(*refs):
        part_refs, (resid_ref, gain_ref, routes_ref), outs = refs[:lines], refs[lines : lines + 3], refs[lines + 3 :]
        mixed = resid_ref[...].astype(jnp.float32)
        for part in part_refs:
            mixed = mixed + part[...].astype(jnp.float32)
        outs[0][...] = mixed
        normed = rms_scaled(mixed, gain_ref[...]).astype(low)
        outs[1][...] = normed[:, head_cols:]
        picked = spread_rows(routes_ref, normed[:, :head_cols])
        for far in range(ways):
            outs[2 + far][...] = picked[far * capacity : (far + 1) * capacity]

    mixed, tail, *heads_out = whole_call(
        norm_body,
        [((tok_rows, width), jnp.float32), ((tok_rows, tail_cols), low)] + [((capacity, head_cols), low)] * ways,
        *parts,
        resid,
        norm_gain[None, :],
        routes,
    )
    tails = mirrored_all([tail] * lines, "z")
    heads_in = mirrored_all(heads_out, "sp")
    groups = {"near": list(range(ways - 1)), "far": [ways - 1]}
    head_blocks = {}
    for group, members in groups.items():
        block = heads_in[members[0]]
        if len(members) > 1:
            block = jnp.concatenate([heads_in[far] for far in members], axis=0)
        head_blocks[group] = mirrored_all([block] * lines, "z")

    weights = (expert_gate[0], expert_up[0], down_w[0])

    def spread_body(*refs):
        tail_refs, routes_refs, outs = refs[:lines], refs[lines : 2 * lines], refs[-ways:]
        for line in range(lines):
            picked = spread_rows(routes_refs[line], tail_refs[line][...])
            for far in range(ways):
                outs[far][line * capacity : (line + 1) * capacity] = picked[far * capacity : (far + 1) * capacity]

    tail_blocks = list(
        whole_call(
            spread_body,
            [((lines * capacity, tail_cols), low)] * ways,
            *tails,
            *line_routes,
            head_blocks["near"][0],
            *weights[:2],
        )
    )
    for members in groups.values():
        for far in members:
            if far > 0:
                tail_blocks[far] = mirrored(tail_blocks[far], "sp", far)

    def join(group, *after):
        members = groups[group]

        def body(*refs):
            head_refs, tail_refs, out = refs[:lines], refs[lines : lines + len(members)], refs[-1]
            for line in range(lines):
                for at in range(len(members)):
                    first = (line * len(members) + at) * capacity
                    out[first : first + capacity, :head_cols] = head_refs[line][at * capacity : (at + 1) * capacity]
                    out[first : first + capacity, head_cols:] = tail_refs[at][line * capacity : (line + 1) * capacity]

        (rows,) = whole_call(
            body,
            [((lines * len(members) * capacity, width), low)],
            *head_blocks[group],
            *[tail_blocks[far] for far in members],
            *after,
        )
        return rows

    def pair(group, own_part, other_parts):
        members = groups[group]

        def body(*refs):
            part_refs, outs = refs[:cores], refs[cores:]
            for line in range(lines):
                for at in range(len(members)):
                    first = (line * len(members) + at) * capacity
                    total = part_refs[0][first : first + capacity].astype(jnp.float32)
                    for part in part_refs[1:]:
                        total = total + part[first : first + capacity].astype(jnp.float32)
                    total = total.astype(low)
                    outs[line][at * capacity : (at + 1) * capacity] = total[:, :back_cols]
                    outs[lines + at][line * capacity : (line + 1) * capacity] = total[:, back_cols:]

        count = len(members)
        return whole_call(
            body,
            [((count * capacity, back_cols), low)] * lines + [((lines * capacity, rest_cols), low)] * count,
            own_part,
            *other_parts,
        )

    assert cores == 2
    tail_back, head_back, before = {}, {}, ()
    for group, members in groups.items():
        rows = join(group, *before)
        other_rows = mirrored(rows, "c", 1)
        hidden = expert_call(rows, weights[:2], weights[0].shape[1])
        after = (hidden,) + tuple(head_back[done][0] for done in head_back)
        other_part = expert_call(other_rows, weights, width, after)
        own_part = expert_call(hidden, weights[2:], width)
        back = pair(group, own_part, [mirrored(other_part, "c", 1)])
        for at, far in reversed(list(enumerate(members))):
            tail_back[far] = mirrored(back[lines + at], "sp", far) if far else back[lines + at]
        head_back[group] = mirrored_all(back[:lines], "z")
        before = (other_part,)
    tail_back = [tail_back[far] for far in range(ways)]

    def blend_body(*refs):
        tail_refs, routes_refs, outs = refs[:ways], refs[ways : ways + lines], refs[ways + lines :]
        for line in range(lines):
            block = jnp.concatenate([ref[line * capacity : (line + 1) * capacity] for ref in tail_refs], axis=0)
            outs[line][...] = blend_rows(routes_refs[line], block).astype(low)

    tail_sums = whole_call(blend_body, [((tok_rows, rest_cols), low)] * lines, *tail_back, *line_routes)
    tail_sums = mirrored_all(tail_sums, "z")

    def total_body(*refs):
        at = 0
        for members in groups.values():
            part_refs = refs[at : at + lines]
            at += lines
            total = sum(part[...].astype(jnp.float32) for part in part_refs).astype(low)
            for index, far in enumerate(members):
                refs[far - ways][...] = total[index * capacity : (index + 1) * capacity]

    head_sums = whole_call(
        total_body, [((capacity, back_cols), low)] * ways, *[block for group in groups for block in head_back[group]]
    )
    head_sums = mirrored_all(head_sums, "sp")

    def final_body(mixed_ref, routes_ref, *refs):
        head_refs, tail_refs, (out,) = refs[:ways], refs[ways : ways + lines], refs[ways + lines :]
        block = jnp.concatenate([ref[...] for ref in head_refs], axis=0)
        total = mixed_ref[:, :back_cols] + blend_rows(routes_ref, block)
        out[:, :back_cols] = total.astype(low)
        total = mixed_ref[:, back_cols:]
        for ref in tail_refs:
            total = total + ref[...].astype(jnp.float32)
        out[:, back_cols:] = total.astype(low)

    (output,) = whole_call(final_body, [((tok_rows, width), low)], mixed, routes, *head_sums, *tail_sums)
    return output


def placements(tp):
    both = ("sp",) + tp
    return (
        (
            P(both, None),
            P("sp", tp, None),
            P("sp", tp, None),
            P("sp", tp, None),
            P("sp", tp, None),
            P("sp", tp, None),
            P("sp", tp, None),
            P(tp),
            P(tp),
            P(),
            P(),
            P(tp, None),
            P(tp, None),
            P(),
            P(both, None),
            P(both, None),
            P("sp", None, tp),
            P("sp", None, tp),
            P("sp", tp, None),
        ),
        P(both, None),
    )


def solution(mesh):
    sp_ways, tp_ways = (mesh.shape[axis] for axis in ("sp", "tp"))
    cores = 2

    def program(*arrays):
        resid, query_a, query_b, route_ids = arrays[0], arrays[1], arrays[4], arrays[14]
        block = resid.shape[0] // (sp_ways * tp_ways)
        heads = (query_a.shape[1] + query_b.shape[1]) // tp_ways
        capacity = 3 * route_ids.shape[1] * block // (2 * sp_ways)
        fits = heads == sp_ways and capacity % 16 == 0 and block % 16 == 0 and resid.shape[1] % 2048 == 0
        if fits:
            devices = mesh.devices.reshape(sp_ways, tp_ways // cores, cores)
            inner, axes = Mesh(devices, ("sp", "z", "c")), ("z", "c")

            def body(*parts):
                return exchanged_device(*parts)

        else:
            inner, axes, body = mesh, ("tp",), gathered_device
        given, returned = placements(axes)
        mapped = jax.shard_map(body, mesh=inner, in_specs=given, out_specs=returned, check_vma=False)
        return mapped(*arrays)

    return program
```

```python
import math

import jax
import jax.numpy as jnp
from jax import lax
from jax.experimental import pallas as pl
from jax.experimental.pallas import tpu as pltpu
from jax.sharding import Mesh, PartitionSpec as P


EPS = 1e-06
NEG = -1e30
HEAD_SCALE = 1.0 - (0.8 - 0.6 * math.exp(-0.3))
KEY_STEP = 512


def partner(value, axis, apart):
    return lax.ppermute(value, axis, [(i, i ^ 1 << apart) for i in range(lax.axis_size(axis))])


def rms_scaled(values, gain):
    return values * lax.rsqrt(jnp.mean(values * values, axis=-1, keepdims=True) + EPS) * gain


def slot_numbers(route_rows, experts, capacity):
    count, top_count = route_rows.shape
    flat = route_rows.reshape(count * top_count)
    onehot = (flat[:, None] == jnp.arange(experts, dtype=jnp.int32)[None, :]).astype(jnp.int32)
    ranks = jnp.sum((jnp.cumsum(onehot, axis=0) - onehot) * onehot, axis=1)
    return (flat * capacity + ranks).reshape(count, top_count)


def empty_map(count, heads, width):
    return (
        jnp.zeros((count, heads, width), jnp.float32),
        jnp.full((heads, count), NEG, jnp.float32),
        jnp.zeros((heads, count), jnp.float32),
    )


def empty_group(query, value):
    return (
        empty_map(query.shape[0], query.shape[1], value.shape[2]),
        empty_map(query.shape[0], query.shape[1], value.shape[2]),
    )


def map_update(state, query, keys, values, allowed, scale):
    weighted, maximum, sums = state
    scores = jnp.einsum("qhd,khd->hqk", query, keys, preferred_element_type=jnp.float32) * scale
    scores = jnp.where(allowed[None], scores, NEG)
    fresh = jnp.maximum(maximum, jnp.max(scores, axis=2))
    weights = jnp.where(allowed[None], jnp.exp(scores - fresh[:, :, None]), 0.0)
    factor = jnp.exp(maximum - fresh)
    sums = sums * factor + jnp.sum(weights, axis=2)
    added = jnp.einsum(
        "hqk,khv->qhv", weights.astype(jnp.bfloat16), values, preferred_element_type=jnp.float32
    )
    weighted = weighted * jnp.transpose(factor)[:, :, None] + added
    return (weighted, fresh, sums)


def group_update(states, query, keys, values, allowed):
    width = query.shape[2] // 2
    scale = 1.0 / math.sqrt(width)
    return tuple(
        (
            map_update(
                states[which],
                query[:, :, which * width : (which + 1) * width],
                keys[:, :, which * width : (which + 1) * width],
                values,
                allowed,
                scale,
            )
            for which in range(2)
        )
    )


def set_update(carry, queries, pieces):
    rows_a, rows_b, query_pos = queries
    piece_key_a, piece_value_a, piece_key_b, piece_value_b = pieces
    length = piece_key_a.shape[0]
    step = math.gcd(length, KEY_STEP)
    latest = query_pos[-1]

    def inner(index, states):
        first = index * step

        def compute(current):
            keys_a = lax.dynamic_slice_in_dim(piece_key_a, first, step, 0)
            values_a = lax.dynamic_slice_in_dim(piece_value_a, first, step, 0)
            keys_b = lax.dynamic_slice_in_dim(piece_key_b, first, step, 0)
            values_b = lax.dynamic_slice_in_dim(piece_value_b, first, step, 0)
            key_pos = first + jnp.arange(step, dtype=jnp.int32)
            allowed = key_pos[None, :] <= query_pos[:, None]
            return (
                group_update(current[0], rows_a, keys_a, values_a, allowed),
                group_update(current[1], rows_b, keys_b, values_b, allowed),
            )

        return lax.cond(first <= latest, compute, lambda current: current, states)

    return lax.fori_loop(0, length // step, inner, carry)


def finish_group(states, mix, gain):
    outputs = [state[0] / jnp.transpose(state[2])[:, :, None] for state in states]
    mixed = outputs[0] - mix[None, :, None] * outputs[1]
    normed = rms_scaled(mixed, gain) * HEAD_SCALE
    return normed.astype(jnp.bfloat16).reshape(mixed.shape[0], -1)


def gathered_device(
    resid,
    query_a,
    key_a,
    value_a,
    query_b,
    key_b,
    value_b,
    mix_a,
    mix_b,
    head_gain_a,
    head_gain_b,
    proj_a,
    proj_b,
    norm_gain,
    route_ids,
    route_weights,
    expert_gate,
    expert_up,
    expert_down,
):
    seq_rows = query_a.shape[0]
    sp_ways = lax.axis_size("sp")
    place = lax.axis_index("sp")
    positions = place * seq_rows + jnp.arange(seq_rows, dtype=jnp.int32)
    levels = sp_ways.bit_length() - 1
    half = seq_rows // 2
    moved = jnp.concatenate(
        [query_a[half:].reshape(half, -1), query_b[half:].reshape(half, -1)], axis=1
    )
    for bit in range(levels):
        moved = partner(moved, "sp", bit)
    split_at = query_a.shape[1] * query_a.shape[2]
    far_a = moved[:, :split_at].reshape(half, query_a.shape[1], query_a.shape[2])
    far_b = moved[:, split_at:].reshape(half, query_b.shape[1], query_b.shape[2])
    far_pos = (sp_ways - 1 - place) * seq_rows + half + jnp.arange(half, dtype=jnp.int32)
    query_sets = ((query_a[:half], query_b[:half], positions[:half]), (far_a, far_b, far_pos))

    def fold_keys(carry, pieces):
        return tuple(
            (set_update(states, queries, pieces) for states, queries in zip(carry, query_sets))
        )

    initial = tuple(
        (
            (empty_group(queries[0], value_a), empty_group(queries[1], value_b))
            for queries in query_sets
        )
    )
    results = fold_keys(
        initial,
        (
            lax.all_gather(key_a, "sp", axis=0, tiled=True),
            lax.all_gather(value_a, "sp", axis=0, tiled=True),
            lax.all_gather(key_b, "sp", axis=0, tiled=True),
            lax.all_gather(value_b, "sp", axis=0, tiled=True),
        ),
    )
    finished = [
        (finish_group(states[0], mix_a, head_gain_a), finish_group(states[1], mix_b, head_gain_b))
        for states in results
    ]
    returned = jnp.concatenate([finished[1][0], finished[1][1]], axis=1)
    for bit in range(levels):
        returned = partner(returned, "sp", bit)
    width_a = finished[0][0].shape[1]
    heads_out_a = jnp.concatenate([finished[0][0], returned[:, :width_a]], axis=0)
    heads_out_b = jnp.concatenate([finished[0][1], returned[:, width_a:]], axis=0)
    width = resid.shape[1]
    tok_rows = resid.shape[0]
    top_count = route_ids.shape[1]
    capacity = 3 * top_count * tok_rows // (2 * sp_ways)
    own_slots = slot_numbers(route_ids, sp_ways, capacity)
    term = jnp.dot(heads_out_a, proj_a, preferred_element_type=jnp.float32)
    term = term + jnp.dot(heads_out_b, proj_b, preferred_element_type=jnp.float32)
    mixed = resid.astype(jnp.float32) + lax.psum_scatter(
        lax.optimization_barrier(term.astype(jnp.bfloat16))
        .astype(jnp.float32)
        .astype(jnp.bfloat16),
        "tp",
        scatter_dimension=0,
        tiled=True,
    ).astype(jnp.float32)
    normed = rms_scaled(mixed, norm_gain).astype(jnp.bfloat16)
    lookup = jnp.arange(sp_ways * capacity, dtype=jnp.int32)[:, None]
    spread = jnp.zeros((sp_ways * capacity, tok_rows), jnp.float32)
    for which in range(top_count):
        spread = spread + (own_slots[:, which][None, :] == lookup).astype(jnp.float32)
    outgoing = jnp.dot(
        spread.astype(jnp.bfloat16), normed, preferred_element_type=jnp.float32
    ).astype(jnp.bfloat16)
    arrived = lax.all_to_all(
        outgoing.reshape(sp_ways, capacity, width), "sp", split_axis=0, concat_axis=0, tiled=True
    )
    piece = lax.all_gather(arrived.reshape(sp_ways * capacity, width), "tp", axis=0, tiled=True)
    gate = jnp.dot(piece, expert_gate[0], preferred_element_type=jnp.float32)
    upward = jnp.dot(piece, expert_up[0], preferred_element_type=jnp.float32)
    hidden = (jax.nn.silu(gate) * upward).astype(jnp.bfloat16)
    term = jnp.dot(hidden, expert_down[0], preferred_element_type=jnp.float32)
    summed = lax.psum_scatter(
        lax.optimization_barrier(term.astype(jnp.bfloat16))
        .astype(jnp.float32)
        .astype(jnp.bfloat16),
        "tp",
        scatter_dimension=0,
        tiled=True,
    )
    finished_rows = summed.reshape(sp_ways, capacity, width)
    back = lax.all_to_all(finished_rows, "sp", split_axis=0, concat_axis=0, tiled=True)
    picked = jnp.take(back.reshape(sp_ways * capacity, width), own_slots.reshape(-1), axis=0)
    picked = picked.reshape(tok_rows, top_count, width)
    output = mixed + jnp.sum(route_weights[:, :, None] * picked.astype(jnp.float32), axis=1)
    return output.astype(jnp.bfloat16)


def attend_kernel(scalars, own, gain, *refs, step, width, maps, block):
    pieces, (out, scores, packed) = refs[:-3], refs[-3:]
    place = pl.program_id(0)
    coef = scalars[0]

    @pl.when(place == 0)
    def _():
        for far, piece in enumerate(pieces):
            packed[own[0] ^ far] = piece[...]

    queries = [jnp.transpose(packed[place, 2 * which * maps : (2 * which + 1) * maps, :]) for which in range(2)]

    def fold(values, combine):
        parts = [values[:, at * width : (at + 1) * width] for at in range(step // width)]
        while len(parts) > 1:
            parts = [combine(*parts[at : at + 2]) for at in range(0, len(parts), 2)]
        return parts[0]

    def raw(which, index):
        keys = packed[index, (2 * which + 1) * maps : (2 * which + 2) * maps, :]
        return jnp.dot(queries[which], keys, preferred_element_type=jnp.float32)

    row = lax.broadcasted_iota(jnp.int32, (step, step), 0)
    column = lax.broadcasted_iota(jnp.int32, (step, step), 1)
    highest = []
    for which in range(2):
        diagonal = jnp.where(column <= row, raw(which, place), NEG)
        scores[which, place] = diagonal
        highest.append(fold(diagonal, jnp.maximum))

    def first_pass(index, carry):
        found = []
        for which in range(2):
            values = raw(which, index)
            scores[which, index] = values
            found.append(jnp.maximum(carry[which], fold(values, jnp.maximum)))
        return tuple(found)

    highest = lax.fori_loop(0, place, first_pass, tuple(highest))
    tops = [jnp.max(found, axis=1, keepdims=True) * coef for found in highest]

    def second_pass(index, carry):
        values = packed[index, 4 * maps : 4 * maps + width, :]
        found = []
        for which in range(2):
            total, mixed = carry[which]
            weights = jnp.exp2(scores[which, index] * coef - tops[which])
            total = total + fold(weights, jnp.add)
            mixed = mixed + lax.dot_general(
                weights.astype(jnp.bfloat16),
                values,
                (((1,), (1,)), ((), ())),
                preferred_element_type=jnp.float32,
            )
            found.append((total, mixed))
        return tuple(found)

    empty = jnp.zeros((step, width), jnp.float32)
    found = lax.fori_loop(0, place + 1, second_pass, ((empty, empty), (empty, empty)))
    outputs = [mixed / jnp.sum(total, axis=1, keepdims=True) for total, mixed in found]
    mixed = outputs[0] - scalars[1] * outputs[1]
    square = jnp.sum(mixed * mixed, axis=1, keepdims=True) * scalars[2]
    normed = (mixed * lax.rsqrt(square + EPS) * gain[...]).astype(jnp.bfloat16)
    cores = out.shape[1]
    for at in range(step // block):
        begin = at // cores * block
        out[0, at % cores, begin : begin + block] = normed[at * block : (at + 1) * block]


def widen(values, width):
    missing = width - values.shape[-1]
    return jnp.pad(values, [(0, 0)] * (values.ndim - 1) + [(0, missing)]) if missing else values


def fast_memory(limit_mib):
    return pltpu.CompilerParams(vmem_limit_bytes=limit_mib << 20)


def mirrored(value, axis, apart):
    return lax.ppermute(value, axis, [(i, i ^ apart) for i in range(lax.axis_size(axis))])


def mirrored_all(values, axis):
    found = {far: mirrored(values[far], axis, far) for far in reversed(range(1, len(values)))}
    return [values[0]] + [found[far] for far in range(1, len(values))]


def whole_call(body, outs, *operands, scalars=(), flops=0, scratch=(), limit=8):
    vmem = pl.BlockSpec(memory_space=pltpu.VMEM)
    return pl.pallas_call(
        body,
        in_specs=[pl.BlockSpec(memory_space=pltpu.SMEM)] * len(scalars) + [vmem] * len(operands),
        out_specs=[vmem] * len(outs),
        out_shape=[pltpu.VMEM(shape, dtype) for shape, dtype in outs],
        scratch_shapes=scratch,
        compiler_params=fast_memory(limit),
        cost_estimate=pl.CostEstimate(flops=flops, bytes_accessed=0, transcendentals=0),
    )(*scalars, *[pltpu.with_memory_space_constraint(operand, pltpu.VMEM) for operand in operands])


def exchanged_heads(query_a, key_a, value_a, query_b, key_b, value_b, mix_a, mix_b, head_gain_a, head_gain_b, block):
    seq_rows, heads_a, _ = query_a.shape
    ways = lax.axis_size("sp")
    cores = lax.axis_size("c")
    place = lax.axis_index("sp")
    groups = ((query_a, key_a, value_a), (query_b, key_b, value_b))
    width = -(-max(group[2].shape[2] for group in groups) // 128) * 128
    maps = -(-max(group[0].shape[2] // 2 for group in groups) // 16) * 16

    def filled(array, size):
        return jnp.pad(array, ((0, 0), (0, size - array.shape[1]), (0, 0)))

    turned = lax.optimization_barrier([[jnp.transpose(array, (1, 2, 0)) for array in group] for group in groups])
    outgoing = []
    for query, key, value in turned:
        half = query.shape[1] // 2
        split = [array[:, first : first + half] for first in (0, half) for array in (query, key)]
        outgoing.append(jnp.concatenate([filled(array, maps) for array in split] + [filled(value, width)], axis=1))
    outgoing = jnp.concatenate(outgoing, axis=0)
    pieces = [lax.dynamic_index_in_dim(outgoing, place ^ far, 0, False) for far in range(ways)]
    pieces = mirrored_all(pieces, "sp")
    first = place < heads_a
    gain = jnp.where(first, widen(head_gain_a, width), widen(head_gain_b, width)) * HEAD_SCALE
    coef_a, coef_b = [math.log2(math.e) / math.sqrt(group[0].shape[2] // 2) for group in groups]
    scalars = jnp.stack(
        [
            jnp.where(first, coef_a, coef_b).astype(jnp.float32),
            lax.dynamic_index_in_dim(jnp.concatenate([mix_a, mix_b]), place, 0, False),
            jnp.where(first, 1.0 / value_a.shape[2], 1.0 / value_b.shape[2]).astype(jnp.float32),
        ]
    )
    pairs = (ways * seq_rows) * (ways + 1) * seq_rows
    shape = (ways, cores, seq_rows // cores, width)
    smem = pl.BlockSpec(memory_space=pltpu.SMEM)
    mixed = pl.pallas_call(
        lambda *refs: attend_kernel(*refs, step=seq_rows, width=width, maps=maps, block=block),
        grid=(ways,),
        in_specs=[smem, smem, pl.BlockSpec((1, width), lambda index: (0, 0))]
        + [pl.BlockSpec(piece.shape, lambda index: (0, 0)) for piece in pieces],
        out_specs=pl.BlockSpec((1,) + shape[1:], lambda index: (index, 0, 0, 0)),
        out_shape=pltpu.HBM(shape, jnp.bfloat16),
        scratch_shapes=[
            pltpu.VMEM((2, ways, seq_rows, seq_rows), jnp.float32),
            pltpu.VMEM((ways,) + pieces[0].shape, jnp.bfloat16),
        ],
        compiler_params=pltpu.CompilerParams(dimension_semantics=("arbitrary",), vmem_limit_bytes=24 << 20),
        cost_estimate=pl.CostEstimate(flops=2 * pairs * (maps + width), bytes_accessed=0, transcendentals=pairs),
        name="attend",
    )(scalars, place[None].astype(jnp.int32), gain[None, :], *pieces)
    flat = mixed.reshape((ways * cores,) + shape[2:])
    return lax.all_to_all(flat, ("sp", "c"), split_axis=0, concat_axis=0, tiled=True).reshape(shape)


def project(heads, proj_a, proj_b, lines, block, heads_a):
    ways, cores, rows, _ = heads.shape
    model = proj_a.shape[1]
    weights = []
    for apart in range(cores):
        weights += [proj_a, proj_b] if apart == 0 else [mirrored(proj_a, "c", apart), mirrored(proj_b, "c", apart)]
    where = jnp.stack([lax.axis_index("c"), lax.axis_index("z")]).astype(jnp.int32)
    step = math.gcd(model, 512)
    narrow = proj_b.shape[0] // (ways - heads_a)
    wide = proj_a.shape[0] // heads_a

    def body(at, heads_ref, *refs):
        sets, outs = refs[: 2 * cores], refs[2 * cores :]
        pairs = []
        for apart in range(cores):
            core = at[0] ^ apart

            def taken(head, used):
                found = [heads_ref[head, core, pl.ds((at[1] ^ far) * block, block), :] for far in range(lines)]
                return jnp.concatenate(found, axis=0)[:, :used]

            left_a = jnp.concatenate([taken(head, wide) for head in range(heads_a)], axis=1)
            left_b = jnp.concatenate([taken(head, narrow) for head in range(heads_a, ways)], axis=1)
            pairs += [(left_a, sets[2 * apart]), (left_b, sets[2 * apart + 1])]
        for first in range(0, model, step):
            span = slice(first, first + step)
            total = None
            for left, right in pairs:
                piece = jnp.dot(left, right[:, span], preferred_element_type=jnp.float32)
                total = piece if total is None else total + piece
            for far in range(lines):
                outs[far][:, span] = total[far * block : (far + 1) * block].astype(jnp.bfloat16)

    return whole_call(
        body,
        [((block, model), jnp.bfloat16)] * lines,
        heads,
        *weights,
        scalars=(where,),
        flops=2 * rows * model * (proj_a.shape[0] + proj_b.shape[0]) * cores,
    )


def expert_hidden(rows_ref, gate_ref, up_ref, held, first, count):
    hidden = gate_ref.shape[1]
    tile = math.gcd(hidden, 256)
    for at in range(hidden // tile):
        span = slice(at * tile, (at + 1) * tile)
        gate = jnp.dot(rows_ref[pl.ds(first, count), :], gate_ref[:, span], preferred_element_type=jnp.float32)
        upward = jnp.dot(rows_ref[pl.ds(first, count), :], up_ref[:, span], preferred_element_type=jnp.float32)
        held[:, span] = (jax.nn.silu(gate) * upward).astype(jnp.bfloat16)


def expert_down(held, down_ref, out_ref, first, count):
    model = down_ref.shape[1]
    tile = math.gcd(model, 512)
    for at in range(model // tile):
        span = slice(at * tile, (at + 1) * tile)
        total = jnp.dot(held, down_ref[:, span], preferred_element_type=jnp.float32)
        out_ref[pl.ds(first, count), span] = total.astype(jnp.bfloat16)


def expert_call(rows, weights, out_cols, after=()):
    count = rows.shape[0]
    hidden = weights[-1].shape[0] if len(weights) != 2 else weights[0].shape[1]
    tile = max(size for size in range(16, 257, 16) if count % size == 0)
    flops = 2 * count * sum(weight.size for weight in weights)

    def body(rows_ref, *refs):
        weight_refs, (out_ref, held) = refs[: len(weights)], refs[-2:]

        def step(index, carry):
            first = index * tile
            if len(weights) > 1:
                expert_hidden(rows_ref, *weight_refs[:2], held, first, tile)
            if len(weights) == 2:
                out_ref[pl.ds(first, tile), :] = held[...]
            else:
                left = held[...] if len(weights) == 3 else rows_ref[pl.ds(first, tile), :]
                expert_down(left, weight_refs[-1], out_ref, first, tile)
            return carry

        lax.fori_loop(0, count // tile, step, 0)

    (out,) = whole_call(
        body,
        [((count, out_cols), jnp.bfloat16)],
        rows,
        *weights,
        *after,
        flops=flops,
        scratch=[pltpu.VMEM((tile, hidden), jnp.bfloat16)],
    )
    return out


def exchanged_device(
    resid,
    query_a,
    key_a,
    value_a,
    query_b,
    key_b,
    value_b,
    mix_a,
    mix_b,
    head_gain_a,
    head_gain_b,
    proj_a,
    proj_b,
    norm_gain,
    route_ids,
    route_weights,
    expert_gate,
    expert_up,
    down_w,
):
    ways, lines, cores = (lax.axis_size(axis) for axis in ("sp", "z", "c"))
    place = lax.axis_index("sp")
    tok_rows, width = resid.shape
    top_count = route_ids.shape[1]
    capacity = 3 * top_count * tok_rows // (2 * ways)
    slots_all = ways * capacity
    low = jnp.bfloat16
    head_cols, back_cols = (width * part // 16 // 128 * 128 for part in (5, 4))
    tail_cols, rest_cols = width - head_cols, width - back_cols

    heads = exchanged_heads(
        query_a, key_a, value_a, query_b, key_b, value_b, mix_a, mix_b, head_gain_a, head_gain_b, tok_rows
    )

    slots = slot_numbers(route_ids ^ place, ways, capacity)
    routes = jnp.concatenate([jnp.transpose(slots).astype(jnp.float32), jnp.transpose(route_weights)], axis=0)
    line_routes = mirrored_all([routes] * lines, "z")

    def hits(routes_ref, which):
        lookup = lax.broadcasted_iota(jnp.int32, (slots_all, tok_rows), 0)
        return routes_ref[which : which + 1, :].astype(jnp.int32) == lookup

    def spread_rows(routes_ref, tokens):
        spread = sum(hits(routes_ref, which).astype(jnp.float32) for which in range(top_count)).astype(low)
        return jnp.dot(spread, tokens, preferred_element_type=jnp.float32).astype(low)

    def blend_rows(routes_ref, block):
        weights = sum(
            jnp.where(hits(routes_ref, which), routes_ref[top_count + which : top_count + which + 1, :], 0.0)
            for which in range(top_count)
        )
        upper = weights.astype(low)
        total = None
        for part in (upper, (weights - upper.astype(jnp.float32)).astype(low)):
            piece = lax.dot_general(part, block, (((0,), (0,)), ((), ())), preferred_element_type=jnp.float32)
            total = piece if total is None else total + piece
        return total

    parts = project(heads, proj_a, proj_b, lines, tok_rows, query_a.shape[1])
    parts = mirrored_all(parts, "z")

    def norm_body(*refs):
        part_refs, (resid_ref, gain_ref, routes_ref), outs = refs[:lines], refs[lines : lines + 3], refs[lines + 3 :]
        mixed = resid_ref[...].astype(jnp.float32)
        for part in part_refs:
            mixed = mixed + part[...].astype(jnp.float32)
        outs[0][...] = mixed
        normed = rms_scaled(mixed, gain_ref[...]).astype(low)
        outs[1][...] = normed[:, head_cols:]
        picked = spread_rows(routes_ref, normed[:, :head_cols])
        for far in range(ways):
            outs[2 + far][...] = picked[far * capacity : (far + 1) * capacity]

    mixed, tail, *heads_out = whole_call(
        norm_body,
        [((tok_rows, width), jnp.float32), ((tok_rows, tail_cols), low)] + [((capacity, head_cols), low)] * ways,
        *parts,
        resid,
        norm_gain[None, :],
        routes,
    )
    tails = mirrored_all([tail] * lines, "z")
    heads_in = mirrored_all(heads_out, "sp")
    groups = {"near": list(range(ways - 1)), "far": [ways - 1]}
    head_own = jnp.concatenate(heads_in, axis=0)
    head_blocks = mirrored_all([head_own] * lines, "z")

    weights = (expert_gate[0], expert_up[0], down_w[0])

    def spread_body(*refs):
        tail_refs, routes_refs, outs = refs[:lines], refs[lines : 2 * lines], refs[-ways:]
        for line in range(lines):
            picked = spread_rows(routes_refs[line], tail_refs[line][...])
            for far in range(ways):
                outs[far][line * capacity : (line + 1) * capacity] = picked[far * capacity : (far + 1) * capacity]

    tail_blocks = list(
        whole_call(
            spread_body, [((lines * capacity, tail_cols), low)] * ways, *tails, *line_routes, head_own, *weights[:2]
        )
    )
    for members in groups.values():
        for far in members:
            if far > 0:
                tail_blocks[far] = mirrored(tail_blocks[far], "sp", far)

    def join(group, *after):
        members = groups[group]

        def body(*refs):
            head_refs, tail_refs, out = refs[:lines], refs[lines : lines + len(members)], refs[-1]
            for line in range(lines):
                for at, far in enumerate(members):
                    first = (line * len(members) + at) * capacity
                    out[first : first + capacity, :head_cols] = head_refs[line][far * capacity : (far + 1) * capacity]
                    out[first : first + capacity, head_cols:] = tail_refs[at][line * capacity : (line + 1) * capacity]

        (rows,) = whole_call(
            body,
            [((lines * len(members) * capacity, width), low)],
            *head_blocks,
            *[tail_blocks[far] for far in members],
            *after,
        )
        return rows

    def pair(group, own_part, other_part, *started):
        members = groups[group]
        count = len(members)

        def body(own_ref, other_ref, *refs):
            outs = refs[len(started) :]
            for line in range(lines):
                if started:
                    outs[line][: members[0] * capacity] = refs[line][...]
                for at, far in enumerate(members):
                    span = slice((line * count + at) * capacity, (line * count + at + 1) * capacity)
                    total = own_ref[span].astype(jnp.float32) + other_ref[span].astype(jnp.float32)
                    total = total.astype(low)
                    outs[line][far * capacity : (far + 1) * capacity] = total[:, :back_cols]
                    outs[lines + at][line * capacity : (line + 1) * capacity] = total[:, back_cols:]

        return whole_call(
            body,
            [(((members[-1] + 1) * capacity, back_cols), low)] * lines
            + [((lines * capacity, rest_cols), low)] * count,
            own_part,
            other_part,
            *started,
        )

    assert cores == 2
    tail_back, started, before, after = {}, (), (), ()
    for group, members in groups.items():
        rows = join(group, *before)
        other_rows = mirrored(rows, "c", 1)
        hidden = expert_call(rows, weights[:2], weights[0].shape[1])
        other_part = expert_call(other_rows, weights, width, (hidden,) + after)
        own_part = expert_call(hidden, weights[2:], width)
        back = pair(group, own_part, mirrored(other_part, "c", 1), *started)
        for at, far in enumerate(members):
            tail_back[far] = mirrored(back[lines + at], "sp", far) if far else back[lines + at]
        started, before, after = back[:lines], (other_part,), (back[0],)
    tail_back = [tail_back[far] for far in range(ways)]
    head_back = mirrored_all(started, "z")

    def blend_body(*refs):
        tail_refs, routes_refs, outs = refs[:ways], refs[ways : ways + lines], refs[ways + lines :]
        for line in range(lines):
            block = jnp.concatenate([ref[line * capacity : (line + 1) * capacity] for ref in tail_refs], axis=0)
            outs[line][...] = blend_rows(routes_refs[line], block).astype(low)

    tail_sums = whole_call(blend_body, [((tok_rows, rest_cols), low)] * lines, *tail_back, *line_routes)
    tail_sums = mirrored_all(tail_sums, "z")

    def total_body(*refs):
        part_refs, outs = refs[:lines], refs[lines:]
        total = sum(part[...].astype(jnp.float32) for part in part_refs).astype(low)
        for far in range(ways):
            outs[far][...] = total[far * capacity : (far + 1) * capacity]

    head_sums = whole_call(total_body, [((capacity, back_cols), low)] * ways, *head_back)
    head_sums = mirrored_all(head_sums, "sp")

    def final_body(mixed_ref, routes_ref, *refs):
        head_refs, tail_refs, (out,) = refs[:ways], refs[ways : ways + lines], refs[ways + lines :]
        block = jnp.concatenate([ref[...] for ref in head_refs], axis=0)
        total = mixed_ref[:, :back_cols] + blend_rows(routes_ref, block)
        out[:, :back_cols] = total.astype(low)
        total = mixed_ref[:, back_cols:]
        for ref in tail_refs:
            total = total + ref[...].astype(jnp.float32)
        out[:, back_cols:] = total.astype(low)

    (output,) = whole_call(final_body, [((tok_rows, width), low)], mixed, routes, *head_sums, *tail_sums)
    return output


def placements(tp):
    both = ("sp",) + tp
    return (
        (
            P(both, None),
            P("sp", tp, None),
            P("sp", tp, None),
            P("sp", tp, None),
            P("sp", tp, None),
            P("sp", tp, None),
            P("sp", tp, None),
            P(tp),
            P(tp),
            P(),
            P(),
            P(tp, None),
            P(tp, None),
            P(),
            P(both, None),
            P(both, None),
            P("sp", None, tp),
            P("sp", None, tp),
            P("sp", tp, None),
        ),
        P(both, None),
    )


def solution(mesh):
    sp_ways, tp_ways = (mesh.shape[axis] for axis in ("sp", "tp"))
    cores = 2

    def program(*arrays):
        resid, query_a, query_b, route_ids = arrays[0], arrays[1], arrays[4], arrays[14]
        block = resid.shape[0] // (sp_ways * tp_ways)
        heads = (query_a.shape[1] + query_b.shape[1]) // tp_ways
        capacity = 3 * route_ids.shape[1] * block // (2 * sp_ways)
        fits = heads == sp_ways and capacity % 16 == 0 and block % 16 == 0 and resid.shape[1] % 2048 == 0
        if fits:
            devices = mesh.devices.reshape(sp_ways, tp_ways // cores, cores)
            inner, axes = Mesh(devices, ("sp", "z", "c")), ("z", "c")

            def body(*parts):
                return exchanged_device(*parts)

        else:
            inner, axes, body = mesh, ("tp",), gathered_device
        given, returned = placements(axes)
        mapped = jax.shard_map(body, mesh=inner, in_specs=given, out_specs=returned, check_vma=False)
        return mapped(*arrays)

    return program
```

```python
import math

import jax
import jax.numpy as jnp
from jax import lax
from jax.experimental import pallas as pl
from jax.experimental.pallas import tpu as pltpu
from jax.sharding import Mesh, PartitionSpec as P


EPS = 1e-06
NEG = -1e30
HEAD_SCALE = 1.0 - (0.8 - 0.6 * math.exp(-0.3))
KEY_STEP = 512


def partner(value, axis, apart):
    return lax.ppermute(value, axis, [(i, i ^ 1 << apart) for i in range(lax.axis_size(axis))])


def rms_scaled(values, gain):
    return values * lax.rsqrt(jnp.mean(values * values, axis=-1, keepdims=True) + EPS) * gain


def slot_numbers(route_rows, experts, capacity):
    count, top_count = route_rows.shape
    flat = route_rows.reshape(count * top_count)
    onehot = (flat[:, None] == jnp.arange(experts, dtype=jnp.int32)[None, :]).astype(jnp.int32)
    ranks = jnp.sum((jnp.cumsum(onehot, axis=0) - onehot) * onehot, axis=1)
    return (flat * capacity + ranks).reshape(count, top_count)


def empty_map(count, heads, width):
    return (
        jnp.zeros((count, heads, width), jnp.float32),
        jnp.full((heads, count), NEG, jnp.float32),
        jnp.zeros((heads, count), jnp.float32),
    )


def empty_group(query, value):
    return (
        empty_map(query.shape[0], query.shape[1], value.shape[2]),
        empty_map(query.shape[0], query.shape[1], value.shape[2]),
    )


def map_update(state, query, keys, values, allowed, scale):
    weighted, maximum, sums = state
    scores = jnp.einsum("qhd,khd->hqk", query, keys, preferred_element_type=jnp.float32) * scale
    scores = jnp.where(allowed[None], scores, NEG)
    fresh = jnp.maximum(maximum, jnp.max(scores, axis=2))
    weights = jnp.where(allowed[None], jnp.exp(scores - fresh[:, :, None]), 0.0)
    factor = jnp.exp(maximum - fresh)
    sums = sums * factor + jnp.sum(weights, axis=2)
    added = jnp.einsum(
        "hqk,khv->qhv", weights.astype(jnp.bfloat16), values, preferred_element_type=jnp.float32
    )
    weighted = weighted * jnp.transpose(factor)[:, :, None] + added
    return (weighted, fresh, sums)


def group_update(states, query, keys, values, allowed):
    width = query.shape[2] // 2
    scale = 1.0 / math.sqrt(width)
    return tuple(
        (
            map_update(
                states[which],
                query[:, :, which * width : (which + 1) * width],
                keys[:, :, which * width : (which + 1) * width],
                values,
                allowed,
                scale,
            )
            for which in range(2)
        )
    )


def set_update(carry, queries, pieces):
    rows_a, rows_b, query_pos = queries
    piece_key_a, piece_value_a, piece_key_b, piece_value_b = pieces
    length = piece_key_a.shape[0]
    step = math.gcd(length, KEY_STEP)
    latest = query_pos[-1]

    def inner(index, states):
        first = index * step

        def compute(current):
            keys_a = lax.dynamic_slice_in_dim(piece_key_a, first, step, 0)
            values_a = lax.dynamic_slice_in_dim(piece_value_a, first, step, 0)
            keys_b = lax.dynamic_slice_in_dim(piece_key_b, first, step, 0)
            values_b = lax.dynamic_slice_in_dim(piece_value_b, first, step, 0)
            key_pos = first + jnp.arange(step, dtype=jnp.int32)
            allowed = key_pos[None, :] <= query_pos[:, None]
            return (
                group_update(current[0], rows_a, keys_a, values_a, allowed),
                group_update(current[1], rows_b, keys_b, values_b, allowed),
            )

        return lax.cond(first <= latest, compute, lambda current: current, states)

    return lax.fori_loop(0, length // step, inner, carry)


def finish_group(states, mix, gain):
    outputs = [state[0] / jnp.transpose(state[2])[:, :, None] for state in states]
    mixed = outputs[0] - mix[None, :, None] * outputs[1]
    normed = rms_scaled(mixed, gain) * HEAD_SCALE
    return normed.astype(jnp.bfloat16).reshape(mixed.shape[0], -1)


def gathered_device(
    resid,
    query_a,
    key_a,
    value_a,
    query_b,
    key_b,
    value_b,
    mix_a,
    mix_b,
    head_gain_a,
    head_gain_b,
    proj_a,
    proj_b,
    norm_gain,
    route_ids,
    route_weights,
    expert_gate,
    expert_up,
    expert_down,
):
    seq_rows = query_a.shape[0]
    sp_ways = lax.axis_size("sp")
    place = lax.axis_index("sp")
    positions = place * seq_rows + jnp.arange(seq_rows, dtype=jnp.int32)
    levels = sp_ways.bit_length() - 1
    half = seq_rows // 2
    moved = jnp.concatenate(
        [query_a[half:].reshape(half, -1), query_b[half:].reshape(half, -1)], axis=1
    )
    for bit in range(levels):
        moved = partner(moved, "sp", bit)
    split_at = query_a.shape[1] * query_a.shape[2]
    far_a = moved[:, :split_at].reshape(half, query_a.shape[1], query_a.shape[2])
    far_b = moved[:, split_at:].reshape(half, query_b.shape[1], query_b.shape[2])
    far_pos = (sp_ways - 1 - place) * seq_rows + half + jnp.arange(half, dtype=jnp.int32)
    query_sets = ((query_a[:half], query_b[:half], positions[:half]), (far_a, far_b, far_pos))

    def fold_keys(carry, pieces):
        return tuple(
            (set_update(states, queries, pieces) for states, queries in zip(carry, query_sets))
        )

    initial = tuple(
        (
            (empty_group(queries[0], value_a), empty_group(queries[1], value_b))
            for queries in query_sets
        )
    )
    results = fold_keys(
        initial,
        (
            lax.all_gather(key_a, "sp", axis=0, tiled=True),
            lax.all_gather(value_a, "sp", axis=0, tiled=True),
            lax.all_gather(key_b, "sp", axis=0, tiled=True),
            lax.all_gather(value_b, "sp", axis=0, tiled=True),
        ),
    )
    finished = [
        (finish_group(states[0], mix_a, head_gain_a), finish_group(states[1], mix_b, head_gain_b))
        for states in results
    ]
    returned = jnp.concatenate([finished[1][0], finished[1][1]], axis=1)
    for bit in range(levels):
        returned = partner(returned, "sp", bit)
    width_a = finished[0][0].shape[1]
    heads_out_a = jnp.concatenate([finished[0][0], returned[:, :width_a]], axis=0)
    heads_out_b = jnp.concatenate([finished[0][1], returned[:, width_a:]], axis=0)
    width = resid.shape[1]
    tok_rows = resid.shape[0]
    top_count = route_ids.shape[1]
    capacity = 3 * top_count * tok_rows // (2 * sp_ways)
    own_slots = slot_numbers(route_ids, sp_ways, capacity)
    term = jnp.dot(heads_out_a, proj_a, preferred_element_type=jnp.float32)
    term = term + jnp.dot(heads_out_b, proj_b, preferred_element_type=jnp.float32)
    mixed = resid.astype(jnp.float32) + lax.psum_scatter(
        lax.optimization_barrier(term.astype(jnp.bfloat16))
        .astype(jnp.float32)
        .astype(jnp.bfloat16),
        "tp",
        scatter_dimension=0,
        tiled=True,
    ).astype(jnp.float32)
    normed = rms_scaled(mixed, norm_gain).astype(jnp.bfloat16)
    lookup = jnp.arange(sp_ways * capacity, dtype=jnp.int32)[:, None]
    spread = jnp.zeros((sp_ways * capacity, tok_rows), jnp.float32)
    for which in range(top_count):
        spread = spread + (own_slots[:, which][None, :] == lookup).astype(jnp.float32)
    outgoing = jnp.dot(
        spread.astype(jnp.bfloat16), normed, preferred_element_type=jnp.float32
    ).astype(jnp.bfloat16)
    arrived = lax.all_to_all(
        outgoing.reshape(sp_ways, capacity, width), "sp", split_axis=0, concat_axis=0, tiled=True
    )
    piece = lax.all_gather(arrived.reshape(sp_ways * capacity, width), "tp", axis=0, tiled=True)
    gate = jnp.dot(piece, expert_gate[0], preferred_element_type=jnp.float32)
    upward = jnp.dot(piece, expert_up[0], preferred_element_type=jnp.float32)
    hidden = (jax.nn.silu(gate) * upward).astype(jnp.bfloat16)
    term = jnp.dot(hidden, expert_down[0], preferred_element_type=jnp.float32)
    summed = lax.psum_scatter(
        lax.optimization_barrier(term.astype(jnp.bfloat16))
        .astype(jnp.float32)
        .astype(jnp.bfloat16),
        "tp",
        scatter_dimension=0,
        tiled=True,
    )
    finished_rows = summed.reshape(sp_ways, capacity, width)
    back = lax.all_to_all(finished_rows, "sp", split_axis=0, concat_axis=0, tiled=True)
    picked = jnp.take(back.reshape(sp_ways * capacity, width), own_slots.reshape(-1), axis=0)
    picked = picked.reshape(tok_rows, top_count, width)
    output = mixed + jnp.sum(route_weights[:, :, None] * picked.astype(jnp.float32), axis=1)
    return output.astype(jnp.bfloat16)


def attend_kernel(scalars, own, gain, *refs, step, width, maps, block):
    pieces, (out, scores, packed) = refs[:-3], refs[-3:]
    place = pl.program_id(0)
    coef = scalars[0]

    @pl.when(place == 0)
    def _():
        for far, piece in enumerate(pieces):
            packed[own[0] ^ far] = piece[...]

    queries = [jnp.transpose(packed[place, 2 * which * maps : (2 * which + 1) * maps, :]) for which in range(2)]

    def fold(values, combine):
        parts = [values[:, at * width : (at + 1) * width] for at in range(step // width)]
        while len(parts) > 1:
            parts = [combine(*parts[at : at + 2]) for at in range(0, len(parts), 2)]
        return parts[0]

    def raw(which, index):
        keys = packed[index, (2 * which + 1) * maps : (2 * which + 2) * maps, :]
        return jnp.dot(queries[which], keys, preferred_element_type=jnp.float32)

    row = lax.broadcasted_iota(jnp.int32, (step, step), 0)
    column = lax.broadcasted_iota(jnp.int32, (step, step), 1)
    highest = []
    for which in range(2):
        diagonal = jnp.where(column <= row, raw(which, place), NEG)
        scores[which, place] = diagonal
        highest.append(fold(diagonal, jnp.maximum))

    def first_pass(index, carry):
        found = []
        for which in range(2):
            values = raw(which, index)
            scores[which, index] = values
            found.append(jnp.maximum(carry[which], fold(values, jnp.maximum)))
        return tuple(found)

    highest = lax.fori_loop(0, place, first_pass, tuple(highest))
    tops = [jnp.max(found, axis=1, keepdims=True) * coef for found in highest]

    def second_pass(index, carry):
        values = packed[index, 4 * maps : 4 * maps + width, :]
        found = []
        for which in range(2):
            total, mixed = carry[which]
            weights = jnp.exp2(scores[which, index] * coef - tops[which])
            total = total + fold(weights, jnp.add)
            mixed = mixed + lax.dot_general(
                weights.astype(jnp.bfloat16),
                values,
                (((1,), (1,)), ((), ())),
                preferred_element_type=jnp.float32,
            )
            found.append((total, mixed))
        return tuple(found)

    empty = jnp.zeros((step, width), jnp.float32)
    found = lax.fori_loop(0, place + 1, second_pass, ((empty, empty), (empty, empty)))
    outputs = [mixed / jnp.sum(total, axis=1, keepdims=True) for total, mixed in found]
    mixed = outputs[0] - scalars[1] * outputs[1]
    square = jnp.sum(mixed * mixed, axis=1, keepdims=True) * scalars[2]
    normed = (mixed * lax.rsqrt(square + EPS) * gain[...]).astype(jnp.bfloat16)
    pairs, cores = out.shape[1:3]
    for at in range(step // block):
        begin = at // (pairs * cores) * block
        out[0, at // cores % pairs, at % cores, begin : begin + block] = normed[at * block : (at + 1) * block]


def widen(values, width):
    missing = width - values.shape[-1]
    return jnp.pad(values, [(0, 0)] * (values.ndim - 1) + [(0, missing)]) if missing else values


def fast_memory(limit_mib):
    return pltpu.CompilerParams(vmem_limit_bytes=limit_mib << 20)


def mirrored(value, axis, apart):
    return lax.ppermute(value, axis, [(i, i ^ apart) for i in range(lax.axis_size(axis))])


def mirrored_all(values, axis):
    found = {far: mirrored(values[far], axis, far) for far in reversed(range(1, len(values)))}
    return [values[0]] + [found[far] for far in range(1, len(values))]


def whole_call(body, outs, *operands, scalars=(), flops=0, scratch=(), limit=8):
    vmem = pl.BlockSpec(memory_space=pltpu.VMEM)
    return pl.pallas_call(
        body,
        in_specs=[pl.BlockSpec(memory_space=pltpu.SMEM)] * len(scalars) + [vmem] * len(operands),
        out_specs=[vmem] * len(outs),
        out_shape=[pltpu.VMEM(shape, dtype) for shape, dtype in outs],
        scratch_shapes=scratch,
        compiler_params=fast_memory(limit),
        cost_estimate=pl.CostEstimate(flops=flops, bytes_accessed=0, transcendentals=0),
    )(*scalars, *[pltpu.with_memory_space_constraint(operand, pltpu.VMEM) for operand in operands])


def exchanged_heads(query_a, key_a, value_a, query_b, key_b, value_b, mix_a, mix_b, head_gain_a, head_gain_b, block):
    seq_rows, heads_a, _ = query_a.shape
    ways = lax.axis_size("sp")
    cores, pair_lines = lax.axis_size("c"), lax.axis_size("zl")
    place = lax.axis_index("sp")
    groups = ((query_a, key_a, value_a), (query_b, key_b, value_b))
    width = -(-max(group[2].shape[2] for group in groups) // 128) * 128
    maps = -(-max(group[0].shape[2] // 2 for group in groups) // 16) * 16

    def filled(array, size):
        return jnp.pad(array, ((0, 0), (0, size - array.shape[1]), (0, 0)))

    turned = lax.optimization_barrier([[jnp.transpose(array, (1, 2, 0)) for array in group] for group in groups])
    outgoing = []
    for query, key, value in turned:
        half = query.shape[1] // 2
        split = [array[:, first : first + half] for first in (0, half) for array in (query, key)]
        outgoing.append(jnp.concatenate([filled(array, maps) for array in split] + [filled(value, width)], axis=1))
    outgoing = jnp.concatenate(outgoing, axis=0)
    pieces = [lax.dynamic_index_in_dim(outgoing, place ^ far, 0, False) for far in range(ways)]
    pieces = mirrored_all(pieces, "sp")
    first = place < heads_a
    gain = jnp.where(first, widen(head_gain_a, width), widen(head_gain_b, width)) * HEAD_SCALE
    coef_a, coef_b = [math.log2(math.e) / math.sqrt(group[0].shape[2] // 2) for group in groups]
    scalars = jnp.stack(
        [
            jnp.where(first, coef_a, coef_b).astype(jnp.float32),
            lax.dynamic_index_in_dim(jnp.concatenate([mix_a, mix_b]), place, 0, False),
            jnp.where(first, 1.0 / value_a.shape[2], 1.0 / value_b.shape[2]).astype(jnp.float32),
        ]
    )
    pairs = (ways * seq_rows) * (ways + 1) * seq_rows
    shape = (ways, pair_lines, cores, seq_rows // (pair_lines * cores), width)
    smem = pl.BlockSpec(memory_space=pltpu.SMEM)
    mixed = pl.pallas_call(
        lambda *refs: attend_kernel(*refs, step=seq_rows, width=width, maps=maps, block=block),
        grid=(ways,),
        in_specs=[smem, smem, pl.BlockSpec((1, width), lambda index: (0, 0))]
        + [pl.BlockSpec(piece.shape, lambda index: (0, 0)) for piece in pieces],
        out_specs=pl.BlockSpec((1,) + shape[1:], lambda index: (index, 0, 0, 0, 0)),
        out_shape=pltpu.HBM(shape, jnp.bfloat16),
        scratch_shapes=[
            pltpu.VMEM((2, ways, seq_rows, seq_rows), jnp.float32),
            pltpu.VMEM((ways,) + pieces[0].shape, jnp.bfloat16),
        ],
        compiler_params=pltpu.CompilerParams(dimension_semantics=("arbitrary",), vmem_limit_bytes=24 << 20),
        cost_estimate=pl.CostEstimate(flops=2 * pairs * (maps + width), bytes_accessed=0, transcendentals=pairs),
        name="attend",
    )(scalars, place[None].astype(jnp.int32), gain[None, :], *pieces)
    flat = mixed.reshape((-1,) + shape[3:])
    return lax.all_to_all(flat, ("sp", "zl", "c"), split_axis=0, concat_axis=0, tiled=True).reshape(shape)


def project(heads, proj_a, proj_b, block, heads_a):
    ways, pair_lines, cores, rows, _ = heads.shape
    model = proj_a.shape[1]
    lines = rows // block
    weights = []
    for line in range(pair_lines):
        found = (proj_a, proj_b)
        if line > 0:
            found = [mirrored(array, "zl", line) for array in found]
        weights += found
        for apart in range(1, cores):
            weights += [mirrored(array, "c", apart) for array in found]
    where = jnp.stack([lax.axis_index(axis) for axis in ("c", "zl", "zh")]).astype(jnp.int32)
    step = math.gcd(model, 512)
    narrow = proj_b.shape[0] // (ways - heads_a)
    wide = proj_a.shape[0] // heads_a

    def body(at, heads_ref, *refs):
        sets, outs = refs[: len(weights)], refs[len(weights) :]
        pairs = []
        for apart in range(pair_lines * cores):
            core, line = at[0] ^ apart % cores, at[1] ^ apart // cores

            def taken(head, used):
                found = [heads_ref[head, line, core, pl.ds((at[2] ^ far) * block, block), :] for far in range(lines)]
                return jnp.concatenate(found, axis=0)[:, :used]

            left_a = jnp.concatenate([taken(head, wide) for head in range(heads_a)], axis=1)
            left_b = jnp.concatenate([taken(head, narrow) for head in range(heads_a, ways)], axis=1)
            pairs += [(left_a, sets[2 * apart]), (left_b, sets[2 * apart + 1])]
        for first in range(0, model, step):
            span = slice(first, first + step)
            total = None
            for left, right in pairs:
                piece = jnp.dot(left, right[:, span], preferred_element_type=jnp.float32)
                total = piece if total is None else total + piece
            for far in range(lines):
                outs[far][:, span] = total[far * block : (far + 1) * block].astype(jnp.bfloat16)

    return whole_call(
        body,
        [((block, model), jnp.bfloat16)] * lines,
        heads,
        *weights,
        scalars=(where,),
        flops=rows * model * (proj_a.shape[0] + proj_b.shape[0]) * len(weights),
    )


def expert_hidden(rows_ref, gate_ref, up_ref, held, first, count):
    hidden = gate_ref.shape[1]
    tile = math.gcd(hidden, 256)
    for at in range(hidden // tile):
        span = slice(at * tile, (at + 1) * tile)
        gate = jnp.dot(rows_ref[pl.ds(first, count), :], gate_ref[:, span], preferred_element_type=jnp.float32)
        upward = jnp.dot(rows_ref[pl.ds(first, count), :], up_ref[:, span], preferred_element_type=jnp.float32)
        held[:, span] = (jax.nn.silu(gate) * upward).astype(jnp.bfloat16)


def expert_down(held, down_ref, out_ref, first, count):
    model = down_ref.shape[1]
    tile = math.gcd(model, 512)
    for at in range(model // tile):
        span = slice(at * tile, (at + 1) * tile)
        total = jnp.dot(held, down_ref[:, span], preferred_element_type=jnp.float32)
        out_ref[pl.ds(first, count), span] = total.astype(jnp.bfloat16)


def expert_call(rows, weights, out_cols, after=()):
    count = rows.shape[0]
    hidden = weights[-1].shape[0] if len(weights) != 2 else weights[0].shape[1]
    tile = max(size for size in range(16, 257, 16) if count % size == 0)
    flops = 2 * count * sum(weight.size for weight in weights)

    def body(rows_ref, *refs):
        weight_refs, (out_ref, held) = refs[: len(weights)], refs[-2:]

        def step(index, carry):
            first = index * tile
            if len(weights) > 1:
                expert_hidden(rows_ref, *weight_refs[:2], held, first, tile)
            if len(weights) == 2:
                out_ref[pl.ds(first, tile), :] = held[...]
            else:
                left = held[...] if len(weights) == 3 else rows_ref[pl.ds(first, tile), :]
                expert_down(left, weight_refs[-1], out_ref, first, tile)
            return carry

        lax.fori_loop(0, count // tile, step, 0)

    (out,) = whole_call(
        body,
        [((count, out_cols), jnp.bfloat16)],
        rows,
        *weights,
        *after,
        flops=flops,
        scratch=[pltpu.VMEM((tile, hidden), jnp.bfloat16)],
    )
    return out


def exchanged_device(
    resid,
    query_a,
    key_a,
    value_a,
    query_b,
    key_b,
    value_b,
    mix_a,
    mix_b,
    head_gain_a,
    head_gain_b,
    proj_a,
    proj_b,
    norm_gain,
    route_ids,
    route_weights,
    expert_gate,
    expert_up,
    down_w,
):
    line_axes = ("zh", "zl")
    ways, cores, line_pairs, lines = (lax.axis_size(axis) for axis in ("sp", "c", "zh", line_axes))
    place = lax.axis_index("sp")
    tok_rows, width = resid.shape
    top_count = route_ids.shape[1]
    capacity = 3 * top_count * tok_rows // (2 * ways)
    slots_all = ways * capacity
    low = jnp.bfloat16
    head_cols, back_cols = (width * part // 16 // 128 * 128 for part in (4, 5))
    tail_cols, rest_cols = width - head_cols, width - back_cols

    heads = exchanged_heads(
        query_a, key_a, value_a, query_b, key_b, value_b, mix_a, mix_b, head_gain_a, head_gain_b, tok_rows
    )

    slots = slot_numbers(route_ids ^ place, ways, capacity)
    routes = jnp.concatenate([jnp.transpose(slots).astype(jnp.float32), jnp.transpose(route_weights)], axis=0)
    line_routes = mirrored_all([routes] * lines, line_axes)

    def hits(routes_ref, which):
        lookup = lax.broadcasted_iota(jnp.int32, (slots_all, tok_rows), 0)
        return routes_ref[which : which + 1, :].astype(jnp.int32) == lookup

    def spread_rows(routes_ref, tokens):
        spread = sum(hits(routes_ref, which).astype(jnp.float32) for which in range(top_count)).astype(low)
        return jnp.dot(spread, tokens, preferred_element_type=jnp.float32).astype(low)

    def blend_rows(routes_ref, block):
        weights = sum(
            jnp.where(hits(routes_ref, which), routes_ref[top_count + which : top_count + which + 1, :], 0.0)
            for which in range(top_count)
        )
        upper = weights.astype(low)
        total = None
        for part in (upper, (weights - upper.astype(jnp.float32)).astype(low)):
            piece = lax.dot_general(part, block, (((0,), (0,)), ((), ())), preferred_element_type=jnp.float32)
            total = piece if total is None else total + piece
        return total

    parts = project(heads, proj_a, proj_b, tok_rows, query_a.shape[1])
    parts = mirrored_all(parts, "zh")

    def norm_body(*refs):
        part_refs, outs = refs[:line_pairs], refs[line_pairs + 3 :]
        resid_ref, gain_ref, routes_ref = refs[line_pairs : line_pairs + 3]
        mixed = resid_ref[...].astype(jnp.float32)
        for part in part_refs:
            mixed = mixed + part[...].astype(jnp.float32)
        outs[0][...] = mixed
        normed = rms_scaled(mixed, gain_ref[...]).astype(low)
        outs[1][...] = normed[:, head_cols:]
        picked = spread_rows(routes_ref, normed[:, :head_cols])
        for far in range(ways):
            outs[2 + far][...] = picked[far * capacity : (far + 1) * capacity]

    mixed, tail, *heads_out = whole_call(
        norm_body,
        [((tok_rows, width), jnp.float32), ((tok_rows, tail_cols), low)] + [((capacity, head_cols), low)] * ways,
        *parts,
        resid,
        norm_gain[None, :],
        routes,
    )
    tails = mirrored_all([tail] * lines, line_axes)
    heads_in = mirrored_all(heads_out, "sp")
    groups = {"near": list(range(ways - 1)), "far": [ways - 1]}
    head_own = jnp.concatenate(heads_in, axis=0)
    head_blocks = mirrored_all([head_own] * lines, line_axes)

    weights = (expert_gate[0], expert_up[0], down_w[0])

    def spread_body(*refs):
        tail_refs, routes_refs, outs = refs[:lines], refs[lines : 2 * lines], refs[-ways:]
        for line in range(lines):
            picked = spread_rows(routes_refs[line], tail_refs[line][...])
            for far in range(ways):
                outs[far][line * capacity : (line + 1) * capacity] = picked[far * capacity : (far + 1) * capacity]

    tail_blocks = list(
        whole_call(
            spread_body, [((lines * capacity, tail_cols), low)] * ways, *tails, *line_routes, head_own, *weights[:2]
        )
    )
    for members in groups.values():
        for far in members:
            if far > 0:
                tail_blocks[far] = mirrored(tail_blocks[far], "sp", far)

    def join(group, *after):
        members = groups[group]

        def body(*refs):
            head_refs, tail_refs, out = refs[:lines], refs[lines : lines + len(members)], refs[-1]
            for line in range(lines):
                for at, far in enumerate(members):
                    first = (line * len(members) + at) * capacity
                    out[first : first + capacity, :head_cols] = head_refs[line][far * capacity : (far + 1) * capacity]
                    out[first : first + capacity, head_cols:] = tail_refs[at][line * capacity : (line + 1) * capacity]

        (rows,) = whole_call(
            body,
            [((lines * len(members) * capacity, width), low)],
            *head_blocks,
            *[tail_blocks[far] for far in members],
            *after,
        )
        return rows

    def pair(group, own_part, other_parts):
        members = groups[group]

        def body(*refs):
            part_refs, outs = refs[:cores], refs[cores:]
            for line in range(lines):
                for at in range(len(members)):
                    first = (line * len(members) + at) * capacity
                    total = part_refs[0][first : first + capacity].astype(jnp.float32)
                    for part in part_refs[1:]:
                        total = total + part[first : first + capacity].astype(jnp.float32)
                    total = total.astype(low)
                    outs[line][at * capacity : (at + 1) * capacity] = total[:, :back_cols]
                    outs[lines + at][line * capacity : (line + 1) * capacity] = total[:, back_cols:]

        count = len(members)
        return whole_call(
            body,
            [((count * capacity, back_cols), low)] * lines + [((lines * capacity, rest_cols), low)] * count,
            own_part,
            *other_parts,
        )

    assert cores == 2
    tail_back, head_back, before = {}, {}, ()
    for group, members in groups.items():
        rows = join(group, *before)
        other_rows = mirrored(rows, "c", 1)
        hidden = expert_call(rows, weights[:2], weights[0].shape[1])
        after = (hidden,) + tuple(head_back[done][0] for done in head_back)
        other_part = expert_call(other_rows, weights, width, after)
        own_part = expert_call(hidden, weights[2:], width)
        back = pair(group, own_part, [mirrored(other_part, "c", 1)])
        for at, far in reversed(list(enumerate(members))):
            tail_back[far] = mirrored(back[lines + at], "sp", far) if far else back[lines + at]
        head_back[group] = mirrored_all(back[:lines], line_axes)
        before = (other_part,)
    tail_back = [tail_back[far] for far in range(ways)]

    def blend_body(*refs):
        tail_refs, routes_refs, outs = refs[:ways], refs[ways : ways + lines], refs[ways + lines :]
        for line in range(lines):
            block = jnp.concatenate([ref[line * capacity : (line + 1) * capacity] for ref in tail_refs], axis=0)
            outs[line][...] = blend_rows(routes_refs[line], block).astype(low)

    tail_sums = whole_call(blend_body, [((tok_rows, rest_cols), low)] * lines, *tail_back, *line_routes)
    tail_sums = mirrored_all(tail_sums, line_axes)

    def total_body(*refs):
        at = 0
        for members in groups.values():
            part_refs = refs[at : at + lines]
            at += lines
            total = sum(part[...].astype(jnp.float32) for part in part_refs).astype(low)
            for index, far in enumerate(members):
                refs[far - ways][...] = total[index * capacity : (index + 1) * capacity]

    head_sums = whole_call(
        total_body, [((capacity, back_cols), low)] * ways, *[block for group in groups for block in head_back[group]]
    )
    head_sums = mirrored_all(head_sums, "sp")

    def final_body(mixed_ref, routes_ref, *refs):
        head_refs, tail_refs, (out,) = refs[:ways], refs[ways : ways + lines], refs[ways + lines :]
        block = jnp.concatenate([ref[...] for ref in head_refs], axis=0)
        total = mixed_ref[:, :back_cols] + blend_rows(routes_ref, block)
        out[:, :back_cols] = total.astype(low)
        total = mixed_ref[:, back_cols:]
        for ref in tail_refs:
            total = total + ref[...].astype(jnp.float32)
        out[:, back_cols:] = total.astype(low)

    (output,) = whole_call(final_body, [((tok_rows, width), low)], mixed, routes, *head_sums, *tail_sums)
    return output


def placements(tp):
    both = ("sp",) + tp
    return (
        (
            P(both, None),
            P("sp", tp, None),
            P("sp", tp, None),
            P("sp", tp, None),
            P("sp", tp, None),
            P("sp", tp, None),
            P("sp", tp, None),
            P(tp),
            P(tp),
            P(),
            P(),
            P(tp, None),
            P(tp, None),
            P(),
            P(both, None),
            P(both, None),
            P("sp", None, tp),
            P("sp", None, tp),
            P("sp", tp, None),
        ),
        P(both, None),
    )


def solution(mesh):
    sp_ways, tp_ways = (mesh.shape[axis] for axis in ("sp", "tp"))
    cores = 2

    def program(*arrays):
        resid, query_a, query_b, route_ids = arrays[0], arrays[1], arrays[4], arrays[14]
        block = resid.shape[0] // (sp_ways * tp_ways)
        heads = (query_a.shape[1] + query_b.shape[1]) // tp_ways
        capacity = 3 * route_ids.shape[1] * block // (2 * sp_ways)
        fits = heads == sp_ways and capacity % 16 == 0 and block % 16 == 0 and resid.shape[1] % 2048 == 0
        fits = fits and tp_ways % (2 * cores) == 0
        if fits:
            devices = mesh.devices.reshape(sp_ways, tp_ways // (2 * cores), 2, cores)
            inner, axes = Mesh(devices, ("sp", "zh", "zl", "c")), ("zh", "zl", "c")

            def body(*parts):
                return exchanged_device(*parts)

        else:
            inner, axes, body = mesh, ("tp",), gathered_device
        given, returned = placements(axes)
        mapped = jax.shard_map(body, mesh=inner, in_specs=given, out_specs=returned, check_vma=False)
        return mapped(*arrays)

    return program
```

```python
import math

import jax
import jax.numpy as jnp
from jax import lax
from jax.experimental import pallas as pl
from jax.experimental.pallas import tpu as pltpu
from jax.sharding import Mesh, PartitionSpec as P


EPS = 1e-06
NEG = -1e30
HEAD_SCALE = 1.0 - (0.8 - 0.6 * math.exp(-0.3))
KEY_STEP = 512


def partner(value, axis, apart):
    return lax.ppermute(value, axis, [(i, i ^ 1 << apart) for i in range(lax.axis_size(axis))])


def rms_scaled(values, gain):
    return values * lax.rsqrt(jnp.mean(values * values, axis=-1, keepdims=True) + EPS) * gain


def slot_numbers(route_rows, experts, capacity):
    count, top_count = route_rows.shape
    flat = route_rows.reshape(count * top_count)
    onehot = (flat[:, None] == jnp.arange(experts, dtype=jnp.int32)[None, :]).astype(jnp.int32)
    ranks = jnp.sum((jnp.cumsum(onehot, axis=0) - onehot) * onehot, axis=1)
    return (flat * capacity + ranks).reshape(count, top_count)


def empty_map(count, heads, width):
    return (
        jnp.zeros((count, heads, width), jnp.float32),
        jnp.full((heads, count), NEG, jnp.float32),
        jnp.zeros((heads, count), jnp.float32),
    )


def empty_group(query, value):
    return (
        empty_map(query.shape[0], query.shape[1], value.shape[2]),
        empty_map(query.shape[0], query.shape[1], value.shape[2]),
    )


def map_update(state, query, keys, values, allowed, scale):
    weighted, maximum, sums = state
    scores = jnp.einsum("qhd,khd->hqk", query, keys, preferred_element_type=jnp.float32) * scale
    scores = jnp.where(allowed[None], scores, NEG)
    fresh = jnp.maximum(maximum, jnp.max(scores, axis=2))
    weights = jnp.where(allowed[None], jnp.exp(scores - fresh[:, :, None]), 0.0)
    factor = jnp.exp(maximum - fresh)
    sums = sums * factor + jnp.sum(weights, axis=2)
    added = jnp.einsum(
        "hqk,khv->qhv", weights.astype(jnp.bfloat16), values, preferred_element_type=jnp.float32
    )
    weighted = weighted * jnp.transpose(factor)[:, :, None] + added
    return (weighted, fresh, sums)


def group_update(states, query, keys, values, allowed):
    width = query.shape[2] // 2
    scale = 1.0 / math.sqrt(width)
    return tuple(
        (
            map_update(
                states[which],
                query[:, :, which * width : (which + 1) * width],
                keys[:, :, which * width : (which + 1) * width],
                values,
                allowed,
                scale,
            )
            for which in range(2)
        )
    )


def set_update(carry, queries, pieces):
    rows_a, rows_b, query_pos = queries
    piece_key_a, piece_value_a, piece_key_b, piece_value_b = pieces
    length = piece_key_a.shape[0]
    step = math.gcd(length, KEY_STEP)
    latest = query_pos[-1]

    def inner(index, states):
        first = index * step

        def compute(current):
            keys_a = lax.dynamic_slice_in_dim(piece_key_a, first, step, 0)
            values_a = lax.dynamic_slice_in_dim(piece_value_a, first, step, 0)
            keys_b = lax.dynamic_slice_in_dim(piece_key_b, first, step, 0)
            values_b = lax.dynamic_slice_in_dim(piece_value_b, first, step, 0)
            key_pos = first + jnp.arange(step, dtype=jnp.int32)
            allowed = key_pos[None, :] <= query_pos[:, None]
            return (
                group_update(current[0], rows_a, keys_a, values_a, allowed),
                group_update(current[1], rows_b, keys_b, values_b, allowed),
            )

        return lax.cond(first <= latest, compute, lambda current: current, states)

    return lax.fori_loop(0, length // step, inner, carry)


def finish_group(states, mix, gain):
    outputs = [state[0] / jnp.transpose(state[2])[:, :, None] for state in states]
    mixed = outputs[0] - mix[None, :, None] * outputs[1]
    normed = rms_scaled(mixed, gain) * HEAD_SCALE
    return normed.astype(jnp.bfloat16).reshape(mixed.shape[0], -1)


def gathered_device(
    resid,
    query_a,
    key_a,
    value_a,
    query_b,
    key_b,
    value_b,
    mix_a,
    mix_b,
    head_gain_a,
    head_gain_b,
    proj_a,
    proj_b,
    norm_gain,
    route_ids,
    route_weights,
    expert_gate,
    expert_up,
    expert_down,
):
    seq_rows = query_a.shape[0]
    sp_ways = lax.axis_size("sp")
    place = lax.axis_index("sp")
    positions = place * seq_rows + jnp.arange(seq_rows, dtype=jnp.int32)
    levels = sp_ways.bit_length() - 1
    half = seq_rows // 2
    moved = jnp.concatenate(
        [query_a[half:].reshape(half, -1), query_b[half:].reshape(half, -1)], axis=1
    )
    for bit in range(levels):
        moved = partner(moved, "sp", bit)
    split_at = query_a.shape[1] * query_a.shape[2]
    far_a = moved[:, :split_at].reshape(half, query_a.shape[1], query_a.shape[2])
    far_b = moved[:, split_at:].reshape(half, query_b.shape[1], query_b.shape[2])
    far_pos = (sp_ways - 1 - place) * seq_rows + half + jnp.arange(half, dtype=jnp.int32)
    query_sets = ((query_a[:half], query_b[:half], positions[:half]), (far_a, far_b, far_pos))

    def fold_keys(carry, pieces):
        return tuple(
            (set_update(states, queries, pieces) for states, queries in zip(carry, query_sets))
        )

    initial = tuple(
        (
            (empty_group(queries[0], value_a), empty_group(queries[1], value_b))
            for queries in query_sets
        )
    )
    results = fold_keys(
        initial,
        (
            lax.all_gather(key_a, "sp", axis=0, tiled=True),
            lax.all_gather(value_a, "sp", axis=0, tiled=True),
            lax.all_gather(key_b, "sp", axis=0, tiled=True),
            lax.all_gather(value_b, "sp", axis=0, tiled=True),
        ),
    )
    finished = [
        (finish_group(states[0], mix_a, head_gain_a), finish_group(states[1], mix_b, head_gain_b))
        for states in results
    ]
    returned = jnp.concatenate([finished[1][0], finished[1][1]], axis=1)
    for bit in range(levels):
        returned = partner(returned, "sp", bit)
    width_a = finished[0][0].shape[1]
    heads_out_a = jnp.concatenate([finished[0][0], returned[:, :width_a]], axis=0)
    heads_out_b = jnp.concatenate([finished[0][1], returned[:, width_a:]], axis=0)
    width = resid.shape[1]
    tok_rows = resid.shape[0]
    top_count = route_ids.shape[1]
    capacity = 3 * top_count * tok_rows // (2 * sp_ways)
    own_slots = slot_numbers(route_ids, sp_ways, capacity)
    term = jnp.dot(heads_out_a, proj_a, preferred_element_type=jnp.float32)
    term = term + jnp.dot(heads_out_b, proj_b, preferred_element_type=jnp.float32)
    mixed = resid.astype(jnp.float32) + lax.psum_scatter(
        lax.optimization_barrier(term.astype(jnp.bfloat16))
        .astype(jnp.float32)
        .astype(jnp.bfloat16),
        "tp",
        scatter_dimension=0,
        tiled=True,
    ).astype(jnp.float32)
    normed = rms_scaled(mixed, norm_gain).astype(jnp.bfloat16)
    lookup = jnp.arange(sp_ways * capacity, dtype=jnp.int32)[:, None]
    spread = jnp.zeros((sp_ways * capacity, tok_rows), jnp.float32)
    for which in range(top_count):
        spread = spread + (own_slots[:, which][None, :] == lookup).astype(jnp.float32)
    outgoing = jnp.dot(
        spread.astype(jnp.bfloat16), normed, preferred_element_type=jnp.float32
    ).astype(jnp.bfloat16)
    arrived = lax.all_to_all(
        outgoing.reshape(sp_ways, capacity, width), "sp", split_axis=0, concat_axis=0, tiled=True
    )
    piece = lax.all_gather(arrived.reshape(sp_ways * capacity, width), "tp", axis=0, tiled=True)
    gate = jnp.dot(piece, expert_gate[0], preferred_element_type=jnp.float32)
    upward = jnp.dot(piece, expert_up[0], preferred_element_type=jnp.float32)
    hidden = (jax.nn.silu(gate) * upward).astype(jnp.bfloat16)
    term = jnp.dot(hidden, expert_down[0], preferred_element_type=jnp.float32)
    summed = lax.psum_scatter(
        lax.optimization_barrier(term.astype(jnp.bfloat16))
        .astype(jnp.float32)
        .astype(jnp.bfloat16),
        "tp",
        scatter_dimension=0,
        tiled=True,
    )
    finished_rows = summed.reshape(sp_ways, capacity, width)
    back = lax.all_to_all(finished_rows, "sp", split_axis=0, concat_axis=0, tiled=True)
    picked = jnp.take(back.reshape(sp_ways * capacity, width), own_slots.reshape(-1), axis=0)
    picked = picked.reshape(tok_rows, top_count, width)
    output = mixed + jnp.sum(route_weights[:, :, None] * picked.astype(jnp.float32), axis=1)
    return output.astype(jnp.bfloat16)


def attend_kernel(scalars, own, gain, *refs, step, width, maps, block, part_rows):
    pieces, (out, scores, packed) = refs[:-3], refs[-3:]
    ways = len(pieces) // 2
    place = pl.program_id(0)
    coef = scalars[0]

    def unpack(group):
        found = pieces[group * ways : (group + 1) * ways]
        value_rows = found[0].shape[0] - 4 * part_rows[group]
        for far, piece in enumerate(found):
            at = own[0] ^ far
            if part_rows[group] < maps or value_rows < width:
                packed[at] = jnp.zeros(packed.shape[1:], packed.dtype)
            for which in range(4):
                begin = which * part_rows[group]
                packed[at, which * maps : which * maps + part_rows[group], :] = piece[begin : begin + part_rows[group], :]
            packed[at, 4 * maps : 4 * maps + value_rows, :] = piece[4 * part_rows[group] :, :]

    @pl.when((place == 0) & (own[1] == 0))
    def _():
        unpack(0)

    @pl.when((place == 0) & (own[1] == 1))
    def _():
        unpack(1)

    queries = [jnp.transpose(packed[place, 2 * which * maps : (2 * which + 1) * maps, :]) for which in range(2)]

    def fold(values, combine):
        parts = [values[:, at * width : (at + 1) * width] for at in range(step // width)]
        while len(parts) > 1:
            parts = [combine(*parts[at : at + 2]) for at in range(0, len(parts), 2)]
        return parts[0]

    def raw(which, index):
        keys = packed[index, (2 * which + 1) * maps : (2 * which + 2) * maps, :]
        return jnp.dot(queries[which], keys, preferred_element_type=jnp.float32)

    row = lax.broadcasted_iota(jnp.int32, (step, step), 0)
    column = lax.broadcasted_iota(jnp.int32, (step, step), 1)
    highest = []
    for which in range(2):
        diagonal = jnp.where(column <= row, raw(which, place), NEG)
        scores[which, place] = diagonal
        highest.append(fold(diagonal, jnp.maximum))

    def first_pass(index, carry):
        found = []
        for which in range(2):
            values = raw(which, index)
            scores[which, index] = values
            found.append(jnp.maximum(carry[which], fold(values, jnp.maximum)))
        return tuple(found)

    highest = lax.fori_loop(0, place, first_pass, tuple(highest))
    tops = [jnp.max(found, axis=1, keepdims=True) * coef for found in highest]

    def second_pass(index, carry):
        values = packed[index, 4 * maps : 4 * maps + width, :]
        found = []
        for which in range(2):
            total, mixed = carry[which]
            weights = jnp.exp2(scores[which, index] * coef - tops[which])
            total = total + fold(weights, jnp.add)
            mixed = mixed + lax.dot_general(
                weights.astype(jnp.bfloat16),
                values,
                (((1,), (1,)), ((), ())),
                preferred_element_type=jnp.float32,
            )
            found.append((total, mixed))
        return tuple(found)

    empty = jnp.zeros((step, width), jnp.float32)
    found = lax.fori_loop(0, place + 1, second_pass, ((empty, empty), (empty, empty)))
    outputs = [mixed / jnp.sum(total, axis=1, keepdims=True) for total, mixed in found]
    mixed = outputs[0] - scalars[1] * outputs[1]
    square = jnp.sum(mixed * mixed, axis=1, keepdims=True) * scalars[2]
    normed = (mixed * lax.rsqrt(square + EPS) * gain[...]).astype(jnp.bfloat16)
    pairs, cores = out.shape[1:3]
    for at in range(step // block):
        begin = at // (pairs * cores) * block
        out[0, at // cores % pairs, at % cores, begin : begin + block] = normed[at * block : (at + 1) * block]


def widen(values, width):
    missing = width - values.shape[-1]
    return jnp.pad(values, [(0, 0)] * (values.ndim - 1) + [(0, missing)]) if missing else values


def fast_memory(limit_mib):
    return pltpu.CompilerParams(vmem_limit_bytes=limit_mib << 20)


def mirrored(value, axis, apart):
    return lax.ppermute(value, axis, [(i, i ^ apart) for i in range(lax.axis_size(axis))])


def mirrored_all(values, axis):
    found = {far: mirrored(values[far], axis, far) for far in reversed(range(1, len(values)))}
    return [values[0]] + [found[far] for far in range(1, len(values))]


def whole_call(body, outs, *operands, scalars=(), flops=0, scratch=(), limit=8, kept=()):
    vmem = pl.BlockSpec(memory_space=pltpu.VMEM)
    return pl.pallas_call(
        body,
        in_specs=[pl.BlockSpec(memory_space=pltpu.SMEM)] * len(scalars) + [vmem] * len(operands),
        out_specs=[vmem] * len(outs),
        out_shape=[(pltpu.HBM if at in kept else pltpu.VMEM)(*out) for at, out in enumerate(outs)],
        scratch_shapes=scratch,
        compiler_params=fast_memory(limit),
        cost_estimate=pl.CostEstimate(flops=flops, bytes_accessed=0, transcendentals=0),
    )(*scalars, *[pltpu.with_memory_space_constraint(operand, pltpu.VMEM) for operand in operands])


def exchanged_heads(query_a, key_a, value_a, query_b, key_b, value_b, mix_a, mix_b, head_gain_a, head_gain_b, block):
    seq_rows, heads_a, _ = query_a.shape
    ways = lax.axis_size("sp")
    cores, pair_lines = lax.axis_size("c"), lax.axis_size("zl")
    place = lax.axis_index("sp")
    groups = ((query_a, key_a, value_a), (query_b, key_b, value_b))
    width = -(-max(group[2].shape[2] for group in groups) // 128) * 128
    maps = -(-max(group[0].shape[2] // 2 for group in groups) // 16) * 16

    turned = lax.optimization_barrier([[jnp.transpose(array, (1, 2, 0)) for array in group] for group in groups])
    core = lax.axis_index("c")
    part_rows = [query.shape[1] // 2 for query, _, _ in turned]
    piece_rows = [4 * part + group[2].shape[1] for part, group in zip(part_rows, turned)]

    def kind_of(index, core):
        return (index + heads_a * core) % ways

    def pack_body(at, *refs):
        arrays, outs = (refs[:3], refs[3:6]), (refs[6 : 6 + ways], refs[6 + ways :])
        for far in range(ways):
            kind = kind_of(at[0] ^ far, at[1])

            def fill(group, head):
                query, key, value = arrays[group]
                out, part = outs[group][far], part_rows[group]
                for which in range(2):
                    for second, array in enumerate((query, key)):
                        begin = (2 * which + second) * part
                        out[begin : begin + part, :] = array[head, which * part : (which + 1) * part, :]
                out[4 * part :, :] = value[head]

            @pl.when(kind < heads_a)
            def _():
                fill(0, kind)

            @pl.when(kind >= heads_a)
            def _():
                fill(1, kind - heads_a)

    packed = whole_call(
        pack_body,
        [((rows, seq_rows), jnp.bfloat16) for rows in piece_rows for _ in range(ways)],
        *turned[0],
        *turned[1],
        scalars=(jnp.stack([place, core]).astype(jnp.int32),),
        kept=(0, ways),
    )
    pieces = []
    for group in range(2):
        pieces.append(packed[group * ways])
        for far in range(1, ways):
            ends = [(index, core) for index in range(ways) for core in range(cores)]
            ends = [(index, core) for index, core in ends if (kind_of(index, core) >= heads_a) == (group == 1)]
            route = [((index ^ far) * cores + core, index * cores + core) for index, core in ends]
            pieces.append(lax.ppermute(packed[group * ways + far], ("sp", "c"), route))
    kind = kind_of(place, core)
    first = kind < heads_a
    gain = jnp.where(first, widen(head_gain_a, width), widen(head_gain_b, width)) * HEAD_SCALE
    coef_a, coef_b = [math.log2(math.e) / math.sqrt(group[0].shape[2] // 2) for group in groups]
    scalars = jnp.stack(
        [
            jnp.where(first, coef_a, coef_b).astype(jnp.float32),
            lax.dynamic_index_in_dim(jnp.concatenate([mix_a, mix_b]), kind, 0, False),
            jnp.where(first, 1.0 / value_a.shape[2], 1.0 / value_b.shape[2]).astype(jnp.float32),
        ]
    )
    pairs = (ways * seq_rows) * (ways + 1) * seq_rows
    shape = (ways, pair_lines, cores, seq_rows // (pair_lines * cores), width)
    smem = pl.BlockSpec(memory_space=pltpu.SMEM)
    pieces_in = [
        pltpu.with_memory_space_constraint(piece, pltpu.VMEM if at % ways else pltpu.HBM)
        for at, piece in enumerate(pieces)
    ]
    mixed = pl.pallas_call(
        lambda *refs: attend_kernel(
            *refs, step=seq_rows, width=width, maps=maps, block=block, part_rows=part_rows
        ),
        grid=(ways,),
        in_specs=[smem, smem, pl.BlockSpec((1, width), lambda index: (0, 0))]
        + [pl.BlockSpec(memory_space=pltpu.VMEM)] * len(pieces),
        out_specs=pl.BlockSpec((1,) + shape[1:], lambda index: (index, 0, 0, 0, 0)),
        out_shape=pltpu.HBM(shape, jnp.bfloat16),
        scratch_shapes=[
            pltpu.VMEM((2, ways, seq_rows, seq_rows), jnp.float32),
            pltpu.VMEM((ways, 4 * maps + width, seq_rows), jnp.bfloat16),
        ],
        compiler_params=pltpu.CompilerParams(dimension_semantics=("arbitrary",), vmem_limit_bytes=16 << 20),
        cost_estimate=pl.CostEstimate(flops=2 * pairs * (maps + width), bytes_accessed=0, transcendentals=pairs),
        name="attend",
    )(scalars, jnp.stack([place, jnp.where(first, 0, 1)]).astype(jnp.int32), gain[None, :], *pieces_in)
    flat = mixed.reshape((-1,) + shape[3:])
    return lax.all_to_all(flat, ("sp", "zl", "c"), split_axis=0, concat_axis=0, tiled=True).reshape(shape)


def project(heads, proj_a, proj_b, block, heads_a):
    ways, pair_lines, cores, rows, _ = heads.shape
    model = proj_a.shape[1]
    lines = rows // block
    weights = []
    for line in range(pair_lines):
        found = (proj_a, proj_b)
        if line > 0:
            found = [mirrored(array, "zl", line) for array in found]
        weights += found
        for apart in range(1, cores):
            weights += [mirrored(array, "c", apart) for array in found]
    where = jnp.stack([lax.axis_index(axis) for axis in ("c", "zl", "zh")]).astype(jnp.int32)
    step = math.gcd(model, 512)
    narrow = proj_b.shape[0] // (ways - heads_a)
    wide = proj_a.shape[0] // heads_a

    def body(at, heads_ref, *refs):
        sets, outs = refs[: len(weights)], refs[len(weights) :]
        pairs = []
        for apart in range(pair_lines * cores):
            core, line = at[0] ^ apart % cores, at[1] ^ apart // cores

            def taken(head, used):
                index = (head + heads_a * core) % ways
                found = [heads_ref[index, line, core, pl.ds((at[2] ^ far) * block, block), :] for far in range(lines)]
                return jnp.concatenate(found, axis=0)[:, :used]

            left_a = jnp.concatenate([taken(head, wide) for head in range(heads_a)], axis=1)
            left_b = jnp.concatenate([taken(head, narrow) for head in range(heads_a, ways)], axis=1)
            pairs += [(left_a, sets[2 * apart]), (left_b, sets[2 * apart + 1])]
        for first in range(0, model, step):
            span = slice(first, first + step)
            total = None
            for left, right in pairs:
                piece = jnp.dot(left, right[:, span], preferred_element_type=jnp.float32)
                total = piece if total is None else total + piece
            for far in range(lines):
                outs[far][:, span] = total[far * block : (far + 1) * block].astype(jnp.bfloat16)

    return whole_call(
        body,
        [((block, model), jnp.bfloat16)] * lines,
        heads,
        *weights,
        scalars=(where,),
        flops=rows * model * (proj_a.shape[0] + proj_b.shape[0]) * len(weights),
    )


def expert_hidden(rows_ref, gate_ref, up_ref, held, first, count):
    hidden = gate_ref.shape[1]
    tile = math.gcd(hidden, 256)
    for at in range(hidden // tile):
        span = slice(at * tile, (at + 1) * tile)
        gate = jnp.dot(rows_ref[pl.ds(first, count), :], gate_ref[:, span], preferred_element_type=jnp.float32)
        upward = jnp.dot(rows_ref[pl.ds(first, count), :], up_ref[:, span], preferred_element_type=jnp.float32)
        held[:, span] = (jax.nn.silu(gate) * upward).astype(jnp.bfloat16)


def expert_down(held, down_ref, out_ref, first, count):
    model = down_ref.shape[1]
    tile = math.gcd(model, 512)
    for at in range(model // tile):
        span = slice(at * tile, (at + 1) * tile)
        total = jnp.dot(held, down_ref[:, span], preferred_element_type=jnp.float32)
        out_ref[pl.ds(first, count), span] = total.astype(jnp.bfloat16)


def expert_call(rows, weights, out_cols, after=()):
    count = rows.shape[0]
    hidden = weights[-1].shape[0] if len(weights) != 2 else weights[0].shape[1]
    tile = max(size for size in range(16, 257, 16) if count % size == 0)
    flops = 2 * count * sum(weight.size for weight in weights)

    def body(rows_ref, *refs):
        weight_refs, (out_ref, held) = refs[: len(weights)], refs[-2:]

        def step(index, carry):
            first = index * tile
            if len(weights) > 1:
                expert_hidden(rows_ref, *weight_refs[:2], held, first, tile)
            if len(weights) == 2:
                out_ref[pl.ds(first, tile), :] = held[...]
            else:
                left = held[...] if len(weights) == 3 else rows_ref[pl.ds(first, tile), :]
                expert_down(left, weight_refs[-1], out_ref, first, tile)
            return carry

        lax.fori_loop(0, count // tile, step, 0)

    (out,) = whole_call(
        body,
        [((count, out_cols), jnp.bfloat16)],
        rows,
        *weights,
        *after,
        flops=flops,
        scratch=[pltpu.VMEM((tile, hidden), jnp.bfloat16)],
    )
    return out


def exchanged_device(
    resid,
    query_a,
    key_a,
    value_a,
    query_b,
    key_b,
    value_b,
    mix_a,
    mix_b,
    head_gain_a,
    head_gain_b,
    proj_a,
    proj_b,
    norm_gain,
    route_ids,
    route_weights,
    expert_gate,
    expert_up,
    down_w,
):
    line_axes = ("zh", "zl")
    ways, cores, line_pairs, lines = (lax.axis_size(axis) for axis in ("sp", "c", "zh", line_axes))
    place = lax.axis_index("sp")
    tok_rows, width = resid.shape
    top_count = route_ids.shape[1]
    capacity = 3 * top_count * tok_rows // (2 * ways)
    slots_all = ways * capacity
    low = jnp.bfloat16
    head_cols, back_cols = (width * part // 16 // 128 * 128 for part in (4, 5))
    tail_cols, rest_cols = width - head_cols, width - back_cols

    heads = exchanged_heads(
        query_a, key_a, value_a, query_b, key_b, value_b, mix_a, mix_b, head_gain_a, head_gain_b, tok_rows
    )

    slots = slot_numbers(route_ids ^ place, ways, capacity)
    routes = jnp.concatenate([jnp.transpose(slots).astype(jnp.float32), jnp.transpose(route_weights)], axis=0)
    line_routes = mirrored_all([routes] * lines, line_axes)

    def hits(routes_ref, which):
        lookup = lax.broadcasted_iota(jnp.int32, (slots_all, tok_rows), 0)
        return routes_ref[which : which + 1, :].astype(jnp.int32) == lookup

    def spread_rows(routes_ref, tokens):
        spread = sum(hits(routes_ref, which).astype(jnp.float32) for which in range(top_count)).astype(low)
        return jnp.dot(spread, tokens, preferred_element_type=jnp.float32).astype(low)

    def blend_rows(routes_ref, block):
        weights = sum(
            jnp.where(hits(routes_ref, which), routes_ref[top_count + which : top_count + which + 1, :], 0.0)
            for which in range(top_count)
        )
        upper = weights.astype(low)
        total = None
        for part in (upper, (weights - upper.astype(jnp.float32)).astype(low)):
            piece = lax.dot_general(part, block, (((0,), (0,)), ((), ())), preferred_element_type=jnp.float32)
            total = piece if total is None else total + piece
        return total

    parts = project(heads, proj_a, proj_b, tok_rows, query_a.shape[1])
    parts = mirrored_all(parts, "zh")

    def norm_body(*refs):
        part_refs, outs = refs[:line_pairs], refs[line_pairs + 3 :]
        resid_ref, gain_ref, routes_ref = refs[line_pairs : line_pairs + 3]
        mixed = resid_ref[...].astype(jnp.float32)
        for part in part_refs:
            mixed = mixed + part[...].astype(jnp.float32)
        outs[0][...] = mixed
        normed = rms_scaled(mixed, gain_ref[...]).astype(low)
        outs[1][...] = normed[:, head_cols:]
        picked = spread_rows(routes_ref, normed[:, :head_cols])
        for far in range(ways):
            outs[2 + far][...] = picked[far * capacity : (far + 1) * capacity]

    mixed, tail, *heads_out = whole_call(
        norm_body,
        [((tok_rows, width), jnp.float32), ((tok_rows, tail_cols), low)] + [((capacity, head_cols), low)] * ways,
        *parts,
        resid,
        norm_gain[None, :],
        routes,
    )
    tails = mirrored_all([tail] * lines, line_axes)
    heads_in = mirrored_all(heads_out, "sp")
    groups = {"near": list(range(ways - 1)), "far": [ways - 1]}
    head_own = jnp.concatenate(heads_in, axis=0)
    head_blocks = mirrored_all([head_own] * lines, line_axes)

    weights = (expert_gate[0], expert_up[0], down_w[0])

    def spread_body(*refs):
        tail_refs, routes_refs, outs = refs[:lines], refs[lines : 2 * lines], refs[-ways:]
        for line in range(lines):
            picked = spread_rows(routes_refs[line], tail_refs[line][...])
            for far in range(ways):
                outs[far][line * capacity : (line + 1) * capacity] = picked[far * capacity : (far + 1) * capacity]

    tail_blocks = list(
        whole_call(
            spread_body, [((lines * capacity, tail_cols), low)] * ways, *tails, *line_routes, head_own, *weights[:2]
        )
    )
    for members in groups.values():
        for far in members:
            if far > 0:
                tail_blocks[far] = mirrored(tail_blocks[far], "sp", far)

    def join(group, *after):
        members = groups[group]

        def body(*refs):
            head_refs, tail_refs, out = refs[:lines], refs[lines : lines + len(members)], refs[-1]
            for line in range(lines):
                for at, far in enumerate(members):
                    first = (line * len(members) + at) * capacity
                    out[first : first + capacity, :head_cols] = head_refs[line][far * capacity : (far + 1) * capacity]
                    out[first : first + capacity, head_cols:] = tail_refs[at][line * capacity : (line + 1) * capacity]

        (rows,) = whole_call(
            body,
            [((lines * len(members) * capacity, width), low)],
            *head_blocks,
            *[tail_blocks[far] for far in members],
            *after,
        )
        return rows

    def pair(group, own_part, other_parts):
        members = groups[group]

        def body(*refs):
            part_refs, outs = refs[:cores], refs[cores:]
            for line in range(lines):
                for at in range(len(members)):
                    first = (line * len(members) + at) * capacity
                    total = part_refs[0][first : first + capacity].astype(jnp.float32)
                    for part in part_refs[1:]:
                        total = total + part[first : first + capacity].astype(jnp.float32)
                    total = total.astype(low)
                    outs[line][at * capacity : (at + 1) * capacity] = total[:, :back_cols]
                    outs[lines + at][line * capacity : (line + 1) * capacity] = total[:, back_cols:]

        count = len(members)
        return whole_call(
            body,
            [((count * capacity, back_cols), low)] * lines + [((lines * capacity, rest_cols), low)] * count,
            own_part,
            *other_parts,
        )

    assert cores == 2
    tail_back, head_back, before = {}, {}, ()
    for group, members in groups.items():
        rows = join(group, *before)
        other_rows = mirrored(rows, "c", 1)
        hidden = expert_call(rows, weights[:2], weights[0].shape[1])
        after = (hidden,) + tuple(head_back[done][0] for done in head_back)
        other_part = expert_call(other_rows, weights, width, after)
        own_part = expert_call(hidden, weights[2:], width)
        back = pair(group, own_part, [mirrored(other_part, "c", 1)])
        for at, far in reversed(list(enumerate(members))):
            tail_back[far] = mirrored(back[lines + at], "sp", far) if far else back[lines + at]
        head_back[group] = mirrored_all(back[:lines], line_axes)
        before = (other_part,)
    tail_back = [tail_back[far] for far in range(ways)]

    def blend_body(*refs):
        tail_refs, routes_refs, outs = refs[:ways], refs[ways : ways + lines], refs[ways + lines :]
        for line in range(lines):
            block = jnp.concatenate([ref[line * capacity : (line + 1) * capacity] for ref in tail_refs], axis=0)
            outs[line][...] = blend_rows(routes_refs[line], block).astype(low)

    tail_sums = whole_call(blend_body, [((tok_rows, rest_cols), low)] * lines, *tail_back, *line_routes)
    tail_sums = mirrored_all(tail_sums, line_axes)

    def total_body(*refs):
        at = 0
        for members in groups.values():
            part_refs = refs[at : at + lines]
            at += lines
            total = sum(part[...].astype(jnp.float32) for part in part_refs).astype(low)
            for index, far in enumerate(members):
                refs[far - ways][...] = total[index * capacity : (index + 1) * capacity]

    head_sums = whole_call(
        total_body, [((capacity, back_cols), low)] * ways, *[block for group in groups for block in head_back[group]]
    )
    head_sums = mirrored_all(head_sums, "sp")

    def final_body(mixed_ref, routes_ref, *refs):
        head_refs, tail_refs, (out,) = refs[:ways], refs[ways : ways + lines], refs[ways + lines :]
        block = jnp.concatenate([ref[...] for ref in head_refs], axis=0)
        total = mixed_ref[:, :back_cols] + blend_rows(routes_ref, block)
        out[:, :back_cols] = total.astype(low)
        total = mixed_ref[:, back_cols:]
        for ref in tail_refs:
            total = total + ref[...].astype(jnp.float32)
        out[:, back_cols:] = total.astype(low)

    (output,) = whole_call(final_body, [((tok_rows, width), low)], mixed, routes, *head_sums, *tail_sums)
    return output


def placements(tp):
    both = ("sp",) + tp
    return (
        (
            P(both, None),
            P("sp", tp, None),
            P("sp", tp, None),
            P("sp", tp, None),
            P("sp", tp, None),
            P("sp", tp, None),
            P("sp", tp, None),
            P(tp),
            P(tp),
            P(),
            P(),
            P(tp, None),
            P(tp, None),
            P(),
            P(both, None),
            P(both, None),
            P("sp", None, tp),
            P("sp", None, tp),
            P("sp", tp, None),
        ),
        P(both, None),
    )


def solution(mesh):
    sp_ways, tp_ways = (mesh.shape[axis] for axis in ("sp", "tp"))
    cores = 2

    def program(*arrays):
        resid, query_a, query_b, route_ids = arrays[0], arrays[1], arrays[4], arrays[14]
        block = resid.shape[0] // (sp_ways * tp_ways)
        heads = (query_a.shape[1] + query_b.shape[1]) // tp_ways
        capacity = 3 * route_ids.shape[1] * block // (2 * sp_ways)
        fits = heads == sp_ways and capacity % 16 == 0 and block % 16 == 0 and resid.shape[1] % 2048 == 0
        fits = fits and tp_ways % (2 * cores) == 0
        if fits:
            devices = mesh.devices.reshape(sp_ways, tp_ways // (2 * cores), 2, cores)
            inner, axes = Mesh(devices, ("sp", "zh", "zl", "c")), ("zh", "zl", "c")

            def body(*parts):
                return exchanged_device(*parts)

        else:
            inner, axes, body = mesh, ("tp",), gathered_device
        given, returned = placements(axes)
        mapped = jax.shard_map(body, mesh=inner, in_specs=given, out_specs=returned, check_vma=False)
        return mapped(*arrays)

    return program
```

```python
import math

import jax
import jax.numpy as jnp
from jax import lax
from jax.experimental import pallas as pl
from jax.experimental.pallas import tpu as pltpu
from jax.sharding import Mesh, PartitionSpec as P


EPS = 1e-06
NEG = -1e30
HEAD_SCALE = 1.0 - (0.8 - 0.6 * math.exp(-0.3))
KEY_STEP = 512


def partner(value, axis, apart):
    return lax.ppermute(value, axis, [(i, i ^ 1 << apart) for i in range(lax.axis_size(axis))])


def rms_scaled(values, gain):
    return values * lax.rsqrt(jnp.mean(values * values, axis=-1, keepdims=True) + EPS) * gain


def slot_numbers(route_rows, experts, capacity):
    count, top_count = route_rows.shape
    flat = route_rows.reshape(count * top_count)
    onehot = (flat[:, None] == jnp.arange(experts, dtype=jnp.int32)[None, :]).astype(jnp.int32)
    ranks = jnp.sum((jnp.cumsum(onehot, axis=0) - onehot) * onehot, axis=1)
    return (flat * capacity + ranks).reshape(count, top_count)


def empty_map(count, heads, width):
    return (
        jnp.zeros((count, heads, width), jnp.float32),
        jnp.full((heads, count), NEG, jnp.float32),
        jnp.zeros((heads, count), jnp.float32),
    )


def empty_group(query, value):
    return (
        empty_map(query.shape[0], query.shape[1], value.shape[2]),
        empty_map(query.shape[0], query.shape[1], value.shape[2]),
    )


def map_update(state, query, keys, values, allowed, scale):
    weighted, maximum, sums = state
    scores = jnp.einsum("qhd,khd->hqk", query, keys, preferred_element_type=jnp.float32) * scale
    scores = jnp.where(allowed[None], scores, NEG)
    fresh = jnp.maximum(maximum, jnp.max(scores, axis=2))
    weights = jnp.where(allowed[None], jnp.exp(scores - fresh[:, :, None]), 0.0)
    factor = jnp.exp(maximum - fresh)
    sums = sums * factor + jnp.sum(weights, axis=2)
    added = jnp.einsum(
        "hqk,khv->qhv", weights.astype(jnp.bfloat16), values, preferred_element_type=jnp.float32
    )
    weighted = weighted * jnp.transpose(factor)[:, :, None] + added
    return (weighted, fresh, sums)


def group_update(states, query, keys, values, allowed):
    width = query.shape[2] // 2
    scale = 1.0 / math.sqrt(width)
    return tuple(
        (
            map_update(
                states[which],
                query[:, :, which * width : (which + 1) * width],
                keys[:, :, which * width : (which + 1) * width],
                values,
                allowed,
                scale,
            )
            for which in range(2)
        )
    )


def set_update(carry, queries, pieces):
    rows_a, rows_b, query_pos = queries
    piece_key_a, piece_value_a, piece_key_b, piece_value_b = pieces
    length = piece_key_a.shape[0]
    step = math.gcd(length, KEY_STEP)
    latest = query_pos[-1]

    def inner(index, states):
        first = index * step

        def compute(current):
            keys_a = lax.dynamic_slice_in_dim(piece_key_a, first, step, 0)
            values_a = lax.dynamic_slice_in_dim(piece_value_a, first, step, 0)
            keys_b = lax.dynamic_slice_in_dim(piece_key_b, first, step, 0)
            values_b = lax.dynamic_slice_in_dim(piece_value_b, first, step, 0)
            key_pos = first + jnp.arange(step, dtype=jnp.int32)
            allowed = key_pos[None, :] <= query_pos[:, None]
            return (
                group_update(current[0], rows_a, keys_a, values_a, allowed),
                group_update(current[1], rows_b, keys_b, values_b, allowed),
            )

        return lax.cond(first <= latest, compute, lambda current: current, states)

    return lax.fori_loop(0, length // step, inner, carry)


def finish_group(states, mix, gain):
    outputs = [state[0] / jnp.transpose(state[2])[:, :, None] for state in states]
    mixed = outputs[0] - mix[None, :, None] * outputs[1]
    normed = rms_scaled(mixed, gain) * HEAD_SCALE
    return normed.astype(jnp.bfloat16).reshape(mixed.shape[0], -1)


def gathered_device(
    resid,
    query_a,
    key_a,
    value_a,
    query_b,
    key_b,
    value_b,
    mix_a,
    mix_b,
    head_gain_a,
    head_gain_b,
    proj_a,
    proj_b,
    norm_gain,
    route_ids,
    route_weights,
    expert_gate,
    expert_up,
    expert_down,
):
    seq_rows = query_a.shape[0]
    sp_ways = lax.axis_size("sp")
    place = lax.axis_index("sp")
    positions = place * seq_rows + jnp.arange(seq_rows, dtype=jnp.int32)
    levels = sp_ways.bit_length() - 1
    half = seq_rows // 2
    moved = jnp.concatenate(
        [query_a[half:].reshape(half, -1), query_b[half:].reshape(half, -1)], axis=1
    )
    for bit in range(levels):
        moved = partner(moved, "sp", bit)
    split_at = query_a.shape[1] * query_a.shape[2]
    far_a = moved[:, :split_at].reshape(half, query_a.shape[1], query_a.shape[2])
    far_b = moved[:, split_at:].reshape(half, query_b.shape[1], query_b.shape[2])
    far_pos = (sp_ways - 1 - place) * seq_rows + half + jnp.arange(half, dtype=jnp.int32)
    query_sets = ((query_a[:half], query_b[:half], positions[:half]), (far_a, far_b, far_pos))

    def fold_keys(carry, pieces):
        return tuple(
            (set_update(states, queries, pieces) for states, queries in zip(carry, query_sets))
        )

    initial = tuple(
        (
            (empty_group(queries[0], value_a), empty_group(queries[1], value_b))
            for queries in query_sets
        )
    )
    results = fold_keys(
        initial,
        (
            lax.all_gather(key_a, "sp", axis=0, tiled=True),
            lax.all_gather(value_a, "sp", axis=0, tiled=True),
            lax.all_gather(key_b, "sp", axis=0, tiled=True),
            lax.all_gather(value_b, "sp", axis=0, tiled=True),
        ),
    )
    finished = [
        (finish_group(states[0], mix_a, head_gain_a), finish_group(states[1], mix_b, head_gain_b))
        for states in results
    ]
    returned = jnp.concatenate([finished[1][0], finished[1][1]], axis=1)
    for bit in range(levels):
        returned = partner(returned, "sp", bit)
    width_a = finished[0][0].shape[1]
    heads_out_a = jnp.concatenate([finished[0][0], returned[:, :width_a]], axis=0)
    heads_out_b = jnp.concatenate([finished[0][1], returned[:, width_a:]], axis=0)
    width = resid.shape[1]
    tok_rows = resid.shape[0]
    top_count = route_ids.shape[1]
    capacity = 3 * top_count * tok_rows // (2 * sp_ways)
    own_slots = slot_numbers(route_ids, sp_ways, capacity)
    term = jnp.dot(heads_out_a, proj_a, preferred_element_type=jnp.float32)
    term = term + jnp.dot(heads_out_b, proj_b, preferred_element_type=jnp.float32)
    mixed = resid.astype(jnp.float32) + lax.psum_scatter(
        lax.optimization_barrier(term.astype(jnp.bfloat16))
        .astype(jnp.float32)
        .astype(jnp.bfloat16),
        "tp",
        scatter_dimension=0,
        tiled=True,
    ).astype(jnp.float32)
    normed = rms_scaled(mixed, norm_gain).astype(jnp.bfloat16)
    lookup = jnp.arange(sp_ways * capacity, dtype=jnp.int32)[:, None]
    spread = jnp.zeros((sp_ways * capacity, tok_rows), jnp.float32)
    for which in range(top_count):
        spread = spread + (own_slots[:, which][None, :] == lookup).astype(jnp.float32)
    outgoing = jnp.dot(
        spread.astype(jnp.bfloat16), normed, preferred_element_type=jnp.float32
    ).astype(jnp.bfloat16)
    arrived = lax.all_to_all(
        outgoing.reshape(sp_ways, capacity, width), "sp", split_axis=0, concat_axis=0, tiled=True
    )
    piece = lax.all_gather(arrived.reshape(sp_ways * capacity, width), "tp", axis=0, tiled=True)
    gate = jnp.dot(piece, expert_gate[0], preferred_element_type=jnp.float32)
    upward = jnp.dot(piece, expert_up[0], preferred_element_type=jnp.float32)
    hidden = (jax.nn.silu(gate) * upward).astype(jnp.bfloat16)
    term = jnp.dot(hidden, expert_down[0], preferred_element_type=jnp.float32)
    summed = lax.psum_scatter(
        lax.optimization_barrier(term.astype(jnp.bfloat16))
        .astype(jnp.float32)
        .astype(jnp.bfloat16),
        "tp",
        scatter_dimension=0,
        tiled=True,
    )
    finished_rows = summed.reshape(sp_ways, capacity, width)
    back = lax.all_to_all(finished_rows, "sp", split_axis=0, concat_axis=0, tiled=True)
    picked = jnp.take(back.reshape(sp_ways * capacity, width), own_slots.reshape(-1), axis=0)
    picked = picked.reshape(tok_rows, top_count, width)
    output = mixed + jnp.sum(route_weights[:, :, None] * picked.astype(jnp.float32), axis=1)
    return output.astype(jnp.bfloat16)


def attend_kernel(scalars, own, gain, *refs, step, width, maps, block):
    pieces, (out, scores, packed) = refs[:-3], refs[-3:]
    place = pl.program_id(0)
    coef = scalars[0]

    @pl.when(place == 0)
    def _():
        for far, piece in enumerate(pieces):
            packed[own[0] ^ far] = piece[...]

    def counted(first, last, body, carry):
        for index in range(first, last):
            carry = body(index, carry)
        return carry

    def attend_block(place):
        queries = [jnp.transpose(packed[place, 2 * which * maps : (2 * which + 1) * maps, :]) for which in range(2)]

        def fold(values, combine):
            parts = [values[:, at * width : (at + 1) * width] for at in range(step // width)]
            while len(parts) > 1:
                parts = [combine(*parts[at : at + 2]) for at in range(0, len(parts), 2)]
            return parts[0]

        def raw(which, index):
            keys = packed[index, (2 * which + 1) * maps : (2 * which + 2) * maps, :]
            return jnp.dot(queries[which], keys, preferred_element_type=jnp.float32)

        row = lax.broadcasted_iota(jnp.int32, (step, step), 0)
        column = lax.broadcasted_iota(jnp.int32, (step, step), 1)
        highest = []
        for which in range(2):
            diagonal = jnp.where(column <= row, raw(which, place), NEG)
            scores[which, place] = diagonal
            highest.append(fold(diagonal, jnp.maximum))

        def first_pass(index, carry):
            found = []
            for which in range(2):
                values = raw(which, index)
                scores[which, index] = values
                found.append(jnp.maximum(carry[which], fold(values, jnp.maximum)))
            return tuple(found)

        highest = counted(0, place, first_pass, tuple(highest))
        tops = [jnp.max(found, axis=1, keepdims=True) * coef for found in highest]

        def second_pass(index, carry):
            values = packed[index, 4 * maps : 4 * maps + width, :]
            found = []
            for which in range(2):
                total, mixed = carry[which]
                weights = jnp.exp2(scores[which, index] * coef - tops[which])
                total = total + fold(weights, jnp.add)
                mixed = mixed + lax.dot_general(
                    weights.astype(jnp.bfloat16),
                    values,
                    (((1,), (1,)), ((), ())),
                    preferred_element_type=jnp.float32,
                )
                found.append((total, mixed))
            return tuple(found)

        empty = jnp.zeros((step, width), jnp.float32)
        found = counted(0, place + 1, second_pass, ((empty, empty), (empty, empty)))
        outputs = [mixed / jnp.sum(total, axis=1, keepdims=True) for total, mixed in found]
        mixed = outputs[0] - scalars[1] * outputs[1]
        square = jnp.sum(mixed * mixed, axis=1, keepdims=True) * scalars[2]
        normed = (mixed * lax.rsqrt(square + EPS) * gain[...]).astype(jnp.bfloat16)
        pairs, cores = out.shape[1:3]
        for at in range(step // block):
            begin = at // (pairs * cores) * block
            out[0, at // cores % pairs, at % cores, begin : begin + block] = normed[at * block : (at + 1) * block]

    for at in range(len(pieces)):
        pl.when(place == at)(lambda at=at: attend_block(at))


def widen(values, width):
    missing = width - values.shape[-1]
    return jnp.pad(values, [(0, 0)] * (values.ndim - 1) + [(0, missing)]) if missing else values


def fast_memory(limit_mib):
    return pltpu.CompilerParams(vmem_limit_bytes=limit_mib << 20)


def mirrored(value, axis, apart):
    return lax.ppermute(value, axis, [(i, i ^ apart) for i in range(lax.axis_size(axis))])


def mirrored_all(values, axis):
    found = {far: mirrored(values[far], axis, far) for far in reversed(range(1, len(values)))}
    return [values[0]] + [found[far] for far in range(1, len(values))]


def whole_call(body, outs, *operands, scalars=(), flops=0, scratch=(), limit=8, kept=(), loose=()):
    vmem = pl.BlockSpec(memory_space=pltpu.VMEM)
    call = pl.pallas_call(
        body,
        in_specs=[pl.BlockSpec(memory_space=pltpu.SMEM)] * len(scalars) + [vmem] * len(operands),
        out_specs=[vmem] * len(outs),
        out_shape=[(pltpu.HBM if at in kept else pltpu.VMEM)(*out) for at, out in enumerate(outs)],
        scratch_shapes=scratch,
        compiler_params=fast_memory(limit),
        cost_estimate=pl.CostEstimate(flops=flops, bytes_accessed=0, transcendentals=0),
    )
    spaces = [pltpu.HBM if at in loose else pltpu.VMEM for at in range(len(operands))]
    return call(*scalars, *[pltpu.with_memory_space_constraint(*pair) for pair in zip(operands, spaces)])


def exchanged_heads(query_a, key_a, value_a, query_b, key_b, value_b, mix_a, mix_b, head_gain_a, head_gain_b, block):
    seq_rows, heads_a, _ = query_a.shape
    ways = lax.axis_size("sp")
    cores, pair_lines = lax.axis_size("c"), lax.axis_size("zl")
    place = lax.axis_index("sp")
    groups = ((query_a, key_a, value_a), (query_b, key_b, value_b))
    width = -(-max(group[2].shape[2] for group in groups) // 128) * 128
    maps = -(-max(group[0].shape[2] // 2 for group in groups) // 16) * 16

    turned = lax.optimization_barrier([[jnp.transpose(array, (1, 2, 0)) for array in group] for group in groups])

    def pack_body(at, *refs):
        arrays, outs = (refs[:3], refs[3:6]), refs[6:]

        def fill(out, group, head):
            query, key, value = arrays[group]
            half = query.shape[1] // 2
            if half < maps or value.shape[1] < width:
                out[...] = jnp.zeros_like(out)
            for which in range(2):
                for second, array in enumerate((query, key)):
                    begin = (2 * which + second) * maps
                    out[begin : begin + half, :] = array[head, which * half : (which + 1) * half, :]
            out[4 * maps : 4 * maps + value.shape[1], :] = value[head]

        for far in range(ways):
            kind = at[0] ^ far
            pl.when(kind < heads_a)(lambda out=outs[far], kind=kind: fill(out, 0, kind))
            pl.when(kind >= heads_a)(lambda out=outs[far], kind=kind: fill(out, 1, kind - heads_a))

    pieces = whole_call(
        pack_body,
        [((4 * maps + width, seq_rows), jnp.bfloat16)] * ways,
        *turned[0],
        *turned[1],
        scalars=(place[None].astype(jnp.int32),),
        loose=(3, 4, 5),
        kept=(0,),
    )
    pieces = mirrored_all(pieces, "sp")
    first = place < heads_a
    gain = jnp.where(first, widen(head_gain_a, width), widen(head_gain_b, width)) * HEAD_SCALE
    coef_a, coef_b = [math.log2(math.e) / math.sqrt(group[0].shape[2] // 2) for group in groups]
    scalars = jnp.stack(
        [
            jnp.where(first, coef_a, coef_b).astype(jnp.float32),
            lax.dynamic_index_in_dim(jnp.concatenate([mix_a, mix_b]), place, 0, False),
            jnp.where(first, 1.0 / value_a.shape[2], 1.0 / value_b.shape[2]).astype(jnp.float32),
        ]
    )
    pairs = (ways * seq_rows) * (ways + 1) * seq_rows
    shape = (ways, pair_lines, cores, seq_rows // (pair_lines * cores), width)
    smem = pl.BlockSpec(memory_space=pltpu.SMEM)
    own_piece = pltpu.with_memory_space_constraint(pieces[0], pltpu.HBM)
    mixed = pl.pallas_call(
        lambda *refs: attend_kernel(*refs, step=seq_rows, width=width, maps=maps, block=block),
        grid=(ways,),
        in_specs=[smem, smem, pl.BlockSpec((1, width), lambda index: (0, 0))]
        + [pl.BlockSpec(piece.shape, lambda index: (0, 0)) for piece in pieces],
        out_specs=pl.BlockSpec((1,) + shape[1:], lambda index: (index, 0, 0, 0, 0)),
        out_shape=pltpu.HBM(shape, jnp.bfloat16),
        scratch_shapes=[
            pltpu.VMEM((2, ways, seq_rows, seq_rows), jnp.float32),
            pltpu.VMEM((ways,) + pieces[0].shape, jnp.bfloat16),
        ],
        compiler_params=pltpu.CompilerParams(dimension_semantics=("arbitrary",), vmem_limit_bytes=24 << 20),
        cost_estimate=pl.CostEstimate(flops=2 * pairs * (maps + width), bytes_accessed=0, transcendentals=pairs),
        name="attend",
    )(scalars, place[None].astype(jnp.int32), gain[None, :], own_piece, *pieces[1:])
    flat = mixed.reshape((-1,) + shape[3:])
    return lax.all_to_all(flat, ("sp", "zl", "c"), split_axis=0, concat_axis=0, tiled=True).reshape(shape)


def project(heads, proj_a, proj_b, block, heads_a):
    ways, pair_lines, cores, rows, _ = heads.shape
    model = proj_a.shape[1]
    lines = rows // block
    weights = []
    for line in range(pair_lines):
        found = (proj_a, proj_b)
        if line > 0:
            found = [mirrored(array, "zl", line) for array in found]
        weights += found
        for apart in range(1, cores):
            weights += [mirrored(array, "c", apart) for array in found]
    where = jnp.stack([lax.axis_index(axis) for axis in ("c", "zl", "zh")]).astype(jnp.int32)
    step = math.gcd(model, 512)
    narrow = proj_b.shape[0] // (ways - heads_a)
    wide = proj_a.shape[0] // heads_a

    def body(at, heads_ref, *refs):
        sets, outs = refs[: len(weights)], refs[len(weights) :]
        pairs = []
        for apart in range(pair_lines * cores):
            core, line = at[0] ^ apart % cores, at[1] ^ apart // cores

            def taken(head, used):
                found = [heads_ref[head, line, core, pl.ds((at[2] ^ far) * block, block), :] for far in range(lines)]
                return jnp.concatenate(found, axis=0)[:, :used]

            left_a = jnp.concatenate([taken(head, wide) for head in range(heads_a)], axis=1)
            left_b = jnp.concatenate([taken(head, narrow) for head in range(heads_a, ways)], axis=1)
            pairs += [(left_a, sets[2 * apart]), (left_b, sets[2 * apart + 1])]
        for first in range(0, model, step):
            span = slice(first, first + step)
            total = None
            for left, right in pairs:
                piece = jnp.dot(left, right[:, span], preferred_element_type=jnp.float32)
                total = piece if total is None else total + piece
            for far in range(lines):
                outs[far][:, span] = total[far * block : (far + 1) * block].astype(jnp.bfloat16)

    return whole_call(
        body,
        [((block, model), jnp.bfloat16)] * lines,
        heads,
        *weights,
        scalars=(where,),
        flops=rows * model * (proj_a.shape[0] + proj_b.shape[0]) * len(weights),
    )


def expert_hidden(rows_ref, gate_ref, up_ref, held, first, count):
    hidden = gate_ref.shape[1]
    tile = math.gcd(hidden, 256)
    for at in range(hidden // tile):
        span = slice(at * tile, (at + 1) * tile)
        gate = jnp.dot(rows_ref[pl.ds(first, count), :], gate_ref[:, span], preferred_element_type=jnp.float32)
        upward = jnp.dot(rows_ref[pl.ds(first, count), :], up_ref[:, span], preferred_element_type=jnp.float32)
        held[:, span] = (jax.nn.silu(gate) * upward).astype(jnp.bfloat16)


def expert_down(held, down_ref, out_ref, first, count):
    model = down_ref.shape[1]
    tile = math.gcd(model, 512)
    for at in range(model // tile):
        span = slice(at * tile, (at + 1) * tile)
        total = jnp.dot(held, down_ref[:, span], preferred_element_type=jnp.float32)
        out_ref[pl.ds(first, count), span] = total.astype(jnp.bfloat16)


def expert_call(rows, weights, out_cols, after=()):
    count = rows.shape[0]
    hidden = weights[-1].shape[0] if len(weights) != 2 else weights[0].shape[1]
    tile = max(size for size in range(16, 257, 16) if count % size == 0)
    flops = 2 * count * sum(weight.size for weight in weights)

    def body(rows_ref, *refs):
        weight_refs, (out_ref, held) = refs[: len(weights)], refs[-2:]

        def step(index, carry):
            first = index * tile
            if len(weights) > 1:
                expert_hidden(rows_ref, *weight_refs[:2], held, first, tile)
            if len(weights) == 2:
                out_ref[pl.ds(first, tile), :] = held[...]
            else:
                left = held[...] if len(weights) == 3 else rows_ref[pl.ds(first, tile), :]
                expert_down(left, weight_refs[-1], out_ref, first, tile)
            return carry

        lax.fori_loop(0, count // tile, step, 0)

    (out,) = whole_call(
        body,
        [((count, out_cols), jnp.bfloat16)],
        rows,
        *weights,
        *after,
        flops=flops,
        scratch=[pltpu.VMEM((tile, hidden), jnp.bfloat16)],
    )
    return out


def exchanged_device(
    resid,
    query_a,
    key_a,
    value_a,
    query_b,
    key_b,
    value_b,
    mix_a,
    mix_b,
    head_gain_a,
    head_gain_b,
    proj_a,
    proj_b,
    norm_gain,
    route_ids,
    route_weights,
    expert_gate,
    expert_up,
    down_w,
):
    line_axes = ("zh", "zl")
    ways, cores, line_pairs, lines = (lax.axis_size(axis) for axis in ("sp", "c", "zh", line_axes))
    place = lax.axis_index("sp")
    tok_rows, width = resid.shape
    top_count = route_ids.shape[1]
    capacity = 3 * top_count * tok_rows // (2 * ways)
    slots_all = ways * capacity
    low = jnp.bfloat16
    head_cols, back_cols = (width * part // 16 // 128 * 128 for part in (4, 5))
    tail_cols, rest_cols = width - head_cols, width - back_cols

    heads = exchanged_heads(
        query_a, key_a, value_a, query_b, key_b, value_b, mix_a, mix_b, head_gain_a, head_gain_b, tok_rows
    )

    slots = slot_numbers(route_ids ^ place, ways, capacity)
    routes = jnp.concatenate([jnp.transpose(slots).astype(jnp.float32), jnp.transpose(route_weights)], axis=0)
    line_routes = mirrored_all([routes] * lines, line_axes)

    def hits(routes_ref, which):
        lookup = lax.broadcasted_iota(jnp.int32, (slots_all, tok_rows), 0)
        return routes_ref[which : which + 1, :].astype(jnp.int32) == lookup

    def spread_rows(routes_ref, tokens):
        spread = sum(hits(routes_ref, which).astype(jnp.float32) for which in range(top_count)).astype(low)
        return jnp.dot(spread, tokens, preferred_element_type=jnp.float32).astype(low)

    def blend_rows(routes_ref, block):
        weights = sum(
            jnp.where(hits(routes_ref, which), routes_ref[top_count + which : top_count + which + 1, :], 0.0)
            for which in range(top_count)
        )
        upper = weights.astype(low)
        total = None
        for part in (upper, (weights - upper.astype(jnp.float32)).astype(low)):
            piece = lax.dot_general(part, block, (((0,), (0,)), ((), ())), preferred_element_type=jnp.float32)
            total = piece if total is None else total + piece
        return total

    parts = project(heads, proj_a, proj_b, tok_rows, query_a.shape[1])
    parts = mirrored_all(parts, "zh")

    def norm_body(*refs):
        part_refs, outs = refs[:line_pairs], refs[line_pairs + 3 :]
        resid_ref, gain_ref, routes_ref = refs[line_pairs : line_pairs + 3]
        mixed = resid_ref[...].astype(jnp.float32)
        for part in part_refs:
            mixed = mixed + part[...].astype(jnp.float32)
        outs[0][...] = mixed
        normed = rms_scaled(mixed, gain_ref[...]).astype(low)
        outs[1][...] = normed[:, head_cols:]
        picked = spread_rows(routes_ref, normed[:, :head_cols])
        for far in range(ways):
            outs[2 + far][...] = picked[far * capacity : (far + 1) * capacity]

    mixed, tail, *heads_out = whole_call(
        norm_body,
        [((tok_rows, width), jnp.float32), ((tok_rows, tail_cols), low)] + [((capacity, head_cols), low)] * ways,
        *parts,
        resid,
        norm_gain[None, :],
        routes,
    )
    tails = mirrored_all([tail] * lines, line_axes)
    heads_in = mirrored_all(heads_out, "sp")
    groups = {"near": list(range(ways - 1)), "far": [ways - 1]}
    head_own = jnp.concatenate(heads_in, axis=0)
    head_blocks = mirrored_all([head_own] * lines, line_axes)

    weights = (expert_gate[0], expert_up[0], down_w[0])

    def spread_body(*refs):
        tail_refs, routes_refs, outs = refs[:lines], refs[lines : 2 * lines], refs[-ways:]
        for line in range(lines):
            picked = spread_rows(routes_refs[line], tail_refs[line][...])
            for far in range(ways):
                outs[far][line * capacity : (line + 1) * capacity] = picked[far * capacity : (far + 1) * capacity]

    tail_blocks = list(
        whole_call(
            spread_body, [((lines * capacity, tail_cols), low)] * ways, *tails, *line_routes, head_own, *weights[:2]
        )
    )
    for members in groups.values():
        for far in members:
            if far > 0:
                tail_blocks[far] = mirrored(tail_blocks[far], "sp", far)

    def join(group, *after):
        members = groups[group]

        def body(*refs):
            head_refs, tail_refs, out = refs[:lines], refs[lines : lines + len(members)], refs[-1]
            for line in range(lines):
                for at, far in enumerate(members):
                    first = (line * len(members) + at) * capacity
                    out[first : first + capacity, :head_cols] = head_refs[line][far * capacity : (far + 1) * capacity]
                    out[first : first + capacity, head_cols:] = tail_refs[at][line * capacity : (line + 1) * capacity]

        (rows,) = whole_call(
            body,
            [((lines * len(members) * capacity, width), low)],
            *head_blocks,
            *[tail_blocks[far] for far in members],
            *after,
        )
        return rows

    def pair(group, own_part, other_parts):
        members = groups[group]

        def body(*refs):
            part_refs, outs = refs[:cores], refs[cores:]
            for line in range(lines):
                for at in range(len(members)):
                    first = (line * len(members) + at) * capacity
                    total = part_refs[0][first : first + capacity].astype(jnp.float32)
                    for part in part_refs[1:]:
                        total = total + part[first : first + capacity].astype(jnp.float32)
                    total = total.astype(low)
                    outs[line][at * capacity : (at + 1) * capacity] = total[:, :back_cols]
                    outs[lines + at][line * capacity : (line + 1) * capacity] = total[:, back_cols:]

        count = len(members)
        return whole_call(
            body,
            [((count * capacity, back_cols), low)] * lines + [((lines * capacity, rest_cols), low)] * count,
            own_part,
            *other_parts,
        )

    assert cores == 2
    tail_back, head_back, before = {}, {}, ()
    for group, members in groups.items():
        rows = join(group, *before)
        other_rows = mirrored(rows, "c", 1)
        hidden = expert_call(rows, weights[:2], weights[0].shape[1])
        after = (hidden,) + tuple(head_back[done][0] for done in head_back)
        other_part = expert_call(other_rows, weights, width, after)
        own_part = expert_call(hidden, weights[2:], width)
        back = pair(group, own_part, [mirrored(other_part, "c", 1)])
        for at, far in reversed(list(enumerate(members))):
            tail_back[far] = mirrored(back[lines + at], "sp", far) if far else back[lines + at]
        head_back[group] = mirrored_all(back[:lines], line_axes)
        before = (other_part,)
    tail_back = [tail_back[far] for far in range(ways)]

    def blend_body(*refs):
        tail_refs, routes_refs, outs = refs[:ways], refs[ways : ways + lines], refs[ways + lines :]
        for line in range(lines):
            block = jnp.concatenate([ref[line * capacity : (line + 1) * capacity] for ref in tail_refs], axis=0)
            outs[line][...] = blend_rows(routes_refs[line], block).astype(low)

    tail_sums = whole_call(blend_body, [((tok_rows, rest_cols), low)] * lines, *tail_back, *line_routes)
    tail_sums = mirrored_all(tail_sums, line_axes)

    def total_body(*refs):
        at = 0
        for members in groups.values():
            part_refs = refs[at : at + lines]
            at += lines
            total = sum(part[...].astype(jnp.float32) for part in part_refs).astype(low)
            for index, far in enumerate(members):
                refs[far - ways][...] = total[index * capacity : (index + 1) * capacity]

    head_sums = whole_call(
        total_body, [((capacity, back_cols), low)] * ways, *[block for group in groups for block in head_back[group]]
    )
    head_sums = mirrored_all(head_sums, "sp")

    def final_body(mixed_ref, routes_ref, *refs):
        head_refs, tail_refs, (out,) = refs[:ways], refs[ways : ways + lines], refs[ways + lines :]
        block = jnp.concatenate([ref[...] for ref in head_refs], axis=0)
        total = mixed_ref[:, :back_cols] + blend_rows(routes_ref, block)
        out[:, :back_cols] = total.astype(low)
        total = mixed_ref[:, back_cols:]
        for ref in tail_refs:
            total = total + ref[...].astype(jnp.float32)
        out[:, back_cols:] = total.astype(low)

    (output,) = whole_call(final_body, [((tok_rows, width), low)], mixed, routes, *head_sums, *tail_sums, kept=(0,))
    return output


def placements(tp):
    both = ("sp",) + tp
    return (
        (
            P(both, None),
            P("sp", tp, None),
            P("sp", tp, None),
            P("sp", tp, None),
            P("sp", tp, None),
            P("sp", tp, None),
            P("sp", tp, None),
            P(tp),
            P(tp),
            P(),
            P(),
            P(tp, None),
            P(tp, None),
            P(),
            P(both, None),
            P(both, None),
            P("sp", None, tp),
            P("sp", None, tp),
            P("sp", tp, None),
        ),
        P(both, None),
    )


def solution(mesh):
    sp_ways, tp_ways = (mesh.shape[axis] for axis in ("sp", "tp"))
    cores = 2

    def program(*arrays):
        resid, query_a, query_b, route_ids = arrays[0], arrays[1], arrays[4], arrays[14]
        block = resid.shape[0] // (sp_ways * tp_ways)
        heads = (query_a.shape[1] + query_b.shape[1]) // tp_ways
        capacity = 3 * route_ids.shape[1] * block // (2 * sp_ways)
        fits = heads == sp_ways and capacity % 16 == 0 and block % 16 == 0 and resid.shape[1] % 2048 == 0
        fits = fits and tp_ways % (2 * cores) == 0
        if fits:
            devices = mesh.devices.reshape(sp_ways, tp_ways // (2 * cores), 2, cores)
            inner, axes = Mesh(devices, ("sp", "zh", "zl", "c")), ("zh", "zl", "c")

            def body(*parts):
                return exchanged_device(*parts)

        else:
            inner, axes, body = mesh, ("tp",), gathered_device
        given, returned = placements(axes)
        mapped = jax.shard_map(body, mesh=inner, in_specs=given, out_specs=returned, check_vma=False)
        return mapped(*arrays)

    return program
```
